128 devices in a mesh: sp: 16 (over z, x), tp: 8 (over y, core).
Axes of the slice: x: 4, y: 4, z: 4, core: 2. Of those that a mesh axis runs over, the one named last changes fastest.
Arguments:
- query_narrow: bfloat16 [4096, 1024], P('sp', 'tp'), may hold values from -6 to 6
- key_narrow: bfloat16 [4096, 1024], P('sp', 'tp'), may hold values from -6 to 6
- value_narrow: bfloat16 [4096, 1024], P('sp', 'tp'), may hold values from -12 to 12
- query_broad: bfloat16 [4096, 1024], P('sp', 'tp'), may hold values from -6 to 6
- key_broad: bfloat16 [4096, 1024], P('sp', 'tp'), may hold values from -6 to 6
- value_broad: bfloat16 [4096, 1024], P('sp', 'tp'), may hold values from -12 to 12
- offset_narrow: bfloat16 [16, 4096], P('tp', 'sp'), as said below
- offset_broad: bfloat16 [8, 4096], P('tp', 'sp'), as said below
- residual: bfloat16 [4096, 2048], P(('sp', 'tp')), may hold values from -6 to 6
- out_narrow: bfloat16 [1024, 2048], P('tp'), may hold values from -0.25 to 0.25
- out_broad: bfloat16 [1024, 2048], P('tp'), may hold values from -0.25 to 0.25
- norm_gain: float32 [2048], replicated, may hold values from 0.1 to 1.9
- up_proj: bfloat16 [2048, 8192], P('sp', 'tp'), may hold values from -0.125 to 0.125
- down_proj: bfloat16 [8192, 2048], P('tp', 'sp'), may hold values from -0.0625 to 0.0625
Outputs:
- output: bfloat16 [4096, 2048], P(('sp', 'tp'))
The draws below stay inside these ranges and needn't reach their ends.
Inputs may be any that keep to these rules, and one draw needn't show every extreme that they name: `offset_narrow`: additive score offsets of each head for each key position. `offset_broad`: additive score offsets of each head for each key position.
All inputs are finite; a program needn't handle non-finite values.
Results may differ from the reference program's by a relative error of at most 0.018.
Values may be sent and summed in bfloat16 or wider, within the bound.
A program may use at most 64 MiB of HBM per device.

```python
import math
import jax
import jax.numpy as jnp
from jax import lax

D = 2048
FF = 8192
NARROW_HEADS = 16
NARROW_SIZE = 64
BROAD_HEADS = 8
BROAD_SIZE = 128
TOKENS_PER_SHARD = 256
SEQUENCE_TOKENS = 4096


def stick_offsets(key, total_heads, salt):
    key = jax.random.fold_in(key, salt)
    random_subkeys = jax.random.split(key, 6)
    gradual_drift = jax.random.randint(random_subkeys[0], (total_heads, 1), 0, 2).astype(jnp.float32)
    slow_base = -jnp.log(jnp.float32(SEQUENCE_TOKENS)) - 2.0
    fast_base = -jnp.log(jnp.float32(40.0)) - 0.5
    base_value = gradual_drift * slow_base + (1.0 - gradual_drift) * fast_base
    base_value = base_value + jax.random.uniform(random_subkeys[1], (total_heads, 1), jnp.float32, -0.3, 0.3)
    slope_factor = jax.random.uniform(random_subkeys[2], (total_heads, SEQUENCE_TOKENS // TOKENS_PER_SHARD), jnp.float32, -0.7, 0.7)
    slope_factor = jnp.repeat(slope_factor, TOKENS_PER_SHARD, axis=1)
    jagged_noise = 0.5 * jax.random.truncated_normal(random_subkeys[3], -2.0, 2.0, (total_heads, SEQUENCE_TOKENS), jnp.float32)
    spike_amount = (jax.random.randint(random_subkeys[4], (total_heads, SEQUENCE_TOKENS), 0, 2 * TOKENS_PER_SHARD) == 0).astype(jnp.float32) * gradual_drift
    spike_height = jax.random.uniform(random_subkeys[5], (total_heads, SEQUENCE_TOKENS), jnp.float32, -1.9, -0.9)
    shift_amount = spike_amount * spike_height + (1.0 - spike_amount) * (base_value + slope_factor + jagged_noise)
    return shift_amount.astype(jnp.bfloat16)


def draw_offset_narrow(key, part):
    return stick_offsets(key, NARROW_HEADS, 11)


def draw_offset_broad(key, part):
    return stick_offsets(key, BROAD_HEADS, 23)


def level_of(own_key, shape, cuts, low, top_value):
    factor_of, own = 1.0, jax.random.fold_in(own_key, 6)
    for dim, parts in cuts:
        draws = jnp.exp(jax.random.uniform(jax.random.fold_in(own, dim), (parts,), jnp.float32, low / len(cuts), top_value / len(cuts)))
        factor_of = factor_of * jnp.repeat(draws, shape[dim] // parts).reshape([-1 if axis == dim else 1 for axis in range(len(shape))])
    return factor_of


def centred(stream_key, extent, spread, bound, pieces=(), held_as=jnp.bfloat16):
    result = spread * jax.random.normal(stream_key, extent, jnp.float32)
    if pieces:
        result = result * level_of(stream_key, extent, pieces, -0.22, 0.18)
    return jnp.clip(result, -bound, bound).astype(held_as)


def setup_inputs(seed: int = 0) -> dict:
    arg_keys = jax.random.split(jax.random.key(seed), 15)
    query_narrow = centred(arg_keys[0], (SEQUENCE_TOKENS, NARROW_HEADS * NARROW_SIZE), 1.0, 6.0, ((0, 16), (1, 8)))
    key_narrow = centred(arg_keys[1], (SEQUENCE_TOKENS, NARROW_HEADS * NARROW_SIZE), 1.0, 6.0, ((0, 16), (1, 8)))
    value_narrow = centred(arg_keys[2], (SEQUENCE_TOKENS, NARROW_HEADS * NARROW_SIZE), 2.0, 12.0, ((0, 16), (1, 8)))
    query_broad = centred(arg_keys[3], (SEQUENCE_TOKENS, BROAD_HEADS * BROAD_SIZE), 1.0, 6.0, ((0, 16), (1, 8)))
    key_broad = centred(arg_keys[4], (SEQUENCE_TOKENS, BROAD_HEADS * BROAD_SIZE), 1.0, 6.0, ((0, 16), (1, 8)))
    value_broad = centred(arg_keys[5], (SEQUENCE_TOKENS, BROAD_HEADS * BROAD_SIZE), 2.0, 12.0, ((0, 16), (1, 8)))
    offset_narrow = draw_offset_narrow(jax.random.fold_in(arg_keys[14], 71), 0)
    offset_broad = draw_offset_broad(jax.random.fold_in(arg_keys[14], 71), 0)
    residual = centred(arg_keys[8], (SEQUENCE_TOKENS, D), 1.0, 6.0, ((0, 128),))
    out_narrow = centred(arg_keys[9], (NARROW_HEADS * NARROW_SIZE, D), ((NARROW_HEADS * NARROW_SIZE + BROAD_HEADS * BROAD_SIZE) // 4) ** -0.5, 0.25, ((0, 8),))
    out_broad = centred(arg_keys[10], (BROAD_HEADS * BROAD_SIZE, D), ((NARROW_HEADS * NARROW_SIZE + BROAD_HEADS * BROAD_SIZE) // 4) ** -0.5, 0.25, ((0, 8),))
    norm_gain = jnp.clip(1.0 + 0.18 * jax.random.normal(arg_keys[11], (D,), jnp.float32), 0.1, 1.9)
    up_proj = centred(arg_keys[12], (D, FF), D ** -0.5, 0.125, ((0, 16), (1, 8)))
    down_proj = centred(arg_keys[13], (FF, D), FF ** -0.5, 0.0625, ((0, 8), (1, 16)))
    return {"query_narrow": query_narrow, "key_narrow": key_narrow, "value_narrow": value_narrow, "query_broad": query_broad, "key_broad": key_broad, "value_broad": value_broad, "offset_narrow": offset_narrow, "offset_broad": offset_broad, "residual": residual, "out_narrow": out_narrow, "out_broad": out_broad, "norm_gain": norm_gain, "up_proj": up_proj, "down_proj": down_proj}


def stick_group(query, key, value, shift_amount, total_heads, head_size):
    tokens = query.shape[0]
    span_rows = math.gcd(tokens, 512)
    blocks = tokens // span_rows
    q_all = query.astype(jnp.float32).reshape(tokens, total_heads, head_size)
    k_all = key.astype(jnp.float32).reshape(tokens, total_heads, head_size)
    v_all = value.astype(jnp.float32).reshape(tokens, total_heads, head_size)
    off_all = shift_amount.astype(jnp.float32)

    def query_block(index):
        q_start = index * span_rows
        q_block = lax.dynamic_slice_in_dim(q_all, q_start, span_rows, 0)
        query_pos = q_start + jnp.arange(span_rows, dtype=jnp.int32)

        def key_block(turn_index, state):
            keep_sum, running = state
            k_start = (index - turn_index) * span_rows
            k_block = lax.dynamic_slice_in_dim(k_all, k_start, span_rows, 0)
            v_block = lax.dynamic_slice_in_dim(v_all, k_start, span_rows, 0)
            o_block = lax.dynamic_slice_in_dim(off_all, k_start, span_rows, 1)
            key_pos = k_start + jnp.arange(span_rows, dtype=jnp.int32)
            scores = jnp.einsum('qhe,khe->hqk', q_block, k_block) * head_size ** (-0.5) + o_block[:, None, :]
            causal = (key_pos[None, :] < query_pos[:, None])[None]
            log_keep = jnp.where(causal, jax.nn.log_sigmoid(-scores), jnp.float32(0.0))
            keep_after = lax.cumsum(log_keep, axis=2, reverse=True) - log_keep
            weight = jnp.where(causal, jnp.exp(jax.nn.log_sigmoid(scores) + keep_after + keep_sum[:, :, None]), jnp.float32(0.0))
            rounded = lax.optimization_barrier(weight.astype(jnp.bfloat16)).astype(jnp.float32)
            running = running + jnp.einsum('hqk,khe->qhe', rounded, v_block)
            return (keep_sum + lax.optimization_barrier(jnp.sum(log_keep, axis=2)), running)
        start_state = (jnp.zeros((total_heads, span_rows), jnp.float32), jnp.zeros((span_rows, total_heads, head_size), jnp.float32))
        keep_sum, running = lax.fori_loop(jnp.int32(0), index + 1, key_block, start_state)
        return running.reshape(span_rows, total_heads * head_size)
    mixed = lax.map(query_block, jnp.arange(blocks, dtype=jnp.int32))
    return mixed.reshape(tokens, total_heads * head_size).astype(jnp.bfloat16)

def reference(query_narrow, key_narrow, value_narrow, query_broad, key_broad, value_broad, offset_narrow, offset_broad, residual, out_narrow, out_broad, norm_gain, up_proj, down_proj):
    mixed_narrow = stick_group(query_narrow, key_narrow, value_narrow, offset_narrow, NARROW_HEADS, NARROW_SIZE)
    mixed_broad = stick_group(query_broad, key_broad, value_broad, offset_broad, BROAD_HEADS, BROAD_SIZE)
    attended = jnp.dot(mixed_narrow, out_narrow, preferred_element_type=jnp.float32) + jnp.dot(mixed_broad, out_broad, preferred_element_type=jnp.float32)
    updated = residual.astype(jnp.float32) + attended
    scale = lax.rsqrt(lax.optimization_barrier(jnp.mean(updated * updated, axis=-1, keepdims=True)) + 1e-06)
    normed = (updated * scale * norm_gain).astype(jnp.bfloat16)
    hidden = jnp.square(jax.nn.relu(jnp.dot(normed, up_proj, preferred_element_type=jnp.float32))).astype(jnp.bfloat16)
    return (updated + jnp.dot(hidden, down_proj, preferred_element_type=jnp.float32)).astype(jnp.bfloat16)
```

```python
import functools
import heapq

import jax
import jax.numpy as jnp
from jax import lax
from jax.experimental import pallas as pl
from jax.experimental.pallas import tpu as pltpu
from jax.sharding import PartitionSpec as P

MESH = pl.DeviceIdType.MESH
LOG2E = 1.4426950408889634
F32 = jnp.float32
BF16 = jnp.bfloat16

KN, OFF, VN, KB, VB, KV_ROWS = 0, 256, 272, 528, 784, 1040
KV_PARTS = ((KN, 272), (VN, 256), (KB, 256), (VB, 256))


def children(q, dx, dz):
    first, second = (dx, dz) if q < 2 else (dz, dx)
    a, b = ("x", "z") if q < 2 else ("z", "x")
    odd = q % 2
    out = []

    def node(f, s):
        return (f, s) if q < 2 else (s, f)

    if second == 0:
        if first == 0:
            out += [(a, 1, *node(1, 0)), (a, -1, *node(3, 0))]
        elif first == 1 and odd == 0:
            out += [(a, 1, *node(2, 0))]
        elif first == 3 and odd == 1:
            out += [(a, -1, *node(2, 0))]
    if second == 0:
        out += [(b, 1, *node(first, 1)), (b, -1, *node(first, 3))]
    elif second == 1 and odd == 0:
        out += [(b, 1, *node(first, 2))]
    elif second == 3 and odd == 1:
        out += [(b, -1, *node(first, 2))]
    return out


def own_sends():
    firsts, rest = [], []
    for q in range(4):
        a = "x" if q < 2 else "z"
        for child in children(q, 0, 0):
            (firsts if child[0] == a else rest).append((q, *child))
    return firsts + rest


def arrivals():
    free = {}
    queue = []

    def send(now, q, axis, step, dx, dz):
        start = max(now, free.get((axis, step), 0.0))
        free[axis, step] = start + 1.4
        heapq.heappush(queue, (start + 1.4 + 1.7, q, dx, dz))

    for entry in own_sends():
        send(0.0, *entry)
    order = []
    while queue:
        now, q, dx, dz = heapq.heappop(queue)
        order.append((q, dx, dz))
        for child in children(q, dx, dz):
            send(now, q, *child)
    return order


ORDER = arrivals()


def body(
    qn_hbm, kn_hbm, vn_hbm, qb_hbm, kb_hbm, vb_hbm, offn_ref, offb_ref, res_hbm,
    on_hbm, ob_hbm, gain_ref, up_hbm, down_hbm, out_ref,
    kv_buf, up_buf, down_buf, q_buf, res_buf, outw_buf, tri_buf, acc_buf,
    part_buf, pair_buf, sum_buf, mid_in, mid_out, last_out, last_in,
    upd_buf, norm_buf, hidden_buf,
    load_sem, recv_sem, send_sem, pair_sem, mid_sem, last_sem, row_sem, y_send,
):
    s = lax.axis_index("sp")
    t = lax.axis_index("tp")
    x, z = lax.rem(s, 4), lax.div(s, 4)
    c, y = lax.rem(t, 2), lax.div(t, 2)

    def xz(dx, dz):
        return lax.rem(z + dz + 4, 4) * 4 + lax.rem(x + dx + 4, 4)

    def at_tp(dy):
        return lax.rem(y + dy + 4, 4) * 2 + c

    neighbour = {
        ("x", 1): {"sp": xz(1, 0), "tp": t},
        ("x", -1): {"sp": xz(-1, 0), "tp": t},
        ("z", 1): {"sp": xz(0, 1), "tp": t},
        ("z", -1): {"sp": xz(0, -1), "tp": t},
        "pair": {"sp": s, "tp": y * 2 + (1 - c)},
        ("y", 1): {"sp": s, "tp": at_tp(1)},
        ("y", -1): {"sp": s, "tp": at_tp(-1)},
    }

    own = pl.multiple_of(s * 128, 128)
    loads = [
        (kn_hbm, kv_buf.at[s, pl.ds(KN, 256)]),
        (vn_hbm, kv_buf.at[s, pl.ds(VN, 256)]),
        (kb_hbm, kv_buf.at[s, pl.ds(KB, 256)]),
        (vb_hbm, kv_buf.at[s, pl.ds(VB, 256)]),
        (up_hbm, up_buf.at[pl.ds(own, 128)]),
        (down_hbm, down_buf.at[s]),
        (qn_hbm, q_buf.at[0]),
        (qb_hbm, q_buf.at[1]),
        (on_hbm, outw_buf.at[pl.ds(0, 128)]),
        (ob_hbm, outw_buf.at[pl.ds(128, 128)]),
        (res_hbm, res_buf),
    ]
    loads = [pltpu.make_async_copy(a, b, load_sem.at[k]) for k, (a, b) in enumerate(loads)]
    for copy in loads:
        copy.start()

    barrier = pltpu.get_barrier_semaphore()
    for target in neighbour.values():
        pl.semaphore_signal(barrier, inc=1, device_id=target, device_id_type=MESH)

    offsets = [offn_ref[0:1, :], offn_ref[1:2, :], offb_ref[0:1, :]]
    rows = []
    for line in offsets:
        wide = line.astype(F32)
        rows += [wide[:, :128], wide[:, 128:]]
    rows.append(jnp.zeros((10, 128), F32))
    kv_buf[s, OFF : OFF + 16, :] = jnp.concatenate(rows, axis=0).astype(BF16)
    later = lax.broadcasted_iota(jnp.int32, (256, 256), 0)
    earlier = lax.broadcasted_iota(jnp.int32, (256, 256), 1)
    tri_buf[...] = jnp.where(later >= earlier, 1.0, 0.0).astype(BF16)
    pl.semaphore_wait(barrier, 7)

    def piece(g, slot, q):
        if g == 0:
            start, size = KV_PARTS[q]
            return kv_buf.at[slot, pl.ds(start, size)]
        if g == 1:
            return up_buf.at[pl.ds(pl.multiple_of(slot * 128 + q * 32, 32), 32)]
        return down_buf.at[slot, pl.ds(q * 256, 256)]

    def send(g, slot, q, axis, step, dx, dz):
        ref = piece(g, slot, q)
        pltpu.make_async_remote_copy(
            src_ref=ref, dst_ref=ref, send_sem=send_sem.at[g],
            recv_sem=recv_sem.at[g, q, dz * 4 + dx],
            device_id=neighbour[axis, step], device_id_type=MESH,
        ).start()

    def start_gather(g):
        for entry in own_sends():
            send(g, s, *entry)

    def pass_on(g, events):
        for q, dx, dz in events:
            slot = xz(-dx, -dz)
            ref = piece(g, slot, q)
            pltpu.make_async_copy(ref, ref, recv_sem.at[g, q, dz * 4 + dx]).wait()
            for child in children(q, dx, dz):
                send(g, slot, q, *child)

    for copy in loads[:4]:
        copy.wait()
    start_gather(0)
    for copy in loads[4:8]:
        copy.wait()
    lane = lax.broadcasted_iota(jnp.int32, (256, 128), 1)
    acc_buf[...] = jnp.zeros_like(acc_buf)
    pass_on(0, ORDER[:44])
    start_gather(1)
    pass_on(0, ORDER[44:])
    start_gather(2)

    zero = jnp.zeros((), BF16)
    queries = (
        jnp.where(lane < 64, q_buf[0], zero),
        jnp.where(lane >= 64, q_buf[0], zero),
        q_buf[1],
    )
    scales = (LOG2E * 64**-0.5, LOG2E * 64**-0.5, LOG2E * 128**-0.5)

    def attend(slot, kept, diagonal):
        offs = kv_buf[slot, OFF : OFF + 16, :].astype(F32) * LOG2E
        new_kept = []
        for h in range(3):
            k = kv_buf[slot, pl.ds(KN if h < 2 else KB, 256), :]
            v = kv_buf[slot, pl.ds(VN if h < 2 else VB, 256), :]
            if h < 2:
                v = jnp.where((lane < 64) if h == 0 else (lane >= 64), v, zero)
            scores = lax.dot_general(queries[h], k, (((1,), (1,)), ((), ())), preferred_element_type=F32)
            off = jnp.concatenate([offs[2 * h : 2 * h + 1], offs[2 * h + 1 : 2 * h + 2]], axis=1)
            scores = scores * scales[h] + off
            drop = jnp.maximum(scores, 0.0) + jnp.log2(1.0 + jnp.exp2(-jnp.abs(scores)))
            if diagonal:
                drop = jnp.where(earlier < later, drop, 0.0)
            high = drop.astype(BF16)
            low = (drop - high.astype(F32)).astype(BF16)
            gone = jnp.dot(high, tri_buf[...], preferred_element_type=F32) + jnp.dot(
                low, tri_buf[...], preferred_element_type=F32
            )
            weight = jnp.exp2(scores - gone - kept[h])
            if diagonal:
                weight = jnp.where(earlier < later, weight, 0.0)
            mixed = jnp.dot(weight.astype(BF16), v, preferred_element_type=F32)
            acc_buf[0 if h < 2 else 1] += mixed
            new_kept.append(kept[h] + gone[:, 0:1])
        return tuple(new_kept)

    kept = attend(s, (jnp.zeros((256, 1), F32),) * 3, True)
    lax.fori_loop(0, s, lambda k, kept: attend(s - 1 - k, kept, False), kept)

    for copy in loads[8:]:
        copy.wait()

    def project(a, w, columns, width):
        return jnp.dot(a, w, preferred_element_type=F32)

    def row_block(yy, core):
        return pl.ds(pl.multiple_of((yy * 2 + core) * 32, 32), 32)

    def y_at(dy):
        return lax.rem(y + dy + 4, 4)

    def pair_copy(r):
        return pltpu.make_async_remote_copy(
            src_ref=part_buf.at[r, 1 - c], dst_ref=pair_buf.at[r],
            send_sem=y_send.at[r, 0], recv_sem=pair_sem.at[r],
            device_id=neighbour["pair"], device_id_type=MESH,
        )

    def mid_copy(r, k):
        return pltpu.make_async_remote_copy(
            src_ref=mid_out.at[r, k], dst_ref=mid_in.at[r, k],
            send_sem=y_send.at[r, 1 + k], recv_sem=mid_sem.at[r, k],
            device_id=neighbour["y", 1 if k == 0 else -1], device_id_type=MESH,
        )

    def last_copy(r, k):
        return pltpu.make_async_remote_copy(
            src_ref=last_out.at[r, k], dst_ref=last_in.at[r, k],
            send_sem=y_send.at[r, 3 + k], recv_sem=last_sem.at[r, k],
            device_id=neighbour["y", 1 if k == 0 else -1], device_id_type=MESH,
        )

    def store_part(r, value, columns, width):
        blocks = value.reshape(4, 2, 32, width)
        for core in range(2):
            for yy in range(4):
                part_buf[r, core, yy, :, columns] = blocks[yy, core].astype(BF16)

    def pair_step(r):
        pair_copy(r).wait_recv()
        for yy in range(4):
            sum_buf[yy] = part_buf[r, c, yy].astype(F32) + pair_buf[r, yy].astype(F32)
        far = y_at(2)
        mid_out[r, 0] = sum_buf[far, :, 0:1024].astype(BF16)
        mid_out[r, 1] = sum_buf[far, :, 1024:2048].astype(BF16)
        mid_copy(r, 0).start()
        mid_copy(r, 1).start()

    def mid_step(r):
        mid_copy(r, 0).wait_recv()
        last_out[r, 0, :, 0:1024] = (sum_buf[y_at(1), :, 0:1024] + mid_in[r, 0].astype(F32)).astype(BF16)
        last_out[r, 0, :, 1024:2048] = sum_buf[y_at(1), :, 1024:2048].astype(BF16)
        last_copy(r, 0).start()
        mid_copy(r, 1).wait_recv()
        last_out[r, 1, :, 0:1024] = sum_buf[y_at(-1), :, 0:1024].astype(BF16)
        last_out[r, 1, :, 1024:2048] = (sum_buf[y_at(-1), :, 1024:2048] + mid_in[r, 1].astype(F32)).astype(BF16)
        last_copy(r, 1).start()

    def last_step(r):
        last_copy(r, 0).wait_recv()
        last_copy(r, 1).wait_recv()
        return sum_buf[y] + last_in[r, 0].astype(F32) + last_in[r, 1].astype(F32)

    mixed = jnp.concatenate([acc_buf[0], acc_buf[1]], axis=1).astype(BF16)

    @pl.loop(0, 4)
    def _(n):
        columns = pl.ds(pl.multiple_of(n * 512, 512), 512)
        store_part(0, jnp.dot(mixed, outw_buf[:, columns], preferred_element_type=F32), columns, 512)

    pair_copy(0).start()
    pass_on(1, ORDER[:16])
    pair_step(0)
    pass_on(1, ORDER[16:28])
    mid_step(0)
    pass_on(1, ORDER[28:36])
    updated = res_buf[...].astype(F32) + last_step(0)
    upd_buf[...] = updated
    scale = lax.rsqrt(jnp.mean(updated * updated, axis=-1, keepdims=True) + 1e-06)
    norm_buf[t] = (updated * scale * gain_ref[...]).astype(BF16)

    def row_copy(ref, target, k):
        return pltpu.make_async_remote_copy(
            src_ref=ref, dst_ref=ref, send_sem=y_send.at[2, k], recv_sem=row_sem.at[k],
            device_id=neighbour[target], device_id_type=MESH,
        )

    here = norm_buf.at[t]
    up_one = norm_buf.at[y_at(-1) * 2 + c]
    down_one = norm_buf.at[y_at(1) * 2 + c]
    far_top = norm_buf.at[y_at(2) * 2 + c, pl.ds(0, 16)]
    far_low = norm_buf.at[y_at(2) * 2 + c, pl.ds(16, 16)]
    first = [row_copy(here, ("y", 1), 0), row_copy(here, ("y", -1), 1), row_copy(here, "pair", 2)]
    for copy in first:
        copy.start()
    pass_on(1, ORDER[36:46])

    def row_wait(ref, k):
        pltpu.make_async_copy(ref, ref, row_sem.at[k]).wait()

    sent = list(first)

    def forward(ref, target, k):
        copy = row_copy(ref, target, k)
        copy.start()
        sent.append(copy)

    row_wait(up_one, 0)
    forward(norm_buf.at[y_at(-1) * 2 + c, pl.ds(0, 16)], ("y", 1), 3)
    forward(up_one, "pair", 5)
    row_wait(down_one, 1)
    forward(norm_buf.at[y_at(1) * 2 + c, pl.ds(16, 16)], ("y", -1), 4)
    forward(down_one, "pair", 6)
    pass_on(1, ORDER[46:60])
    row_wait(far_top, 3)
    forward(far_top, "pair", 7)
    row_wait(far_low, 4)
    forward(far_low, "pair", 8)
    pass_on(2, ORDER[:16])
    other = 1 - c
    row_wait(norm_buf.at[y * 2 + other], 2)
    row_wait(norm_buf.at[y_at(-1) * 2 + other], 5)
    row_wait(norm_buf.at[y_at(1) * 2 + other], 6)
    row_wait(norm_buf.at[y_at(2) * 2 + other, pl.ds(0, 16)], 7)
    row_wait(norm_buf.at[y_at(2) * 2 + other, pl.ds(16, 16)], 8)

    @pl.loop(0, 4)
    def _(n):
        columns = pl.ds(pl.multiple_of(n * 256, 256), 256)
        rows = norm_buf[...].reshape(256, 2048)
        pre = jnp.maximum(jnp.dot(rows, up_buf[:, columns], preferred_element_type=F32), 0.0)
        hidden_buf[:, columns] = (pre * pre).astype(BF16)

    pass_on(2, ORDER[16:])

    @pl.loop(0, 8)
    def _(n):
        w = jnp.concatenate([down_buf[2 * n], down_buf[2 * n + 1]], axis=1)
        value = jnp.dot(hidden_buf[...], w, preferred_element_type=F32)
        store_part(1, value, pl.ds(pl.multiple_of(n * 256, 256), 256), 256)

    pair_copy(1).start()
    pair_step(1)
    mid_step(1)
    out_ref[...] = (upd_buf[...] + last_step(1)).astype(BF16)

    for r in range(2):
        pair_copy(r).wait_send()
        for k in range(2):
            mid_copy(r, k).wait_send()
            last_copy(r, k).wait_send()
    for copy in sent:
        copy.wait_send()
    for g, ref in enumerate((kv_buf.at[pl.ds(0, 15)], up_buf.at[pl.ds(0, 1920)], down_buf.at[pl.ds(0, 15)])):
        pltpu.make_async_copy(ref, ref, send_sem.at[g]).wait()


def local(qn, kn, vn, qb, kb, vb, offn, offb, res, on, ob, gain, up, down):
    hbm = pl.BlockSpec(memory_space=pl.ANY)
    vmem = pl.BlockSpec(memory_space=pltpu.VMEM)
    dma = pltpu.SemaphoreType.DMA
    return pl.pallas_call(
        body,
        out_shape=jax.ShapeDtypeStruct((32, 2048), BF16),
        in_specs=[hbm, hbm, hbm, hbm, hbm, hbm, vmem, vmem, hbm, hbm, hbm, vmem, hbm, hbm],
        out_specs=vmem,
        scratch_shapes=[
            pltpu.VMEM((16, KV_ROWS, 128), BF16),
            pltpu.VMEM((2048, 1024), BF16),
            pltpu.VMEM((16, 1024, 128), BF16),
            pltpu.VMEM((2, 256, 128), BF16),
            pltpu.VMEM((32, 2048), BF16),
            pltpu.VMEM((256, 2048), BF16),
            pltpu.VMEM((256, 256), BF16),
            pltpu.VMEM((2, 256, 128), F32),
            pltpu.VMEM((2, 2, 4, 32, 2048), BF16),
            pltpu.VMEM((2, 4, 32, 2048), BF16),
            pltpu.VMEM((4, 32, 2048), F32),
            pltpu.VMEM((2, 2, 32, 1024), BF16),
            pltpu.VMEM((2, 2, 32, 1024), BF16),
            pltpu.VMEM((2, 2, 32, 2048), BF16),
            pltpu.VMEM((2, 2, 32, 2048), BF16),
            pltpu.VMEM((32, 2048), F32),
            pltpu.VMEM((8, 32, 2048), BF16),
            pltpu.VMEM((256, 1024), BF16),
            dma((11,)),
            dma((3, 4, 16)),
            dma((3,)),
            dma((2,)),
            dma((2, 2)),
            dma((2, 2)),
            dma((9,)),
            dma((3, 9)),
        ],
        compiler_params=pltpu.CompilerParams(
            collective_id=0, has_side_effects=True, vmem_limit_bytes=60 * 1024 * 1024
        ),
    )(qn, kn, vn, qb, kb, vb, offn, offb, res, on, ob, gain.reshape(1, 2048), up, down)


def solution(mesh):
    return jax.shard_map(
        local,
        mesh=mesh,
        in_specs=(
            P("sp", "tp"), P("sp", "tp"), P("sp", "tp"), P("sp", "tp"), P("sp", "tp"), P("sp", "tp"),
            P("tp", "sp"), P("tp", "sp"), P(("sp", "tp"), None), P("tp", None), P("tp", None), P(),
            P("sp", "tp"), P("tp", "sp"),
        ),
        out_specs=P(("sp", "tp"), None),
        check_vma=False,
    )
```

```python
import functools
import heapq

import jax
import jax.numpy as jnp
from jax import lax
from jax.experimental import pallas as pl
from jax.experimental.pallas import tpu as pltpu
from jax.sharding import PartitionSpec as P

MESH = pl.DeviceIdType.MESH
LOG2E = 1.4426950408889634
F32 = jnp.float32
BF16 = jnp.bfloat16

KN, OFF, VN, KB, VB, KV_ROWS = 0, 256, 272, 528, 784, 1040
KV_PARTS = ((KN, 272), (VN, 256), (KB, 256), (VB, 256))


def children(q, dx, dz):
    first, second = (dx, dz) if q < 2 else (dz, dx)
    a, b = ("x", "z") if q < 2 else ("z", "x")
    odd = q % 2
    out = []

    def node(f, s):
        return (f, s) if q < 2 else (s, f)

    if second == 0:
        if first == 0:
            out += [(a, 1, *node(1, 0)), (a, -1, *node(3, 0))]
        elif first == 1 and odd == 0:
            out += [(a, 1, *node(2, 0))]
        elif first == 3 and odd == 1:
            out += [(a, -1, *node(2, 0))]
    if second == 0:
        out += [(b, 1, *node(first, 1)), (b, -1, *node(first, 3))]
    elif second == 1 and odd == 0:
        out += [(b, 1, *node(first, 2))]
    elif second == 3 and odd == 1:
        out += [(b, -1, *node(first, 2))]
    return out


def own_sends():
    firsts, rest = [], []
    for q in range(4):
        a = "x" if q < 2 else "z"
        for child in children(q, 0, 0):
            (firsts if child[0] == a else rest).append((q, *child))
    return firsts + rest


def arrivals():
    free = {}
    queue = []

    def send(now, q, axis, step, dx, dz):
        start = max(now, free.get((axis, step), 0.0))
        free[axis, step] = start + 1.4
        heapq.heappush(queue, (start + 1.4 + 1.7, q, dx, dz))

    for entry in own_sends():
        send(0.0, *entry)
    order = []
    while queue:
        now, q, dx, dz = heapq.heappop(queue)
        order.append((q, dx, dz))
        for child in children(q, dx, dz):
            send(now, q, *child)
    return order


ORDER = arrivals()


def after_rows(rows):
    return 1 + max(i for i, (q, dx, dz) in enumerate(ORDER) if dz in rows)


ROW0, ROW1 = after_rows((0,)), after_rows((0, 1))
N1, N2, N3, N4 = 8, 16, 24, 36
FIRST = [e for e in ORDER if e[1:] in ((0, 1), (0, 3), (1, 0), (3, 0))]
REST = [e for e in ORDER if e not in FIRST]


def body(
    qn_hbm, kn_hbm, vn_hbm, qb_hbm, kb_hbm, vb_hbm, offn_ref, offb_ref, res_hbm,
    on_hbm, ob_hbm, gain_ref, up_hbm, down_hbm, out_ref,
    kv_buf, up_buf, down_buf, q_buf, head_buf, kept_buf, res_buf, outw_buf, tri_buf, acc_buf,
    part_buf, pair_buf, sum_buf, mid_in, mid_out, last_out, last_in,
    upd_buf, norm_buf, hidden_buf,
    load_sem, recv_sem, send_sem, pair_sem, mid_sem, last_sem, row_sem, row_send, y_send,
):
    s = lax.axis_index("sp")
    t = lax.axis_index("tp")
    x, z = lax.rem(s, 4), lax.div(s, 4)
    c, y = lax.rem(t, 2), lax.div(t, 2)

    def xz(dx, dz):
        return lax.rem(z + dz + 4, 4) * 4 + lax.rem(x + dx + 4, 4)

    def at_tp(dy):
        return lax.rem(y + dy + 4, 4) * 2 + c

    neighbour = {
        ("x", 1): {"sp": xz(1, 0), "tp": t},
        ("x", -1): {"sp": xz(-1, 0), "tp": t},
        ("z", 1): {"sp": xz(0, 1), "tp": t},
        ("z", -1): {"sp": xz(0, -1), "tp": t},
        "pair": {"sp": s, "tp": y * 2 + (1 - c)},
        ("y", 1): {"sp": s, "tp": at_tp(1)},
        ("y", -1): {"sp": s, "tp": at_tp(-1)},
    }

    own = pl.multiple_of(s * 128, 128)
    loads = [
        (kn_hbm, kv_buf.at[s, pl.ds(KN, 256)]),
        (vn_hbm, kv_buf.at[s, pl.ds(VN, 256)]),
        (kb_hbm, kv_buf.at[s, pl.ds(KB, 256)]),
        (vb_hbm, kv_buf.at[s, pl.ds(VB, 256)]),
        (up_hbm, up_buf.at[pl.ds(own, 128)]),
        (down_hbm, down_buf.at[s]),
        (qn_hbm, q_buf.at[0]),
        (qb_hbm, q_buf.at[1]),
        (on_hbm, outw_buf.at[pl.ds(0, 128)]),
        (ob_hbm, outw_buf.at[pl.ds(128, 128)]),
        (res_hbm, res_buf),
    ]
    loads = [pltpu.make_async_copy(a, b, load_sem.at[k]) for k, (a, b) in enumerate(loads)]
    for copy in loads:
        copy.start()

    barrier = pltpu.get_barrier_semaphore()
    for target in neighbour.values():
        pl.semaphore_signal(barrier, inc=1, device_id=target, device_id_type=MESH)

    offsets = [offn_ref[0:1, :], offn_ref[1:2, :], offb_ref[0:1, :]]
    rows = []
    for line in offsets:
        wide = line.astype(F32)
        rows += [wide[:, :128], wide[:, 128:]]
    rows.append(jnp.zeros((10, 128), F32))
    kv_buf[s, OFF : OFF + 16, :] = jnp.concatenate(rows, axis=0).astype(BF16)
    later = lax.broadcasted_iota(jnp.int32, (256, 256), 0)
    earlier = lax.broadcasted_iota(jnp.int32, (256, 256), 1)
    tri_buf[...] = jnp.where(later >= earlier, 1.0, 0.0).astype(BF16)
    pl.semaphore_wait(barrier, 7)

    def piece(g, slot, q):
        if g == 0:
            start, size = KV_PARTS[q]
            return kv_buf.at[slot, pl.ds(start, size)]
        if g == 1:
            return up_buf.at[pl.ds(pl.multiple_of(slot * 128 + q * 32, 32), 32)]
        return down_buf.at[slot, pl.ds(q * 256, 256)]

    def send(g, slot, q, axis, step, dx, dz):
        ref = piece(g, slot, q)
        pltpu.make_async_remote_copy(
            src_ref=ref, dst_ref=ref, send_sem=send_sem.at[g],
            recv_sem=recv_sem.at[g, q, dz * 4 + dx],
            device_id=neighbour[axis, step], device_id_type=MESH,
        ).start()

    def start_gather(g):
        for entry in own_sends():
            send(g, s, *entry)

    def pass_on(g, events):
        for q, dx, dz in events:
            slot = xz(-dx, -dz)
            ref = piece(g, slot, q)
            pltpu.make_async_copy(ref, ref, recv_sem.at[g, q, dz * 4 + dx]).wait()
            for child in children(q, dx, dz):
                send(g, slot, q, *child)

    for copy in loads[:4]:
        copy.wait()
    start_gather(0)
    for copy in loads[4:8]:
        copy.wait()
    lane = lax.broadcasted_iota(jnp.int32, (256, 128), 1)
    zero = jnp.zeros((), BF16)
    acc_buf[...] = jnp.zeros_like(acc_buf)
    kept_buf[...] = jnp.zeros_like(kept_buf)
    head_buf[0] = jnp.where(lane < 64, q_buf[0], zero)
    head_buf[1] = jnp.where(lane >= 64, q_buf[0], zero)
    head_buf[2] = q_buf[1]
    scales = (LOG2E * 64**-0.5, LOG2E * 64**-0.5, LOG2E * 128**-0.5)

    def attend(slot, diagonal=False):
        offs = kv_buf[slot, OFF : OFF + 16, :].astype(F32) * LOG2E
        scores, gone, out = [], [], [[], []]
        for h in range(3):
            k = kv_buf[slot, pl.ds(KN if h < 2 else KB, 256), :]
            product = lax.dot_general(head_buf[h], k, (((1,), (1,)), ((), ())), preferred_element_type=F32)
            off = jnp.concatenate([offs[2 * h : 2 * h + 1], offs[2 * h + 1 : 2 * h + 2]], axis=1)
            scores.append(product * scales[h] + off)
        for h in range(3):
            drop = jnp.maximum(scores[h], lax.log2(1.0 + lax.exp2(jnp.minimum(scores[h], 126.0))))
            if diagonal:
                drop = jnp.where(earlier < later, drop, 0.0)
            gone.append(jnp.dot(drop.astype(BF16), tri_buf[...], preferred_element_type=F32))
        for h in range(3):
            kept = kept_buf[h]
            weight = lax.exp2(scores[h] - gone[h] - jnp.concatenate([kept, kept], axis=1))
            if diagonal:
                weight = jnp.where(earlier < later, weight, 0.0)
            kept_buf[h] = kept + jnp.broadcast_to(gone[h][:, 0:1], (256, 128))
            v = kv_buf[slot, pl.ds(VN if h < 2 else VB, 256), :]
            if h < 2:
                v = jnp.where((lane < 64) if h == 0 else (lane >= 64), v, zero)
            out[h // 2].append((weight.astype(BF16), v))
        for g in range(2):
            total = acc_buf[g]
            for weight, v in out[g]:
                total = total + jnp.dot(weight, v, preferred_element_type=F32)
            acc_buf[g] = total

    attend(s, True)
    pass_on(0, ORDER[:ROW0])
    pl.loop(0, x)(lambda k: attend(s - 1 - k))
    pass_on(0, ORDER[ROW0:ROW1])
    start_gather(1)
    pl.loop(0, jnp.minimum(z, 1) * 4)(lambda k: attend(z * 4 - 1 - k))
    pass_on(0, ORDER[ROW1:])
    start_gather(2)
    pl.loop(0, jnp.maximum(z - 1, 0) * 4)(lambda k: attend(z * 4 - 5 - k))
    pass_on(1, FIRST)

    for copy in loads[8:]:
        copy.wait()

    def project(a, w, columns, width):
        return jnp.dot(a, w, preferred_element_type=F32)

    def row_block(yy, core):
        return pl.ds(pl.multiple_of((yy * 2 + core) * 32, 32), 32)

    def y_at(dy):
        return lax.rem(y + dy + 4, 4)

    widths = (2048, 512, 512, 512, 512)
    starts = (0, 2048, 2560, 3072, 3584)

    def cols(r, lo=0, hi=None):
        hi = widths[r] if hi is None else hi
        return pl.ds(starts[r] + lo, hi - lo)

    def half_cols(r, k=0):
        return pl.ds(starts[r] // 2, widths[r] // 2)

    def pair_copy(r):
        return pltpu.make_async_remote_copy(
            src_ref=part_buf.at[1 - c, :, :, cols(r)], dst_ref=pair_buf.at[:, :, cols(r)],
            send_sem=y_send.at[r, 0], recv_sem=pair_sem.at[r],
            device_id=neighbour["pair"], device_id_type=MESH,
        )

    def mid_copy(r, k):
        return pltpu.make_async_remote_copy(
            src_ref=mid_out.at[k, :, half_cols(r)], dst_ref=mid_in.at[k, :, half_cols(r)],
            send_sem=y_send.at[r, 1 + k], recv_sem=mid_sem.at[r, k],
            device_id=neighbour["y", 1 if k == 0 else -1], device_id_type=MESH,
        )

    def last_copy(r, k):
        return pltpu.make_async_remote_copy(
            src_ref=last_out.at[k, :, cols(r)], dst_ref=last_in.at[k, :, cols(r)],
            send_sem=y_send.at[r, 3 + k], recv_sem=last_sem.at[r, k],
            device_id=neighbour["y", 1 if k == 0 else -1], device_id_type=MESH,
        )

    def store_part(value, columns, width):
        blocks = value.reshape(4, 2, 32, width)
        for core in range(2):
            for yy in range(4):
                part_buf[core, yy, :, columns] = blocks[yy, core].astype(BF16)

    def pair_step(r):
        pair_copy(r).wait_recv()
        half = widths[r] // 2
        for yy in range(4):
            sum_buf[yy, :, cols(r)] = (
                part_buf[c, yy, :, cols(r)].astype(F32) + pair_buf[yy, :, cols(r)].astype(F32)
            )
        far = y_at(2)
        mid_out[0, :, half_cols(r)] = sum_buf[far, :, cols(r, 0, half)].astype(BF16)
        mid_out[1, :, half_cols(r)] = sum_buf[far, :, cols(r, half)].astype(BF16)
        mid_copy(r, 0).start()
        mid_copy(r, 1).start()

    def mid_step(r):
        half = widths[r] // 2
        for k, dy in ((0, 1), (1, -1)):
            to = y_at(dy)
            mid_copy(r, k).wait_recv()
            left = sum_buf[to, :, cols(r, 0, half)]
            right = sum_buf[to, :, cols(r, half)]
            passing = mid_in[k, :, half_cols(r)].astype(F32)
            left, right = (left + passing, right) if k == 0 else (left, right + passing)
            last_out[k, :, cols(r, 0, half)] = left.astype(BF16)
            last_out[k, :, cols(r, half)] = right.astype(BF16)
            last_copy(r, k).start()

    def last_step(r):
        last_copy(r, 0).wait_recv()
        last_copy(r, 1).wait_recv()
        return (
            sum_buf[y, :, cols(r)] + last_in[0, :, cols(r)].astype(F32) + last_in[1, :, cols(r)].astype(F32)
        )

    mixed = jnp.concatenate([acc_buf[0], acc_buf[1]], axis=1).astype(BF16)

    @pl.loop(0, 4)
    def _(n):
        columns = pl.ds(pl.multiple_of(n * 512, 512), 512)
        store_part(jnp.dot(mixed, outw_buf[:, columns], preferred_element_type=F32), columns, 512)

    pair_copy(0).start()
    pass_on(2, FIRST[:8])
    pair_step(0)
    pass_on(1, REST[:N1])
    mid_step(0)
    pass_on(1, REST[N1:N2])
    updated = res_buf[...].astype(F32) + last_step(0)
    upd_buf[...] = updated
    scale = lax.rsqrt(jnp.mean(updated * updated, axis=-1, keepdims=True) + 1e-06)
    norm_buf[t] = (updated * scale * gain_ref[...]).astype(BF16)

    def row_copy(ref, target, k):
        return pltpu.make_async_remote_copy(
            src_ref=ref, dst_ref=ref, send_sem=row_send.at[k], recv_sem=row_sem.at[k],
            device_id=neighbour[target], device_id_type=MESH,
        )

    here = norm_buf.at[t]
    up_one = norm_buf.at[y_at(-1) * 2 + c]
    down_one = norm_buf.at[y_at(1) * 2 + c]
    far_top = norm_buf.at[y_at(2) * 2 + c, pl.ds(0, 16)]
    far_low = norm_buf.at[y_at(2) * 2 + c, pl.ds(16, 16)]
    first = [row_copy(here, ("y", 1), 0), row_copy(here, ("y", -1), 1), row_copy(here, "pair", 2)]
    for copy in first:
        copy.start()
    pass_on(1, REST[N2:N3])

    def row_wait(ref, k):
        pltpu.make_async_copy(ref, ref, row_sem.at[k]).wait()

    sent = list(first)

    def forward(ref, target, k):
        copy = row_copy(ref, target, k)
        copy.start()
        sent.append(copy)

    row_wait(up_one, 0)
    forward(norm_buf.at[y_at(-1) * 2 + c, pl.ds(0, 16)], ("y", 1), 3)
    forward(up_one, "pair", 5)
    row_wait(down_one, 1)
    forward(norm_buf.at[y_at(1) * 2 + c, pl.ds(16, 16)], ("y", -1), 4)
    forward(down_one, "pair", 6)
    pass_on(1, REST[N3:N4])
    pass_on(2, FIRST[8:])
    row_wait(far_top, 3)
    forward(far_top, "pair", 7)
    row_wait(far_low, 4)
    forward(far_low, "pair", 8)
    pass_on(1, REST[N4:])
    other = 1 - c
    row_wait(norm_buf.at[y * 2 + other], 2)
    row_wait(norm_buf.at[y_at(-1) * 2 + other], 5)
    row_wait(norm_buf.at[y_at(1) * 2 + other], 6)
    row_wait(norm_buf.at[y_at(2) * 2 + other, pl.ds(0, 16)], 7)
    row_wait(norm_buf.at[y_at(2) * 2 + other, pl.ds(16, 16)], 8)

    @pl.loop(0, 4)
    def _(n):
        columns = pl.ds(pl.multiple_of(n * 256, 256), 256)
        rows = norm_buf[...].reshape(256, 2048)
        pre = jnp.maximum(jnp.dot(rows, up_buf[:, columns], preferred_element_type=F32), 0.0)
        hidden_buf[:, columns] = (pre * pre).astype(BF16)

    def mixer_sums(r, dz):
        zz = lax.rem(z - dz + 4, 4)
        for pair in range(2):
            slot = zz * 4 + pair * 2
            w = jnp.concatenate([down_buf[slot], down_buf[slot + 1]], axis=1)
            value = jnp.dot(hidden_buf[...], w, preferred_element_type=F32)
            store_part(value, pl.ds(starts[r] + pair * 256, 256), 256)
        pair_copy(r).start()

    def finish(r, dz):
        columns = pl.ds(pl.multiple_of(lax.rem(z - dz + 4, 4) * 512, 512), 512)
        out_ref[:, columns] = (upd_buf[:, columns] + last_step(r)).astype(BF16)

    done = 0
    rounds = ((1, 0), (2, 1), (3, 3), (4, 2))
    rest_down = REST
    for i, (r, dz) in enumerate(rounds):
        need = 1 + max(k for k, e in enumerate(rest_down) if e[2] == dz)
        if need > done:
            pass_on(2, rest_down[done:need])
            done = need
        mixer_sums(r, dz)
        if i >= 1:
            pair_step(r - 1)
        if i >= 2:
            mid_step(r - 2)
        if i >= 3:
            finish(*rounds[i - 3])
    pair_step(4)
    mid_step(3)
    finish(*rounds[1])
    mid_step(4)
    finish(*rounds[2])
    finish(*rounds[3])

    for r in range(5):
        pair_copy(r).wait_send()
        for k in range(2):
            mid_copy(r, k).wait_send()
            last_copy(r, k).wait_send()
    for copy in sent:
        copy.wait_send()
    for g, ref in enumerate((kv_buf.at[pl.ds(0, 15)], up_buf.at[pl.ds(0, 1920)], down_buf.at[pl.ds(0, 15)])):
        pltpu.make_async_copy(ref, ref, send_sem.at[g]).wait()


def local(qn, kn, vn, qb, kb, vb, offn, offb, res, on, ob, gain, up, down):
    hbm = pl.BlockSpec(memory_space=pl.ANY)
    vmem = pl.BlockSpec(memory_space=pltpu.VMEM)
    dma = pltpu.SemaphoreType.DMA
    return pl.pallas_call(
        body,
        out_shape=jax.ShapeDtypeStruct((32, 2048), BF16),
        in_specs=[hbm, hbm, hbm, hbm, hbm, hbm, vmem, vmem, hbm, hbm, hbm, vmem, hbm, hbm],
        out_specs=vmem,
        scratch_shapes=[
            pltpu.VMEM((16, KV_ROWS, 128), BF16),
            pltpu.VMEM((2048, 1024), BF16),
            pltpu.VMEM((16, 1024, 128), BF16),
            pltpu.VMEM((2, 256, 128), BF16),
            pltpu.VMEM((3, 256, 128), BF16),
            pltpu.VMEM((3, 256, 128), F32),
            pltpu.VMEM((32, 2048), BF16),
            pltpu.VMEM((256, 2048), BF16),
            pltpu.VMEM((256, 256), BF16),
            pltpu.VMEM((2, 256, 128), F32),
            pltpu.VMEM((2, 4, 32, 4096), BF16),
            pltpu.VMEM((4, 32, 4096), BF16),
            pltpu.VMEM((4, 32, 4096), F32),
            pltpu.VMEM((2, 32, 2048), BF16),
            pltpu.VMEM((2, 32, 2048), BF16),
            pltpu.VMEM((2, 32, 4096), BF16),
            pltpu.VMEM((2, 32, 4096), BF16),
            pltpu.VMEM((32, 2048), F32),
            pltpu.VMEM((8, 32, 2048), BF16),
            pltpu.VMEM((256, 1024), BF16),
            dma((11,)),
            dma((3, 4, 16)),
            dma((3,)),
            dma((5,)),
            dma((5, 2)),
            dma((5, 2)),
            dma((9,)),
            dma((9,)),
            dma((5, 5)),
        ],
        compiler_params=pltpu.CompilerParams(
            collective_id=0, has_side_effects=True, vmem_limit_bytes=60 * 1024 * 1024
        ),
    )(qn, kn, vn, qb, kb, vb, offn, offb, res, on, ob, gain.reshape(1, 2048), up, down)


def solution(mesh):
    return jax.shard_map(
        local,
        mesh=mesh,
        in_specs=(
            P("sp", "tp"), P("sp", "tp"), P("sp", "tp"), P("sp", "tp"), P("sp", "tp"), P("sp", "tp"),
            P("tp", "sp"), P("tp", "sp"), P(("sp", "tp"), None), P("tp", None), P("tp", None), P(),
            P("sp", "tp"), P("tp", "sp"),
        ),
        out_specs=P(("sp", "tp"), None),
        check_vma=False,
    )
```

```python
import functools

import jax
import jax.numpy as jnp
from jax import lax
from jax.experimental import pallas as pl
from jax.experimental.pallas import tpu as pltpu
from jax.sharding import PartitionSpec as P

MESH = pl.DeviceIdType.MESH
LOG2E = 1.4426950408889634
F32 = jnp.float32
BF16 = jnp.bfloat16

OFF, VAL, KV_ROWS = 256, 272, 528


def children(q, dx, dz):
    first, second = (dx, dz) if q < 2 else (dz, dx)
    a, b = ("x", "z") if q < 2 else ("z", "x")
    odd = q % 2
    out = []

    def node(f, s):
        return (f, s) if q < 2 else (s, f)

    if second == 0:
        if first == 0:
            out += [(a, 1, *node(1, 0)), (a, -1, *node(3, 0))]
        elif first == 1 and odd == 0:
            out += [(a, 1, *node(2, 0))]
        elif first == 3 and odd == 1:
            out += [(a, -1, *node(2, 0))]
    if second == 0:
        out += [(b, 1, *node(first, 1)), (b, -1, *node(first, 3))]
    elif second == 1 and odd == 0:
        out += [(b, 1, *node(first, 2))]
    elif second == 3 and odd == 1:
        out += [(b, -1, *node(first, 2))]
    return out


WIRE, DELAY = 6.0, 2.2
POINTS = (
    ("sides", 2.8, 10.0),
    ("keys1", 12.5, 19.0),
    ("keys2", 17.5, 23.0),
    ("att1", 22.0, 25.5),
    ("att2", 24.5, 26.5),
    ("mix1", 28.3, 33.0),
    ("mix2", 30.0, 36.0),
    ("mix3", 35.0, 41.0),
    ("rows0", 38.5, 43.0),
    ("rows1", 42.0, 46.0),
    ("rows2", 43.5, 50.0),
)
SIZES = ((16, 16, 48, 48), (240, 240, 272, 272))
STARTS = ((0, 16, 32, 80), (0, 240, 480, 752))


def plan():
    free = {(axis, step): 0.0 for axis in "xz" for step in (1, -1)}
    landing, backlog, steps = {}, [], {}
    left = {(g, dz): 12 if dz == 0 else 16 for g in range(2) for dz in range(4)}

    def offer(g, q, child):
        first = (child[0] == "x") == (q < 2)
        backlog.append((g, 0 if first else 1, len(backlog), q, child))

    def issue(now, out, until, axes=("x", "z")):
        for entry in sorted(backlog):
            g, _, _, q, child = entry
            axis, step, dx, dz = child
            if axis in axes and free[axis, step] <= until:
                start = max(now, free[axis, step])
                free[axis, step] = start + WIRE * SIZES[g][q] / sum(SIZES[g])
                landing[g, q, dx, dz] = free[axis, step] + DELAY
                out.append(("send", g, q, child))
                backlog.remove(entry)

    def take(out, event):
        g, q, dx, dz = event
        del landing[event]
        left[g, dz] -= 1
        out.append(("wait", g, q, (dx, dz)))
        for child in children(q, dx, dz):
            offer(g, q, child)

    for g in range(2):
        for q in range(4):
            for child in children(q, 0, 0):
                offer(g, q, child)
    for point, now, until in POINTS:
        out = []
        axes = ("x",) if point in ("sides", "keys1") else ("x", "z")
        for when, event in sorted((when, event) for event, when in landing.items()):
            if when <= now - 0.3:
                take(out, event)
        issue(now, out, until, axes)
        steps[point] = out
    order, out = [], []
    while landing or backlog:
        when, event = min((when, event) for event, when in landing.items())
        now = max(now, when)
        take(out, event)
        issue(now, out, now + 6.0)
        if not any(left[0, dz] for dz in range(4)) and "up" not in steps:
            steps["up"] = out
            out = []
        for dz in range(4):
            if "up" in steps and not left[1, dz] and dz not in order:
                order.append(dz)
                steps["row", dz] = out
                out = []
    return steps, order, now


PLAN, ROW_ORDER, PLAN_END = plan()


def body(
    qn_hbm, kn_hbm, vn_hbm, qb_hbm, kb_hbm, vb_hbm, offn_ref, offb_ref, res_hbm,
    on_hbm, ob_hbm, gain_ref, up_hbm, down_hbm, out_ref,
    stage, kv_buf, up_buf, down_buf, outw, q_own, q_all, head_buf, kept_buf, acc_buf, tri_buf,
    mix_out, mix_all, res_buf, att_buf, ex_out, ex_in, part_buf, pair_buf, sum_buf, mid_in, mid_out, last_out, last_in,
    upd_buf, norm_buf, hidden_buf,
    load_sem, recv_sem, send_sem, x_sem, x_send, z_sem, far_sem, kv_send, kvp_sem, kvf_sem,
    q_sem, q_send, m_sem, m_send, ow_sem, ow_send, owp_sem, owp_send, ex_sem, ex_send,
    pair_sem, mid_sem, last_sem, row_sem, row_send, y_send,
):
    s = lax.axis_index("sp")
    t = lax.axis_index("tp")
    x, z = lax.rem(s, 4), lax.div(s, 4)
    c, y = lax.rem(t, 2), lax.div(t, 2)
    part = z * 2 + c
    primary = lax.rem(x, 2) == c
    y_odd = lax.rem(y, 2)
    y_mate = y + 1 - 2 * y_odd
    same_pair = lax.div(z, 2) == lax.div(y, 2)
    mix_y = jnp.where(same_pair, z, 3 - z)
    mix_block = jnp.where(same_pair, jnp.int32(0), jnp.int32(1))
    holds_own = mix_y == y

    def xz(dx, dz):
        return lax.rem(z + dz % 4, 4) * 4 + lax.rem(x + dx % 4, 4)

    def y_at(dy):
        return lax.rem(y + dy + 4, 4)

    def z_at(dz):
        return lax.rem(z + dz + 4, 4)

    neighbour = {
        ("x", 1): {"sp": xz(1, 0), "tp": t},
        ("x", -1): {"sp": xz(-1, 0), "tp": t},
        ("z", 1): {"sp": xz(0, 1), "tp": t},
        ("z", -1): {"sp": xz(0, -1), "tp": t},
        "pair": {"sp": s, "tp": y * 2 + (1 - c)},
        ("y", 1): {"sp": s, "tp": y_at(1) * 2 + c},
        ("y", -1): {"sp": s, "tp": y_at(-1) * 2 + c},
    }

    def remote(src, dst, send, recv, target):
        return pltpu.make_async_remote_copy(
            src_ref=src, dst_ref=dst, send_sem=send, recv_sem=recv, device_id=target, device_id_type=MESH
        )

    def arrived(ref, sem):
        pltpu.make_async_copy(ref, ref, sem).wait()

    own = pl.multiple_of(s * 128, 128)
    loads = [
        (kn_hbm, stage.at[0, pl.ds(0, 256)]),
        (vn_hbm, stage.at[0, pl.ds(VAL, 256)]),
        (kb_hbm, stage.at[1, pl.ds(0, 256)]),
        (vb_hbm, stage.at[1, pl.ds(VAL, 256)]),
        (qn_hbm, q_own.at[0]),
        (qb_hbm, q_own.at[1]),
        (on_hbm, outw.at[y_odd * 4 + c]),
        (ob_hbm, outw.at[y_odd * 4 + 2 + c]),
        (up_hbm, up_buf.at[pl.ds(own, 128)]),
        (down_hbm, down_buf.at[s]),
        (res_hbm, res_buf),
    ]
    loads = [pltpu.make_async_copy(a, b, load_sem.at[k]) for k, (a, b) in enumerate(loads)]
    for copy in loads:
        copy.start()

    mine = [
        [
            pltpu.make_async_copy(k_hbm, kv_buf.at[s, pl.ds(0, 256)], load_sem.at[11]),
            pltpu.make_async_copy(v_hbm, kv_buf.at[s, pl.ds(VAL, 256)], load_sem.at[12]),
            pltpu.make_async_copy(q_hbm.at[pl.ds(pl.multiple_of(part * 32, 32), 32)], q_all.at[s], load_sem.at[13]),
        ]
        for k_hbm, v_hbm, q_hbm in ((kn_hbm, vn_hbm, qn_hbm), (kb_hbm, vb_hbm, qb_hbm))
    ]
    for unit in range(2):

        @pl.when(x == c + 2 * unit)
        def _():
            for copy in mine[unit]:
                copy.start()

    def greet(target, unless=None):
        def signal():
            pl.semaphore_signal(barrier, inc=1, device_id=target, device_id_type=MESH)

        if unless is None:
            signal()
        else:
            pl.when(jnp.logical_not(unless))(signal)

    barrier = pltpu.get_barrier_semaphore()
    for target in neighbour.values():
        greet(target)
    for dz in range(4):
        for dx in range(4):
            here = (dx, dz) == (0, 0)
            greet({"sp": xz(dx, dz), "tp": y * 2 + lax.rem(x, 2)}, primary if here else None)
    for block, rows_z in enumerate((y, 3 - y)):
        for plane in (y, y_mate):
            for dx in range(4):
                here = dx == 0 and plane is y
                greet(
                    {"sp": rows_z * 4 + lax.rem(x + dx, 4), "tp": plane * 2 + c},
                    rows_z == z if here else None,
                )

    offn = offn_ref[...].astype(F32)
    offb = offb_ref[...].astype(F32)
    blank = jnp.zeros((14, 128), F32)
    narrow_rows = [offn[0:1, :128], offn[0:1, 128:], offn[1:2, :128], offn[1:2, 128:], blank[:12]]
    broad_rows = [offb[0:1, :128], offb[0:1, 128:], blank]
    for unit, rows in enumerate((narrow_rows, broad_rows)):
        value = jnp.concatenate(rows, axis=0).astype(BF16)
        stage[unit, OFF : OFF + 16, :] = value

        @pl.when(x == c + 2 * unit)
        def _():
            kv_buf[s, OFF : OFF + 16, :] = value

    later = lax.broadcasted_iota(jnp.int32, (256, 256), 0)
    earlier = lax.broadcasted_iota(jnp.int32, (256, 256), 1)
    tri_buf[...] = jnp.where(later >= earlier, 1.0, 0.0).astype(BF16)
    one, none = jnp.int32(1), jnp.int32(0)
    pl.semaphore_wait(barrier, 39 - jnp.where(primary, one, none) - jnp.where(holds_own, one, none))

    def piece(g, slot, q):
        if g == 0:
            return up_buf.at[pl.ds(pl.multiple_of(slot * 128 + STARTS[0][q], 16), SIZES[0][q])]
        return down_buf.at[slot, pl.ds(STARTS[1][q], SIZES[1][q])]

    def send(g, slot, q, axis, step, dx, dz):
        ref = piece(g, slot, q)
        remote(ref, ref, send_sem.at[g], recv_sem.at[g, q, dz * 4 + dx], neighbour[axis, step]).start()

    def run(point):
        for kind, g, q, what in PLAN[point]:
            if kind == "send":
                axis, step, dx, dz = what
                here = (dx - step, dz) if axis == "x" else (dx, dz - step)
                send(g, xz(-here[0], -here[1]), q, axis, step, dx, dz)
            else:
                dx, dz = what
                arrived(piece(g, xz(-dx, -dz), q), recv_sem.at[g, q, dz * 4 + dx])

    for copy in loads[:4]:
        copy.wait()

    def x_copy(unit):
        col = c + 2 * unit
        return remote(
            stage.at[unit], kv_buf.at[s], x_send.at[unit], x_sem.at[lax.rem(x - col + 4, 4)],
            {"sp": z * 4 + col, "tp": t},
        )

    for unit in range(2):

        @pl.when(x != c + 2 * unit)
        def _():
            x_copy(unit).start()

    def kv_slot(d, dz):
        return xz(d, -dz)

    def to_column(d):
        ref = kv_buf.at[kv_slot(d, 0)]
        remote(ref, ref, kv_send.at[0], z_sem.at[d, 0], neighbour["z", 1]).start()
        remote(ref, ref, kv_send.at[0], z_sem.at[d, 1], neighbour["z", -1]).start()
        remote(ref, ref, kv_send.at[1], kvp_sem.at[d, 0], neighbour["pair"]).start()

    def from_row(d):
        for k, dz in ((0, 1), (1, 3)):
            slot = kv_slot(d, dz)
            ref = kv_buf.at[slot]
            arrived(ref, z_sem.at[d, k])
            half = kv_buf.at[slot, pl.ds(0, VAL) if k == 0 else pl.ds(VAL, 256)]
            remote(half, half, kv_send.at[0], far_sem.at[d, k], neighbour["z", 1 if k == 0 else -1]).start()
            remote(ref, ref, kv_send.at[1], kvp_sem.at[d, dz], neighbour["pair"]).start()

    def far_half(d, k):
        return kv_buf.at[kv_slot(d, 2), pl.ds(0, VAL) if k == 0 else pl.ds(VAL, 256)]

    def from_far(d):
        for k in range(2):
            half = far_half(d, k)
            arrived(half, far_sem.at[d, k])
            remote(half, half, kv_send.at[1], kvf_sem.at[d, k], neighbour["pair"]).start()

    @pl.when(primary)
    def _():
        for unit in range(2):

            @pl.when(x == c + 2 * unit)
            def _():
                for copy in mine[unit]:
                    copy.wait()

        to_column(0)

    for copy in loads[4:8]:
        copy.wait()

    def q_copy(unit, dz, dc):
        core = c if dc == 0 else 1 - c
        rows = pl.ds(pl.multiple_of((z_at(dz) * 2 + core) * 32, 32), 32)
        return remote(
            q_own.at[unit, rows], q_all.at[s], q_send.at[unit, dz, dc], q_sem.at[s],
            {"sp": z_at(dz) * 4 + c + 2 * unit, "tp": y * 2 + core},
        )

    def each_query(act):
        for unit in range(2):
            for dz in range(4):
                for dc in range(2):
                    if (dz, dc) == (0, 0):
                        pl.when(x != c + 2 * unit)(lambda: act(q_copy(unit, dz, dc)))
                    else:
                        act(q_copy(unit, dz, dc))

    each_query(lambda copy: copy.start())

    def ow(k, foreign, core):
        plane = 1 - y_odd if foreign else y_odd
        return outw.at[plane * 4 + core + 2 * k]

    mate = {"sp": s, "tp": y_mate * 2 + c}

    def ow_copy(k):
        return remote(ow(k, 0, c), ow(k, 0, c), ow_send.at[k], ow_sem.at[k], mate)

    def ow_pair(k, foreign):
        ref = ow(k, foreign, c)
        return remote(ref, ref, owp_send.at[k, foreign], owp_sem.at[k, foreign], neighbour["pair"])

    ow_sent = [ow_copy(0), ow_copy(1), ow_pair(0, 0), ow_pair(1, 0)]
    for copy in ow_sent:
        copy.start()

    def ow_pass(k):
        arrived(ow(k, 1, c), ow_sem.at[k])
        copy = ow_pair(k, 1)
        copy.start()
        ow_sent.append(copy)

    loads[8].wait()
    loads[9].wait()
    for unit in range(2):
        pl.when(x != c + 2 * unit)(lambda: x_copy(unit).wait_send())
    run("sides")

    @pl.when(primary)
    def _():
        for d in (1, 3):
            arrived(kv_buf.at[kv_slot(d, 0)], x_sem.at[d])
            to_column(d)
        from_row(0)
        arrived(kv_buf.at[kv_slot(2, 0)], x_sem.at[2])
        to_column(2)
        from_row(1)
        from_row(3)

    run("keys1")

    @pl.when(primary)
    def _():
        from_row(2)
        for d in (0, 1, 3, 2):
            from_far(d)

    @pl.when(jnp.logical_not(primary))
    def _():
        for d in (0, 1, 3, 2):
            for dz in (0, 1, 3):
                arrived(kv_buf.at[kv_slot(d, dz)], kvp_sem.at[d, dz])
            for k in range(2):
                arrived(far_half(d, k), kvf_sem.at[d, k])

    for slot in range(16):
        pl.when(jnp.logical_not(jnp.logical_and(primary, s == slot)))(
            lambda: arrived(q_all.at[slot], q_sem.at[slot])
        )
    ow_pass(0)
    run("keys2")

    lane = lax.broadcasted_iota(jnp.int32, (512, 128), 1)
    zero = jnp.zeros((), BF16)
    acc_buf[...] = jnp.zeros_like(acc_buf)
    kept_buf[...] = jnp.zeros_like(kept_buf)
    queries = q_all[...].reshape(512, 128)
    ahead = (later // 32) * 256 + lax.rem(later, 32) - earlier + part * 32

    def attend(slot, heads, chunks, scale):
        offs = kv_buf[slot, OFF:VAL, :].astype(F32) * LOG2E
        k = kv_buf[slot, pl.ds(0, 256), :]
        v = kv_buf[slot, pl.ds(VAL, 256), :]
        items = [(chunk, masked, h) for chunk, masked in chunks for h in range(heads)]
        scores, gone, weights = [], [], []
        for chunk, masked, h in items:
            product = lax.dot_general(
                head_buf[h, chunk * 256 : chunk * 256 + 256], k, (((1,), (1,)), ((), ())),
                preferred_element_type=F32,
            )
            off = jnp.concatenate([offs[2 * h : 2 * h + 1], offs[2 * h + 1 : 2 * h + 2]], axis=1)
            scores.append(product * scale + off)
        for (chunk, masked, h), score in zip(items, scores):
            drop = jnp.maximum(score, lax.log2(1.0 + lax.exp2(jnp.minimum(score, 126.0))))
            if masked:
                drop = jnp.where(ahead > slot * 256 - chunk * 2048, drop, 0.0)
            gone.append(jnp.dot(drop.astype(BF16), tri_buf[...], preferred_element_type=F32))
        for (chunk, masked, h), score, lost in zip(items, scores, gone):
            rows = slice(chunk * 256, chunk * 256 + 256)
            kept = kept_buf[h, rows]
            weight = lax.exp2(score - lost - jnp.concatenate([kept, kept], axis=1))
            if masked:
                weight = jnp.where(ahead > slot * 256 - chunk * 2048, weight, 0.0)
            kept_buf[h, rows] = kept + jnp.broadcast_to(lost[:, 0:1], (256, 128))
            weights.append(weight.astype(BF16))
        for chunk, _ in chunks:
            rows = slice(chunk * 256, chunk * 256 + 256)
            total = acc_buf[rows]
            for (other, _, h), weight in zip(items, weights):
                if other == chunk:
                    values = v
                    if heads == 2:
                        values = jnp.where((lane[:256] < 64) if h == 0 else (lane[:256] >= 64), v, zero)
                    total = total + jnp.dot(weight, values, preferred_element_type=F32)
            acc_buf[rows] = total

    def attention(heads, scale):
        if heads == 2:
            head_buf[0] = jnp.where(lane < 64, queries, zero)
            head_buf[1] = jnp.where(lane >= 64, queries, zero)
        else:
            head_buf[0] = queries

    def each_group(act):
        pl.when(x < 2)(lambda: act(2, LOG2E * 64**-0.5))
        pl.when(x >= 2)(lambda: act(1, LOG2E * 128**-0.5))

    def late_keys(heads, scale):
        if heads == 2:
            head_buf[0] = jnp.where(lane < 64, queries, zero)
            head_buf[1] = jnp.where(lane >= 64, queries, zero)
        else:
            head_buf[0] = queries
        pl.loop(0, 8)(lambda k: attend(15 - k, heads, ((1, True),), scale))

    def early_keys(first, heads, scale):
        pl.loop(0, 4)(lambda k: attend(first - k, heads, ((0, True), (1, False)), scale))

    each_group(late_keys)
    run("att1")
    each_group(functools.partial(early_keys, 7))
    run("att2")
    each_group(functools.partial(early_keys, 3))

    mix_out[...] = acc_buf[...].reshape(16, 32, 128).astype(BF16)

    def m_copy(dx, dz):
        return remote(
            mix_out.at[xz(dx, dz)], mix_all.at[mix_block, y_odd * 4 + x], m_send.at[dz, dx],
            m_sem.at[mix_block, y_odd * 4 + x], {"sp": xz(dx, dz), "tp": mix_y * 2 + c},
        )

    def each_mixed(act):
        for dz in range(4):
            for dx in range(4):
                if (dx, dz) == (0, 0):
                    pl.when(jnp.logical_not(holds_own))(lambda: act(m_copy(dx, dz)))
                else:
                    act(m_copy(dx, dz))

    each_mixed(lambda copy: copy.start())

    @pl.when(holds_own)
    def _():
        mix_all[mix_block, y_odd * 4 + x] = mix_out[s]

    run("mix1")
    ow_pass(1)
    run("mix2")
    for block in range(2):
        for unit in range(8):
            from_me = jnp.logical_and(holds_own, jnp.logical_and(mix_block == block, y_odd * 4 + x == unit))
            pl.when(jnp.logical_not(from_me))(
                lambda: arrived(mix_all.at[block, unit], m_sem.at[block, unit])
            )
    for k in range(2):
        for foreign in range(2):
            arrived(ow(k, foreign, 1 - c), owp_sem.at[k, foreign])
    loads[10].wait()

    mixed = jnp.concatenate([mix_all[:, unit].reshape(64, 128) for unit in range(8)], axis=1)

    def ex_copy(n):
        columns = pl.ds(n * 512, 512)
        return remote(
            ex_out.at[:, columns], ex_in.at[:, columns], ex_send.at[n], ex_sem.at[n],
            {"sp": s, "tp": (3 - y) * 2 + c},
        )

    for n in range(4):
        columns = slice(n * 512, n * 512 + 512)
        sums = jnp.dot(mixed, outw[:, :, columns].reshape(1024, 512), preferred_element_type=F32)
        att_buf[:, columns] = sums[:32]
        ex_out[:, columns] = sums[32:].astype(BF16)
        ex_copy(n).start()
    run("mix3")
    for n in range(4):
        ex_copy(n).wait_recv()
    updated = res_buf[...].astype(F32) + (att_buf[...] + ex_in[...].astype(F32))
    upd_buf[...] = updated
    scale = lax.rsqrt(jnp.mean(updated * updated, axis=-1, keepdims=True) + 1e-06)
    norm_buf[t] = (updated * scale * gain_ref[...]).astype(BF16)

    def row_copy(ref, target, k):
        return remote(ref, ref, row_send.at[k], row_sem.at[k], neighbour[target])

    def half_rows(dy, k, core=None):
        slot = y_at(dy) * 2 + (c if core is None else core)
        return norm_buf.at[slot, pl.ds(16 * k, 16)]

    sent = []

    def row_send_to(ref, target, k):
        copy = row_copy(ref, target, k)
        copy.start()
        sent.append(copy)

    row_send_to(half_rows(0, 0), ("y", 1), 0)
    row_send_to(half_rows(0, 1), ("y", -1), 1)
    row_send_to(half_rows(0, 1), ("y", 1), 2)
    row_send_to(half_rows(0, 0), ("y", -1), 3)
    row_send_to(norm_buf.at[t], "pair", 6)
    run("rows0")
    arrived(half_rows(-1, 0), row_sem.at[0])
    row_send_to(half_rows(-1, 0), ("y", 1), 4)
    arrived(half_rows(1, 1), row_sem.at[1])
    row_send_to(half_rows(1, 1), ("y", -1), 5)
    row_send_to(half_rows(-1, 0), "pair", 7)
    row_send_to(half_rows(1, 1), "pair", 8)
    run("rows1")
    arrived(half_rows(-1, 1), row_sem.at[2])
    row_send_to(half_rows(-1, 1), "pair", 9)
    arrived(half_rows(1, 0), row_sem.at[3])
    row_send_to(half_rows(1, 0), "pair", 10)
    run("rows2")
    arrived(half_rows(2, 0), row_sem.at[4])
    row_send_to(half_rows(2, 0), "pair", 11)
    arrived(half_rows(2, 1), row_sem.at[5])
    row_send_to(half_rows(2, 1), "pair", 12)
    other = 1 - c
    arrived(norm_buf.at[y * 2 + other], row_sem.at[6])
    for k, (dy, half) in enumerate(((-1, 0), (1, 1), (-1, 1), (1, 0), (2, 0), (2, 1))):
        arrived(half_rows(dy, half, other), row_sem.at[7 + k])

    run("up")
    @pl.loop(0, 4)
    def _(n):
        columns = pl.ds(pl.multiple_of(n * 256, 256), 256)
        rows = norm_buf[...].reshape(256, 2048)
        pre = jnp.maximum(jnp.dot(rows, up_buf[:, columns], preferred_element_type=F32), 0.0)
        hidden_buf[:, columns] = (pre * pre).astype(BF16)

    widths = (512, 512, 512, 512)
    starts = (0, 512, 1024, 1536)

    def cols(r, lo=0, hi=None):
        hi = widths[r] if hi is None else hi
        return pl.ds(starts[r] + lo, hi - lo)

    def half_cols(r, k=0):
        return pl.ds(starts[r] // 2, widths[r] // 2)

    def pair_copy(r):
        return pltpu.make_async_remote_copy(
            src_ref=part_buf.at[1 - c, :, :, cols(r)], dst_ref=pair_buf.at[:, :, cols(r)],
            send_sem=y_send.at[r, 0], recv_sem=pair_sem.at[r],
            device_id=neighbour["pair"], device_id_type=MESH,
        )

    def mid_copy(r, k):
        return pltpu.make_async_remote_copy(
            src_ref=mid_out.at[k, :, half_cols(r)], dst_ref=mid_in.at[k, :, half_cols(r)],
            send_sem=y_send.at[r, 1 + k], recv_sem=mid_sem.at[r, k],
            device_id=neighbour["y", 1 if k == 0 else -1], device_id_type=MESH,
        )

    def last_copy(r, k):
        return pltpu.make_async_remote_copy(
            src_ref=last_out.at[k, :, cols(r)], dst_ref=last_in.at[k, :, cols(r)],
            send_sem=y_send.at[r, 3 + k], recv_sem=last_sem.at[r, k],
            device_id=neighbour["y", 1 if k == 0 else -1], device_id_type=MESH,
        )

    def store_part(value, columns, width):
        blocks = value.reshape(4, 2, 32, width)
        for core in range(2):
            for yy in range(4):
                part_buf[core, yy, :, columns] = blocks[yy, core].astype(BF16)

    def pair_step(r):
        pair_copy(r).wait_recv()
        half = widths[r] // 2
        for yy in range(4):
            sum_buf[yy, :, cols(r)] = (
                part_buf[c, yy, :, cols(r)].astype(F32) + pair_buf[yy, :, cols(r)].astype(F32)
            )
        far = y_at(2)
        mid_out[0, :, half_cols(r)] = sum_buf[far, :, cols(r, 0, half)].astype(BF16)
        mid_out[1, :, half_cols(r)] = sum_buf[far, :, cols(r, half)].astype(BF16)
        mid_copy(r, 0).start()
        mid_copy(r, 1).start()

    def mid_step(r):
        half = widths[r] // 2
        for k, dy in ((0, 1), (1, -1)):
            to = y_at(dy)
            mid_copy(r, k).wait_recv()
            left = sum_buf[to, :, cols(r, 0, half)]
            right = sum_buf[to, :, cols(r, half)]
            passing = mid_in[k, :, half_cols(r)].astype(F32)
            left, right = (left + passing, right) if k == 0 else (left, right + passing)
            last_out[k, :, cols(r, 0, half)] = left.astype(BF16)
            last_out[k, :, cols(r, half)] = right.astype(BF16)
            last_copy(r, k).start()

    def last_step(r):
        last_copy(r, 0).wait_recv()
        last_copy(r, 1).wait_recv()
        return (
            sum_buf[y, :, cols(r)] + last_in[0, :, cols(r)].astype(F32) + last_in[1, :, cols(r)].astype(F32)
        )

    def mixer_sums(r, dz):
        zz = lax.rem(z - dz + 4, 4)
        for pair in range(2):
            slot = zz * 4 + pair * 2
            w = jnp.concatenate([down_buf[slot], down_buf[slot + 1]], axis=1)
            value = jnp.dot(hidden_buf[...], w, preferred_element_type=F32)
            store_part(value, pl.ds(starts[r] + pair * 256, 256), 256)
        pair_copy(r).start()

    def finish(r, dz):
        columns = pl.ds(pl.multiple_of(lax.rem(z - dz + 4, 4) * 512, 512), 512)
        out_ref[:, columns] = (upd_buf[:, columns] + last_step(r)).astype(BF16)

    rounds = tuple(enumerate(ROW_ORDER))
    for i, (r, dz) in enumerate(rounds):
        run(("row", dz))
        mixer_sums(r, dz)
        if i >= 1:
            pair_step(r - 1)
        if i >= 2:
            mid_step(r - 2)
        if i >= 3:
            finish(*rounds[i - 3])
    pair_step(3)
    mid_step(2)
    finish(*rounds[1])
    mid_step(3)
    finish(*rounds[2])
    finish(*rounds[3])

    for r in range(4):
        pair_copy(r).wait_send()
        for k in range(2):
            mid_copy(r, k).wait_send()
            last_copy(r, k).wait_send()
    for copy in sent + ow_sent + [ex_copy(n) for n in range(4)]:
        copy.wait_send()
    each_query(lambda copy: copy.wait_send())
    each_mixed(lambda copy: copy.wait_send())
    for g, ref in enumerate((up_buf.at[pl.ds(0, 1920)], down_buf.at[pl.ds(0, 15)])):
        arrived(ref, send_sem.at[g])

    @pl.when(primary)
    def _():
        arrived(kv_buf.at[pl.ds(0, 12)], kv_send.at[0])
        arrived(kv_buf, kv_send.at[1])


def local(qn, kn, vn, qb, kb, vb, offn, offb, res, on, ob, gain, up, down):
    hbm = pl.BlockSpec(memory_space=pl.ANY)
    vmem = pl.BlockSpec(memory_space=pltpu.VMEM)
    dma = pltpu.SemaphoreType.DMA
    return pl.pallas_call(
        body,
        out_shape=jax.ShapeDtypeStruct((32, 2048), BF16),
        in_specs=[hbm, hbm, hbm, hbm, hbm, hbm, vmem, vmem, hbm, hbm, hbm, vmem, hbm, hbm],
        out_specs=vmem,
        scratch_shapes=[
            pltpu.VMEM((2, KV_ROWS, 128), BF16),
            pltpu.VMEM((16, KV_ROWS, 128), BF16),
            pltpu.VMEM((2048, 1024), BF16),
            pltpu.VMEM((16, 1024, 128), BF16),
            pltpu.VMEM((8, 128, 2048), BF16),
            pltpu.VMEM((2, 256, 128), BF16),
            pltpu.VMEM((16, 32, 128), BF16),
            pltpu.VMEM((2, 512, 128), BF16),
            pltpu.VMEM((2, 512, 128), F32),
            pltpu.VMEM((512, 128), F32),
            pltpu.VMEM((256, 256), BF16),
            pltpu.VMEM((16, 32, 128), BF16),
            pltpu.VMEM((2, 8, 32, 128), BF16),
            pltpu.VMEM((32, 2048), BF16),
            pltpu.VMEM((32, 2048), F32),
            pltpu.VMEM((32, 2048), BF16),
            pltpu.VMEM((32, 2048), BF16),
            pltpu.VMEM((2, 4, 32, 2048), BF16),
            pltpu.VMEM((4, 32, 2048), BF16),
            pltpu.VMEM((4, 32, 2048), F32),
            pltpu.VMEM((2, 32, 1024), BF16),
            pltpu.VMEM((2, 32, 1024), BF16),
            pltpu.VMEM((2, 32, 2048), BF16),
            pltpu.VMEM((2, 32, 2048), BF16),
            pltpu.VMEM((32, 2048), F32),
            pltpu.VMEM((8, 32, 2048), BF16),
            pltpu.VMEM((256, 1024), BF16),
            dma((14,)),
            dma((2, 4, 16)),
            dma((2,)),
            dma((4,)),
            dma((2,)),
            dma((4, 2)),
            dma((4, 2)),
            dma((2,)),
            dma((4, 4)),
            dma((4, 2)),
            dma((16,)),
            dma((2, 4, 2)),
            dma((2, 8)),
            dma((4, 4)),
            dma((2,)),
            dma((2,)),
            dma((2, 2)),
            dma((2, 2)),
            dma((4,)),
            dma((4,)),
            dma((4,)),
            dma((4, 2)),
            dma((4, 2)),
            dma((13,)),
            dma((13,)),
            dma((4, 5)),
        ],
        compiler_params=pltpu.CompilerParams(
            collective_id=0, has_side_effects=True, vmem_limit_bytes=60 * 1024 * 1024
        ),
    )(qn, kn, vn, qb, kb, vb, offn, offb, res, on, ob, gain.reshape(1, 2048), up, down)


def solution(mesh):
    return jax.shard_map(
        local,
        mesh=mesh,
        in_specs=(
            P("sp", "tp"), P("sp", "tp"), P("sp", "tp"), P("sp", "tp"), P("sp", "tp"), P("sp", "tp"),
            P("tp", "sp"), P("tp", "sp"), P(("sp", "tp"), None), P("tp", None), P("tp", None), P(),
            P("sp", "tp"), P("tp", "sp"),
        ),
        out_specs=P(("sp", "tp"), None),
        check_vma=False,
    )
```

```python
import functools

import jax
import jax.numpy as jnp
from jax import lax
from jax.experimental import pallas as pl
from jax.experimental.pallas import tpu as pltpu
from jax.sharding import PartitionSpec as P

MESH = pl.DeviceIdType.MESH
LOG2E = 1.4426950408889634
F32 = jnp.float32
BF16 = jnp.bfloat16

OFF, VAL, KV_ROWS = 256, 272, 528


def children(q, dx, dz):
    first, second = (dx, dz) if q < 2 else (dz, dx)
    a, b = ("x", "z") if q < 2 else ("z", "x")
    odd = q % 2
    out = []

    def node(f, s):
        return (f, s) if q < 2 else (s, f)

    if second == 0:
        if first == 0:
            out += [(a, 1, *node(1, 0)), (a, -1, *node(3, 0))]
        elif first == 1 and odd == 0:
            out += [(a, 1, *node(2, 0))]
        elif first == 3 and odd == 1:
            out += [(a, -1, *node(2, 0))]
    if second == 0:
        out += [(b, 1, *node(first, 1)), (b, -1, *node(first, 3))]
    elif second == 1 and odd == 0:
        out += [(b, 1, *node(first, 2))]
    elif second == 3 and odd == 1:
        out += [(b, -1, *node(first, 2))]
    return out


WIRE, DELAY = 6.0, 2.2
POINTS = (
    ("sides", 2.8, 10.0),
    ("keys1", 13.5, 18.0),
    ("keys2", 17.0, 20.5),
    ("att1", 20.3, 22.5),
    ("mix1", 24.0, 29.0),
    ("mix2", 26.0, 32.0),
    ("mix3", 31.0, 37.0),
    ("rows0", 34.0, 39.0),
    ("rows1", 37.5, 42.0),
    ("rows2", 39.0, 46.0),
)
SIZES = ((16, 16, 48, 48), (272, 272, 240, 240))
STARTS = ((0, 16, 32, 80), (0, 272, 544, 784))


def plan():
    free = {(axis, step): 0.0 for axis in "xz" for step in (1, -1)}
    landing, backlog, steps = {}, [], {}
    left = {(g, dz): 12 if dz == 0 else 16 for g in range(2) for dz in range(4)}

    def offer(g, q, child):
        first = (child[0] == "x") == (q < 2)
        backlog.append((g, 0 if first else 1, len(backlog), q, child))

    def issue(now, out, until, axes=("x", "z")):
        for entry in sorted(backlog):
            g, _, _, q, child = entry
            axis, step, dx, dz = child
            if axis in axes and free[axis, step] <= until:
                start = max(now, free[axis, step])
                free[axis, step] = start + WIRE * SIZES[g][q] / sum(SIZES[g])
                landing[g, q, dx, dz] = free[axis, step] + DELAY
                out.append(("send", g, q, child))
                backlog.remove(entry)

    def take(out, event):
        g, q, dx, dz = event
        del landing[event]
        left[g, dz] -= 1
        out.append(("wait", g, q, (dx, dz)))
        for child in children(q, dx, dz):
            offer(g, q, child)

    for g in range(2):
        for q in range(4):
            for child in children(q, 0, 0):
                offer(g, q, child)
    for point, now, until in POINTS:
        out = []
        axes = ("x",) if point == "sides" else ("x", "z")
        for when, event in sorted((when, event) for event, when in landing.items()):
            if when <= now - 0.3:
                take(out, event)
        issue(now, out, until, axes)
        steps[point] = out
    order, out = [], []
    while landing or backlog:
        when, event = min((when, event) for event, when in landing.items())
        now = max(now, when)
        take(out, event)
        issue(now, out, now + 6.0)
        if not any(left[0, dz] for dz in range(4)) and "up" not in steps:
            steps["up"] = out
            out = []
        for dz in range(4):
            if "up" in steps and not left[1, dz] and dz not in order:
                order.append(dz)
                steps["row", dz] = out
                out = []
    return steps, order, now


PLAN, ROW_ORDER, PLAN_END = plan()


def body(
    qn_hbm, kn_hbm, vn_hbm, qb_hbm, kb_hbm, vb_hbm, offn_ref, offb_ref, res_hbm,
    on_hbm, ob_hbm, gain_ref, up_hbm, down_hbm, out_ref,
    stage, kv_buf, up_buf, down_buf, outw, q_own, q_all, head_buf, kept_buf, acc_buf, tri_buf,
    mix_out, mix_all, res_buf, att_buf, ex_out, ex_in, part_buf, pair_buf, last_out, last_in,
    upd_buf, norm_buf, hidden_buf,
    load_sem, recv_sem, send_sem, x_sem, x_send, z_sem, far_sem, kv_send, kvp_sem, kvf_sem,
    q_sem, q_send, m_sem, m_send, ow_sem, ow_send, owp_sem, owp_send, ex_sem, ex_send,
    pair_sem, last_sem, row_sem, row_send, y_send,
):
    s = lax.axis_index("sp")
    t = lax.axis_index("tp")
    x, z = lax.rem(s, 4), lax.div(s, 4)
    c, y = lax.rem(t, 2), lax.div(t, 2)
    part = z * 2 + c
    primary = lax.rem(x, 2) == c
    y_odd = lax.rem(y, 2)
    y_mate = y + 1 - 2 * y_odd
    same_pair = lax.div(z, 2) == lax.div(y, 2)
    mix_y = jnp.where(same_pair, z, 3 - z)
    mix_block = jnp.where(same_pair, jnp.int32(0), jnp.int32(1))
    holds_own = mix_y == y

    def xz(dx, dz):
        return lax.rem(z + dz % 4, 4) * 4 + lax.rem(x + dx % 4, 4)

    def y_at(dy):
        return lax.rem(y + dy + 4, 4)

    def z_at(dz):
        return lax.rem(z + dz + 4, 4)

    neighbour = {
        ("x", 1): {"sp": xz(1, 0), "tp": t},
        ("x", -1): {"sp": xz(-1, 0), "tp": t},
        ("z", 1): {"sp": xz(0, 1), "tp": t},
        ("z", -1): {"sp": xz(0, -1), "tp": t},
        "pair": {"sp": s, "tp": y * 2 + (1 - c)},
        ("y", 1): {"sp": s, "tp": y_at(1) * 2 + c},
        ("y", -1): {"sp": s, "tp": y_at(-1) * 2 + c},
        ("y", 2): {"sp": s, "tp": y_at(2) * 2 + c},
    }

    def remote(src, dst, send, recv, target):
        return pltpu.make_async_remote_copy(
            src_ref=src, dst_ref=dst, send_sem=send, recv_sem=recv, device_id=target, device_id_type=MESH
        )

    def arrived(ref, sem):
        pltpu.make_async_copy(ref, ref, sem).wait()

    own = pl.multiple_of(s * 128, 128)
    loads = [
        (kn_hbm, stage.at[0, pl.ds(0, 256)]),
        (vn_hbm, stage.at[0, pl.ds(VAL, 256)]),
        (kb_hbm, stage.at[1, pl.ds(0, 256)]),
        (vb_hbm, stage.at[1, pl.ds(VAL, 256)]),
        (qn_hbm, q_own.at[0]),
        (qb_hbm, q_own.at[1]),
        (on_hbm, outw.at[y_odd * 4 + c]),
        (ob_hbm, outw.at[y_odd * 4 + 2 + c]),
        (up_hbm, up_buf.at[pl.ds(own, 128)]),
        (down_hbm, down_buf.at[s]),
        (res_hbm, res_buf),
    ]
    loads = [pltpu.make_async_copy(a, b, load_sem.at[k]) for k, (a, b) in enumerate(loads)]
    for copy in loads:
        copy.start()

    mine = [
        [
            pltpu.make_async_copy(k_hbm, kv_buf.at[s, pl.ds(0, 256)], load_sem.at[11]),
            pltpu.make_async_copy(v_hbm, kv_buf.at[s, pl.ds(VAL, 256)], load_sem.at[12]),
            pltpu.make_async_copy(q_hbm.at[pl.ds(pl.multiple_of(part * 32, 32), 32)], q_all.at[s], load_sem.at[13]),
        ]
        for k_hbm, v_hbm, q_hbm in ((kn_hbm, vn_hbm, qn_hbm), (kb_hbm, vb_hbm, qb_hbm))
    ]
    for unit in range(2):

        @pl.when(x == c + 2 * unit)
        def _():
            for copy in mine[unit]:
                copy.start()

    def greet(target, unless=None):
        def signal():
            pl.semaphore_signal(barrier, inc=1, device_id=target, device_id_type=MESH)

        if unless is None:
            signal()
        else:
            pl.when(jnp.logical_not(unless))(signal)

    barrier = pltpu.get_barrier_semaphore()
    for target in neighbour.values():
        greet(target)
    for dz in range(4):
        for dx in range(4):
            here = (dx, dz) == (0, 0)
            greet({"sp": xz(dx, dz), "tp": y * 2 + lax.rem(x, 2)}, primary if here else None)
    for block, rows_z in enumerate((y, 3 - y)):
        for plane in (y, y_mate):
            for dx in range(4):
                here = dx == 0 and plane is y
                greet(
                    {"sp": rows_z * 4 + lax.rem(x + dx, 4), "tp": plane * 2 + c},
                    rows_z == z if here else None,
                )

    offn = offn_ref[...].astype(F32)
    offb = offb_ref[...].astype(F32)
    blank = jnp.zeros((14, 128), F32)
    narrow_rows = [offn[0:1, :128], offn[0:1, 128:], offn[1:2, :128], offn[1:2, 128:], blank[:12]]
    broad_rows = [offb[0:1, :128], offb[0:1, 128:], blank]
    for unit, rows in enumerate((narrow_rows, broad_rows)):
        value = jnp.concatenate(rows, axis=0).astype(BF16)
        stage[unit, OFF : OFF + 16, :] = value

        @pl.when(x == c + 2 * unit)
        def _():
            kv_buf[s, OFF : OFF + 16, :] = value

    later = lax.broadcasted_iota(jnp.int32, (256, 256), 0)
    earlier = lax.broadcasted_iota(jnp.int32, (256, 256), 1)
    tri_buf[...] = jnp.where(later >= earlier, 1.0, 0.0).astype(BF16)
    acc_buf[...] = jnp.zeros_like(acc_buf)
    kept_buf[...] = jnp.zeros_like(kept_buf)
    one, none = jnp.int32(1), jnp.int32(0)
    pl.semaphore_wait(barrier, 40 - jnp.where(primary, one, none) - jnp.where(holds_own, one, none))

    def piece(g, slot, q):
        if g == 0:
            return up_buf.at[pl.ds(pl.multiple_of(slot * 128 + STARTS[0][q], 16), SIZES[0][q])]
        return down_buf.at[slot, pl.ds(STARTS[1][q], SIZES[1][q])]

    def send(g, slot, q, axis, step, dx, dz):
        ref = piece(g, slot, q)
        remote(ref, ref, send_sem.at[g], recv_sem.at[g, q, dz * 4 + dx], neighbour[axis, step]).start()

    def run(point):
        for kind, g, q, what in PLAN[point]:
            if kind == "send":
                axis, step, dx, dz = what
                here = (dx - step, dz) if axis == "x" else (dx, dz - step)
                send(g, xz(-here[0], -here[1]), q, axis, step, dx, dz)
            else:
                dx, dz = what
                arrived(piece(g, xz(-dx, -dz), q), recv_sem.at[g, q, dz * 4 + dx])

    for copy in loads[:4]:
        copy.wait()

    def x_copy(unit):
        col = c + 2 * unit
        return remote(
            stage.at[unit], kv_buf.at[s], x_send.at[unit], x_sem.at[lax.rem(x - col + 4, 4)],
            {"sp": z * 4 + col, "tp": t},
        )

    for unit in range(2):

        @pl.when(x != c + 2 * unit)
        def _():
            x_copy(unit).start()

    def kv_slot(d, dz):
        return xz(d, -dz)

    def to_column(d):
        ref = kv_buf.at[kv_slot(d, 0)]
        remote(ref, ref, kv_send.at[0], z_sem.at[d, 0], neighbour["z", 1]).start()
        remote(ref, ref, kv_send.at[0], z_sem.at[d, 1], neighbour["z", -1]).start()
        remote(ref, ref, kv_send.at[1], kvp_sem.at[d, 0], neighbour["pair"]).start()

    def from_row(d):
        for k, dz in ((0, 1), (1, 3)):
            slot = kv_slot(d, dz)
            ref = kv_buf.at[slot]
            arrived(ref, z_sem.at[d, k])
            half = kv_buf.at[slot, pl.ds(0, VAL) if k == 0 else pl.ds(VAL, 256)]
            remote(half, half, kv_send.at[0], far_sem.at[d, k], neighbour["z", 1 if k == 0 else -1]).start()
            remote(ref, ref, kv_send.at[1], kvp_sem.at[d, dz], neighbour["pair"]).start()

    def far_half(d, k):
        return kv_buf.at[kv_slot(d, 2), pl.ds(0, VAL) if k == 0 else pl.ds(VAL, 256)]

    def from_far(d):
        for k in range(2):
            half = far_half(d, k)
            arrived(half, far_sem.at[d, k])
            remote(half, half, kv_send.at[1], kvf_sem.at[d, k], neighbour["pair"]).start()

    @pl.when(primary)
    def _():
        for unit in range(2):

            @pl.when(x == c + 2 * unit)
            def _():
                for copy in mine[unit]:
                    copy.wait()

        to_column(0)

    for copy in loads[4:8]:
        copy.wait()

    def q_copy(unit, dz, dc):
        core = c if dc == 0 else 1 - c
        rows = pl.ds(pl.multiple_of((z_at(dz) * 2 + core) * 32, 32), 32)
        return remote(
            q_own.at[unit, rows], q_all.at[s], q_send.at[unit, dz, dc], q_sem.at[s],
            {"sp": z_at(dz) * 4 + c + 2 * unit, "tp": y * 2 + core},
        )

    def each_query(act):
        for unit in range(2):
            for dz in range(4):
                for dc in range(2):
                    if (dz, dc) == (0, 0):
                        pl.when(x != c + 2 * unit)(lambda: act(q_copy(unit, dz, dc)))
                    else:
                        act(q_copy(unit, dz, dc))

    each_query(lambda copy: copy.start())

    def ow(k, foreign, core):
        plane = 1 - y_odd if foreign else y_odd
        return outw.at[plane * 4 + core + 2 * k]

    mate = {"sp": s, "tp": y_mate * 2 + c}

    def ow_copy(k):
        return remote(ow(k, 0, c), ow(k, 0, c), ow_send.at[k], ow_sem.at[k], mate)

    def ow_pair(k, foreign):
        ref = ow(k, foreign, c)
        return remote(ref, ref, owp_send.at[k, foreign], owp_sem.at[k, foreign], neighbour["pair"])

    ow_sent = [ow_copy(0), ow_copy(1), ow_pair(0, 0), ow_pair(1, 0)]
    for copy in ow_sent:
        copy.start()

    def ow_pass(k):
        arrived(ow(k, 1, c), ow_sem.at[k])
        copy = ow_pair(k, 1)
        copy.start()
        ow_sent.append(copy)

    loads[8].wait()
    loads[9].wait()
    for unit in range(2):
        pl.when(x != c + 2 * unit)(lambda: x_copy(unit).wait_send())
    run("sides")

    lane = lax.broadcasted_iota(jnp.int32, (512, 128), 1)
    zero = jnp.zeros((), BF16)
    ahead = (later // 32) * 256 + lax.rem(later, 32) - earlier + part * 32

    def attend(slot, zz, heads, chunks, scale):
        offs = kv_buf[slot, OFF:VAL, :].astype(F32) * LOG2E
        k = kv_buf[slot, pl.ds(0, 256), :]
        v = kv_buf[slot, pl.ds(VAL, 256), :]
        items = [(chunk, masked, h) for chunk, masked in chunks for h in range(heads)]
        scores, gone, weights = [], [], []
        for chunk, masked, h in items:
            product = lax.dot_general(
                head_buf[h, chunk * 256 : chunk * 256 + 256], k, (((1,), (1,)), ((), ())),
                preferred_element_type=F32,
            )
            off = jnp.concatenate([offs[2 * h : 2 * h + 1], offs[2 * h + 1 : 2 * h + 2]], axis=1)
            scores.append(product * scale + off)
        for (chunk, masked, h), score in zip(items, scores):
            drop = jnp.maximum(score, lax.log2(1.0 + lax.exp2(jnp.minimum(score, 126.0))))
            if masked:
                drop = jnp.where(ahead > slot * 256 - chunk * 2048, drop, 0.0)
            gone.append(jnp.dot(drop.astype(BF16), tri_buf[...], preferred_element_type=F32))
        for (chunk, masked, h), score, lost in zip(items, scores, gone):
            rows = slice(chunk * 256, chunk * 256 + 256)
            kept = kept_buf[zz, h, rows]
            weight = lax.exp2(score - lost - jnp.concatenate([kept, kept], axis=1))
            if masked:
                weight = jnp.where(ahead > slot * 256 - chunk * 2048, weight, 0.0)
            kept_buf[zz, h, rows] = kept + jnp.broadcast_to(lost[:, 0:1], (256, 128))
            weights.append(weight.astype(BF16))
        for chunk, _ in chunks:
            rows = slice(chunk * 256, chunk * 256 + 256)
            total = acc_buf[zz, rows]
            for (other, _, h), weight in zip(items, weights):
                if other == chunk:
                    values = v
                    if heads == 2:
                        values = jnp.where((lane[:256] < 64) if h == 0 else (lane[:256] >= 64), v, zero)
                    total = total + jnp.dot(weight, values, preferred_element_type=F32)
            acc_buf[zz, rows] = total

    def each_group(act):
        pl.when(x < 2)(lambda: act(2, LOG2E * 64**-0.5))
        pl.when(x >= 2)(lambda: act(1, LOG2E * 128**-0.5))

    def set_heads(heads, scale):
        queries = q_all[...].reshape(512, 128)
        if heads == 2:
            head_buf[0] = jnp.where(lane < 64, queries, zero)
            head_buf[1] = jnp.where(lane >= 64, queries, zero)
        else:
            head_buf[0] = queries

    def attend_row(dz):
        zz = z_at(-dz)

        def act(heads, scale):
            for near, chunks in ((True, ((1, True),)), (False, ((0, True), (1, False)))):

                @pl.when((zz >= 2) if near else (zz < 2))
                def _():
                    pl.loop(0, 4)(lambda k: attend(zz * 4 + 3 - k, zz, heads, chunks, scale))

        each_group(act)

    def join_rows(heads, scale):
        total, past = acc_buf[3], None
        for zz in (2, 1, 0):
            kept = kept_buf[zz + 1, 0]
            if heads == 2:
                kept = jnp.where(lane < 64, kept, kept_buf[zz + 1, 1])
            past = kept if past is None else past + kept
            total = total + acc_buf[zz] * lax.exp2(-past)
        mix_out[...] = total.reshape(16, 32, 128).astype(BF16)

    def secondary_waits(rows):
        @pl.when(jnp.logical_not(primary))
        def _():
            for d in (0, 1, 3, 2):
                for dz in rows:
                    if dz == 2:
                        for k in range(2):
                            arrived(far_half(d, k), kvf_sem.at[d, k])
                    else:
                        arrived(kv_buf.at[kv_slot(d, dz)], kvp_sem.at[d, dz])

    @pl.when(primary)
    def _():
        for d in (1, 3):
            arrived(kv_buf.at[kv_slot(d, 0)], x_sem.at[d])
            to_column(d)
        from_row(0)
        arrived(kv_buf.at[kv_slot(2, 0)], x_sem.at[2])
        to_column(2)

    for slot in range(16):
        pl.when(jnp.logical_not(jnp.logical_and(primary, s == slot)))(
            lambda: arrived(q_all.at[slot], q_sem.at[slot])
        )
    each_group(set_heads)
    secondary_waits((0,))
    attend_row(0)

    @pl.when(primary)
    def _():
        from_row(1)
        from_row(3)
        from_row(2)

    run("keys1")
    secondary_waits((1, 3))
    attend_row(1)
    ow_pass(0)

    @pl.when(primary)
    def _():
        for d in (0, 1, 3, 2):
            from_far(d)

    run("keys2")
    attend_row(3)
    run("att1")
    secondary_waits((2,))
    attend_row(2)
    each_group(join_rows)

    def m_copy(dx, dz):
        return remote(
            mix_out.at[xz(dx, dz)], mix_all.at[mix_block, y_odd * 4 + x], m_send.at[dz, dx],
            m_sem.at[mix_block, y_odd * 4 + x], {"sp": xz(dx, dz), "tp": mix_y * 2 + c},
        )

    def each_mixed(act):
        for dz in range(4):
            for dx in range(4):
                if (dx, dz) == (0, 0):
                    pl.when(jnp.logical_not(holds_own))(lambda: act(m_copy(dx, dz)))
                else:
                    act(m_copy(dx, dz))

    each_mixed(lambda copy: copy.start())

    @pl.when(holds_own)
    def _():
        mix_all[mix_block, y_odd * 4 + x] = mix_out[s]

    run("mix1")
    ow_pass(1)
    run("mix2")
    for block in range(2):
        for unit in range(8):
            from_me = jnp.logical_and(holds_own, jnp.logical_and(mix_block == block, y_odd * 4 + x == unit))
            pl.when(jnp.logical_not(from_me))(
                lambda: arrived(mix_all.at[block, unit], m_sem.at[block, unit])
            )
    for k in range(2):
        for foreign in range(2):
            arrived(ow(k, foreign, 1 - c), owp_sem.at[k, foreign])
    loads[10].wait()

    mixed = jnp.concatenate([mix_all[:, unit].reshape(64, 128) for unit in range(8)], axis=1)

    def ex_copy(n):
        columns = pl.ds(n * 512, 512)
        return remote(
            ex_out.at[:, columns], ex_in.at[:, columns], ex_send.at[n], ex_sem.at[n],
            {"sp": s, "tp": (3 - y) * 2 + c},
        )

    for n in range(4):
        columns = slice(n * 512, n * 512 + 512)
        sums = jnp.dot(mixed, outw[:, :, columns].reshape(1024, 512), preferred_element_type=F32)
        att_buf[:, columns] = sums[:32]
        ex_out[:, columns] = sums[32:].astype(BF16)
        ex_copy(n).start()
    run("mix3")
    for n in range(4):
        ex_copy(n).wait_recv()
    updated = res_buf[...].astype(F32) + (att_buf[...] + ex_in[...].astype(F32))
    upd_buf[...] = updated
    scale = lax.rsqrt(jnp.mean(updated * updated, axis=-1, keepdims=True) + 1e-06)
    norm_buf[t] = (updated * scale * gain_ref[...]).astype(BF16)

    def row_copy(ref, target, k):
        return remote(ref, ref, row_send.at[k], row_sem.at[k], neighbour[target])

    def half_rows(dy, k, core=None):
        slot = y_at(dy) * 2 + (c if core is None else core)
        return norm_buf.at[slot, pl.ds(16 * k, 16)]

    sent = []

    def row_send_to(ref, target, k):
        copy = row_copy(ref, target, k)
        copy.start()
        sent.append(copy)

    row_send_to(half_rows(0, 0), ("y", 1), 0)
    row_send_to(half_rows(0, 1), ("y", -1), 1)
    row_send_to(half_rows(0, 1), ("y", 1), 2)
    row_send_to(half_rows(0, 0), ("y", -1), 3)
    row_send_to(norm_buf.at[t], "pair", 6)
    run("rows0")
    arrived(half_rows(-1, 0), row_sem.at[0])
    row_send_to(half_rows(-1, 0), ("y", 1), 4)
    arrived(half_rows(1, 1), row_sem.at[1])
    row_send_to(half_rows(1, 1), ("y", -1), 5)
    row_send_to(half_rows(-1, 0), "pair", 7)
    row_send_to(half_rows(1, 1), "pair", 8)
    run("rows1")
    arrived(half_rows(-1, 1), row_sem.at[2])
    row_send_to(half_rows(-1, 1), "pair", 9)
    arrived(half_rows(1, 0), row_sem.at[3])
    row_send_to(half_rows(1, 0), "pair", 10)
    run("rows2")
    arrived(half_rows(2, 0), row_sem.at[4])
    row_send_to(half_rows(2, 0), "pair", 11)
    arrived(half_rows(2, 1), row_sem.at[5])
    row_send_to(half_rows(2, 1), "pair", 12)
    other = 1 - c
    arrived(norm_buf.at[y * 2 + other], row_sem.at[6])
    for k, (dy, half) in enumerate(((-1, 0), (1, 1), (-1, 1), (1, 0), (2, 0), (2, 1))):
        arrived(half_rows(dy, half, other), row_sem.at[7 + k])

    run("up")
    @pl.loop(0, 4)
    def _(n):
        columns = pl.ds(pl.multiple_of(n * 256, 256), 256)
        rows = norm_buf[...].reshape(256, 2048)
        pre = jnp.maximum(jnp.dot(rows, up_buf[:, columns], preferred_element_type=F32), 0.0)
        hidden_buf[:, columns] = (pre * pre).astype(BF16)

    def cols(r):
        return pl.ds(r * 512, 512)

    def pair_copy(r):
        return remote(
            part_buf.at[1 - c, :, :, cols(r)], pair_buf.at[:, :, cols(r)], y_send.at[r, 3], pair_sem.at[r],
            neighbour["pair"],
        )

    def last_copy(r, k):
        return remote(
            last_out.at[k, :, cols(r)], last_in.at[k, :, cols(r)], y_send.at[r, k], last_sem.at[r, k],
            neighbour["y", (2, 1, -1)[k]],
        )

    def store_part(value, columns, width):
        blocks = value.reshape(4, 2, 32, width)
        for core in range(2):
            for yy in range(4):
                part_buf[core, yy, :, columns] = blocks[yy, core].astype(BF16)

    def pair_sum(r, dy):
        yy = y_at(dy)
        return part_buf[c, yy, :, cols(r)].astype(F32) + pair_buf[yy, :, cols(r)].astype(F32)

    def pair_step(r):
        pair_copy(r).wait_recv()
        for k, dy in enumerate((2, 1, -1)):
            last_out[k, :, cols(r)] = pair_sum(r, dy).astype(BF16)
            last_copy(r, k).start()

    def last_step(r):
        total = pair_sum(r, 0)
        for k in range(3):
            last_copy(r, k).wait_recv()
            total = total + last_in[k, :, cols(r)].astype(F32)
        return total

    def mixer_sums(r, dz):
        zz = lax.rem(z - dz + 4, 4)
        for pair in range(2):
            slot = zz * 4 + pair * 2
            w = jnp.concatenate([down_buf[slot], down_buf[slot + 1]], axis=1)
            value = jnp.dot(hidden_buf[...], w, preferred_element_type=F32)
            store_part(value, pl.ds(r * 512 + pair * 256, 256), 256)
        pair_copy(r).start()

    def finish(r, dz):
        columns = pl.ds(pl.multiple_of(lax.rem(z - dz + 4, 4) * 512, 512), 512)
        out_ref[:, columns] = (upd_buf[:, columns] + last_step(r)).astype(BF16)

    rounds = tuple(enumerate(ROW_ORDER))
    for i, (r, dz) in enumerate(rounds):
        run(("row", dz))
        mixer_sums(r, dz)
        if i >= 1:
            pair_step(r - 1)
        if i >= 3:
            finish(*rounds[i - 3])
    pair_step(3)
    for r, dz in rounds[1:]:
        finish(r, dz)

    for r in range(4):
        pair_copy(r).wait_send()
        for k in range(3):
            last_copy(r, k).wait_send()
    for copy in sent + ow_sent + [ex_copy(n) for n in range(4)]:
        copy.wait_send()
    each_query(lambda copy: copy.wait_send())
    each_mixed(lambda copy: copy.wait_send())
    for g, ref in enumerate((up_buf.at[pl.ds(0, 1920)], down_buf.at[pl.ds(0, 15)])):
        arrived(ref, send_sem.at[g])

    @pl.when(primary)
    def _():
        arrived(kv_buf.at[pl.ds(0, 12)], kv_send.at[0])
        arrived(kv_buf, kv_send.at[1])


def local(qn, kn, vn, qb, kb, vb, offn, offb, res, on, ob, gain, up, down):
    hbm = pl.BlockSpec(memory_space=pl.ANY)
    vmem = pl.BlockSpec(memory_space=pltpu.VMEM)
    dma = pltpu.SemaphoreType.DMA
    return pl.pallas_call(
        body,
        out_shape=jax.ShapeDtypeStruct((32, 2048), BF16),
        in_specs=[hbm, hbm, hbm, hbm, hbm, hbm, vmem, vmem, hbm, hbm, hbm, vmem, hbm, hbm],
        out_specs=vmem,
        scratch_shapes=[
            pltpu.VMEM((2, KV_ROWS, 128), BF16),
            pltpu.VMEM((16, KV_ROWS, 128), BF16),
            pltpu.VMEM((2048, 1024), BF16),
            pltpu.VMEM((16, 1024, 128), BF16),
            pltpu.VMEM((8, 128, 2048), BF16),
            pltpu.VMEM((2, 256, 128), BF16),
            pltpu.VMEM((16, 32, 128), BF16),
            pltpu.VMEM((2, 512, 128), BF16),
            pltpu.VMEM((4, 2, 512, 128), F32),
            pltpu.VMEM((4, 512, 128), F32),
            pltpu.VMEM((256, 256), BF16),
            pltpu.VMEM((16, 32, 128), BF16),
            pltpu.VMEM((2, 8, 32, 128), BF16),
            pltpu.VMEM((32, 2048), BF16),
            pltpu.VMEM((32, 2048), F32),
            pltpu.VMEM((32, 2048), BF16),
            pltpu.VMEM((32, 2048), BF16),
            pltpu.VMEM((2, 4, 32, 2048), BF16),
            pltpu.VMEM((4, 32, 2048), BF16),
            pltpu.VMEM((3, 32, 2048), BF16),
            pltpu.VMEM((3, 32, 2048), BF16),
            pltpu.VMEM((32, 2048), F32),
            pltpu.VMEM((8, 32, 2048), BF16),
            pltpu.VMEM((256, 1024), BF16),
            dma((14,)),
            dma((2, 4, 16)),
            dma((2,)),
            dma((4,)),
            dma((2,)),
            dma((4, 2)),
            dma((4, 2)),
            dma((2,)),
            dma((4, 4)),
            dma((4, 2)),
            dma((16,)),
            dma((2, 4, 2)),
            dma((2, 8)),
            dma((4, 4)),
            dma((2,)),
            dma((2,)),
            dma((2, 2)),
            dma((2, 2)),
            dma((4,)),
            dma((4,)),
            dma((4,)),
            dma((4, 3)),
            dma((13,)),
            dma((13,)),
            dma((4, 4)),
        ],
        compiler_params=pltpu.CompilerParams(
            collective_id=0, has_side_effects=True, vmem_limit_bytes=60 * 1024 * 1024
        ),
    )(qn, kn, vn, qb, kb, vb, offn, offb, res, on, ob, gain.reshape(1, 2048), up, down)


def solution(mesh):
    return jax.shard_map(
        local,
        mesh=mesh,
        in_specs=(
            P("sp", "tp"), P("sp", "tp"), P("sp", "tp"), P("sp", "tp"), P("sp", "tp"), P("sp", "tp"),
            P("tp", "sp"), P("tp", "sp"), P(("sp", "tp"), None), P("tp", None), P("tp", None), P(),
            P("sp", "tp"), P("tp", "sp"),
        ),
        out_specs=P(("sp", "tp"), None),
        check_vma=False,
    )
```

```python
import functools

import jax
import jax.numpy as jnp
from jax import lax
from jax.experimental import pallas as pl
from jax.experimental.pallas import tpu as pltpu
from jax.sharding import PartitionSpec as P

MESH = pl.DeviceIdType.MESH
LOG2E = 1.4426950408889634
F32 = jnp.float32
BF16 = jnp.bfloat16

OFF, VAL, KV_ROWS = 256, 272, 528


def children(q, dx, dz):
    first, second = (dx, dz) if q < 2 else (dz, dx)
    a, b = ("x", "z") if q < 2 else ("z", "x")
    odd = q % 2
    out = []

    def node(f, s):
        return (f, s) if q < 2 else (s, f)

    if second == 0:
        if first == 0:
            out += [(a, 1, *node(1, 0)), (a, -1, *node(3, 0))]
        elif first == 1 and odd == 0:
            out += [(a, 1, *node(2, 0))]
        elif first == 3 and odd == 1:
            out += [(a, -1, *node(2, 0))]
    if second == 0:
        out += [(b, 1, *node(first, 1)), (b, -1, *node(first, 3))]
    elif second == 1 and odd == 0:
        out += [(b, 1, *node(first, 2))]
    elif second == 3 and odd == 1:
        out += [(b, -1, *node(first, 2))]
    return out


WIRE, DELAY = 6.0, 2.2
POINTS = (
    ("sides", 2.8, 14.0),
    ("keys1", 15.5, 20.0),
    ("keys2", 19.0, 22.5),
    ("att1", 22.3, 24.5),
    ("mix1", 26.0, 31.0),
    ("mix2", 28.0, 34.0),
    ("mix3", 33.0, 39.0),
    ("rows0", 36.0, 41.0),
    ("rows1", 39.5, 44.0),
    ("rows2", 41.0, 48.0),
)
SIZES = ((16, 16, 48, 48), (272, 272, 240, 240))
STARTS = ((0, 16, 32, 80), (0, 272, 544, 784))


def plan():
    free = {(axis, step): 0.0 for axis in "xz" for step in (1, -1)}
    landing, backlog, steps = {}, [], {}
    left = {(g, dz): 12 if dz == 0 else 16 for g in range(2) for dz in range(4)}

    def offer(g, q, child):
        first = (child[0] == "x") == (q < 2)
        backlog.append((g, 0 if first else 1, len(backlog), q, child))

    def issue(now, out, until, axes=("x", "z")):
        for entry in sorted(backlog):
            g, _, _, q, child = entry
            axis, step, dx, dz = child
            if axis in axes and free[axis, step] <= until:
                start = max(now, free[axis, step])
                free[axis, step] = start + WIRE * SIZES[g][q] / sum(SIZES[g])
                landing[g, q, dx, dz] = free[axis, step] + DELAY
                out.append(("send", g, q, child))
                backlog.remove(entry)

    def take(out, event):
        g, q, dx, dz = event
        del landing[event]
        left[g, dz] -= 1
        out.append(("wait", g, q, (dx, dz)))
        for child in children(q, dx, dz):
            offer(g, q, child)

    for g in range(2):
        for q in range(4):
            for child in children(q, 0, 0):
                offer(g, q, child)
    for point, now, until in POINTS:
        out = []
        axes = ("x",) if point == "sides" else ("x", "z")
        for when, event in sorted((when, event) for event, when in landing.items()):
            if when <= now - 0.3:
                take(out, event)
        issue(now, out, until, axes)
        steps[point] = out
    order, out = [], []
    while landing or backlog:
        when, event = min((when, event) for event, when in landing.items())
        now = max(now, when)
        take(out, event)
        issue(now, out, now + 6.0)
        if not any(left[0, dz] for dz in range(4)) and "up" not in steps:
            steps["up"] = out
            out = []
        for dz in range(4):
            if "up" in steps and not left[1, dz] and dz not in order:
                order.append(dz)
                steps["row", dz] = out
                out = []
    return steps, order, now


PLAN, ROW_ORDER, PLAN_END = plan()


def body(
    qn_hbm, kn_hbm, vn_hbm, qb_hbm, kb_hbm, vb_hbm, offn_ref, offb_ref, res_hbm,
    on_hbm, ob_hbm, gain_ref, up_hbm, down_hbm, out_hbm,
    stage, kv_buf, up_buf, down_buf, outw, q_own, q_all, head_buf, kept_buf, acc_buf, tri_buf,
    mix_out, mix_all, res_buf, att_buf, ex_out, ex_in, part_buf, pair_buf, last_out, last_in,
    upd_buf, norm_buf, hidden_buf, out_buf,
    load_sem, recv_sem, send_sem, x_sem, x_send, z_sem, far_sem, kv_send, kvp_sem,
    q_sem, m_sem, ow_sem, ex_sem, pair_sem, last_sem, row_sem, y_send, out_sem,
):
    s = lax.axis_index("sp")
    t = lax.axis_index("tp")
    x, z = lax.rem(s, 4), lax.div(s, 4)
    c, y = lax.rem(t, 2), lax.div(t, 2)
    part = z * 2 + c
    primary = lax.rem(x, 2) == c
    y_odd = lax.rem(y, 2)
    y_mate = y + 1 - 2 * y_odd
    same_pair = lax.div(z, 2) == lax.div(y, 2)
    mix_y = jnp.where(same_pair, z, 3 - z)
    mix_block = jnp.where(same_pair, jnp.int32(0), jnp.int32(1))
    holds_own = mix_y == y

    def xz(dx, dz):
        return lax.rem(z + dz % 4, 4) * 4 + lax.rem(x + dx % 4, 4)

    def y_at(dy):
        return lax.rem(y + dy + 4, 4)

    def z_at(dz):
        return lax.rem(z + dz + 4, 4)

    neighbour = {
        ("x", 1): {"sp": xz(1, 0), "tp": t},
        ("x", -1): {"sp": xz(-1, 0), "tp": t},
        ("z", 1): {"sp": xz(0, 1), "tp": t},
        ("z", -1): {"sp": xz(0, -1), "tp": t},
        "pair": {"sp": s, "tp": y * 2 + (1 - c)},
        ("y", 1): {"sp": s, "tp": y_at(1) * 2 + c},
        ("y", -1): {"sp": s, "tp": y_at(-1) * 2 + c},
        ("y", 2): {"sp": s, "tp": y_at(2) * 2 + c},
    }

    def remote(src, dst, send, recv, target):
        return pltpu.make_async_remote_copy(
            src_ref=src, dst_ref=dst, send_sem=send, recv_sem=recv, device_id=target, device_id_type=MESH
        )

    def arrived(ref, sem):
        pltpu.make_async_copy(ref, ref, sem).wait()

    own = pl.multiple_of(s * 128, 128)
    loads = [
        (kn_hbm, stage.at[0, pl.ds(0, 256)]),
        (vn_hbm, stage.at[0, pl.ds(VAL, 256)]),
        (kb_hbm, stage.at[1, pl.ds(0, 256)]),
        (vb_hbm, stage.at[1, pl.ds(VAL, 256)]),
        (qn_hbm, q_own.at[0]),
        (qb_hbm, q_own.at[1]),
        (on_hbm, outw.at[y_odd * 4 + c]),
        (ob_hbm, outw.at[y_odd * 4 + 2 + c]),
        (up_hbm, up_buf.at[pl.ds(own, 128)]),
        (down_hbm, down_buf.at[s]),
        (res_hbm, res_buf),
    ]
    groups = (0, 0, 0, 0, 1, 1, 2, 2, 3, 3, 4)
    loads = [pltpu.make_async_copy(a, b, load_sem.at[k]) for k, (a, b) in zip(groups, loads)]
    for copy in loads:
        copy.start()

    mine = [
        [
            pltpu.make_async_copy(k_hbm, kv_buf.at[s, pl.ds(0, 256)], load_sem.at[5]),
            pltpu.make_async_copy(v_hbm, kv_buf.at[s, pl.ds(VAL, 256)], load_sem.at[5]),
            pltpu.make_async_copy(q_hbm.at[pl.ds(pl.multiple_of(part * 32, 32), 32)], q_all.at[s], load_sem.at[6]),
        ]
        for k_hbm, v_hbm, q_hbm in ((kn_hbm, vn_hbm, qn_hbm), (kb_hbm, vb_hbm, qb_hbm))
    ]
    for unit in range(2):

        @pl.when(x == c + 2 * unit)
        def _():
            for copy in mine[unit]:
                copy.start()

    def greet(target, unless=None):
        def signal():
            pl.semaphore_signal(barrier, inc=1, device_id=target, device_id_type=MESH)

        if unless is None:
            signal()
        else:
            pl.when(jnp.logical_not(unless))(signal)

    barrier = pltpu.get_barrier_semaphore()
    for target in neighbour.values():
        greet(target)
    for dz in range(4):
        for dx in range(4):
            here = (dx, dz) == (0, 0)
            greet({"sp": xz(dx, dz), "tp": y * 2 + lax.rem(x, 2)}, primary if here else None)
    for block, rows_z in enumerate((y, 3 - y)):
        for plane in (y, y_mate):
            for dx in range(4):
                here = dx == 0 and plane is y
                greet(
                    {"sp": rows_z * 4 + lax.rem(x + dx, 4), "tp": plane * 2 + c},
                    rows_z == z if here else None,
                )

    offn = offn_ref[...].astype(F32)
    offb = offb_ref[...].astype(F32)
    blank = jnp.zeros((14, 128), F32)
    narrow_rows = [offn[0:1, :128], offn[0:1, 128:], offn[1:2, :128], offn[1:2, 128:], blank[:12]]
    broad_rows = [offb[0:1, :128], offb[0:1, 128:], blank]
    for unit, rows in enumerate((narrow_rows, broad_rows)):
        value = jnp.concatenate(rows, axis=0).astype(BF16)
        stage[unit, OFF : OFF + 16, :] = value

        @pl.when(x == c + 2 * unit)
        def _():
            kv_buf[s, OFF : OFF + 16, :] = value

    later = lax.broadcasted_iota(jnp.int32, (256, 256), 0)
    earlier = lax.broadcasted_iota(jnp.int32, (256, 256), 1)
    tri_buf[...] = jnp.where(later >= earlier, 1.0, 0.0).astype(BF16)
    acc_buf[...] = jnp.zeros_like(acc_buf)
    kept_buf[...] = jnp.zeros_like(kept_buf)
    one, none = jnp.int32(1), jnp.int32(0)
    pl.semaphore_wait(barrier, 40 - jnp.where(primary, one, none) - jnp.where(holds_own, one, none))

    def piece(g, slot, q):
        if g == 0:
            return up_buf.at[pl.ds(pl.multiple_of(slot * 128 + STARTS[0][q], 16), SIZES[0][q])]
        return down_buf.at[slot, pl.ds(STARTS[1][q], SIZES[1][q])]

    def send(g, slot, q, axis, step, dx, dz):
        ref = piece(g, slot, q)
        remote(ref, ref, send_sem.at[g], recv_sem.at[g, q, dz * 4 + dx], neighbour[axis, step]).start()

    def run(point):
        for kind, g, q, what in PLAN[point]:
            if kind == "send":
                axis, step, dx, dz = what
                here = (dx - step, dz) if axis == "x" else (dx, dz - step)
                send(g, xz(-here[0], -here[1]), q, axis, step, dx, dz)
            else:
                dx, dz = what
                arrived(piece(g, xz(-dx, -dz), q), recv_sem.at[g, q, dz * 4 + dx])

    arrived(head_buf, load_sem.at[0])

    def x_copy(unit):
        col = c + 2 * unit
        return remote(
            stage.at[unit], kv_buf.at[s], x_send.at[unit], x_sem.at[lax.rem(x - col + 4, 4)],
            {"sp": z * 4 + col, "tp": t},
        )

    for unit in range(2):

        @pl.when(x != c + 2 * unit)
        def _():
            x_copy(unit).start()

    def kv_slot(d, dz):
        return xz(d, -dz)

    def to_column(d):
        ref = kv_buf.at[kv_slot(d, 0)]
        remote(ref, ref, kv_send.at[0], z_sem.at[d, 0], neighbour["z", 1]).start()
        remote(ref, ref, kv_send.at[0], z_sem.at[d, 1], neighbour["z", -1]).start()
        remote(ref, ref, kv_send.at[1], kvp_sem.at[0], neighbour["pair"]).start()

    def from_row(d):
        for k, dz in ((0, 1), (1, 3)):
            slot = kv_slot(d, dz)
            ref = kv_buf.at[slot]
            arrived(ref, z_sem.at[d, k])
            half = kv_buf.at[slot, pl.ds(0, VAL) if k == 0 else pl.ds(VAL, 256)]
            remote(half, half, kv_send.at[0], far_sem.at[d, k], neighbour["z", 1 if k == 0 else -1]).start()
            remote(ref, ref, kv_send.at[1], kvp_sem.at[dz], neighbour["pair"]).start()

    def far_half(d, k):
        return kv_buf.at[kv_slot(d, 2), pl.ds(0, VAL) if k == 0 else pl.ds(VAL, 256)]

    def from_far(d):
        for k in range(2):
            half = far_half(d, k)
            arrived(half, far_sem.at[d, k])
            remote(half, half, kv_send.at[1], kvp_sem.at[2], neighbour["pair"]).start()

    @pl.when(primary)
    def _():
        arrived(q_own, load_sem.at[5])
        arrived(q_all.at[s], load_sem.at[6])
        to_column(0)

    arrived(q_own, load_sem.at[1])
    arrived(outw.at[pl.ds(0, 2)], load_sem.at[2])

    def q_copy(unit, dz, dc):
        core = c if dc == 0 else 1 - c
        rows = pl.ds(pl.multiple_of((z_at(dz) * 2 + core) * 32, 32), 32)
        return remote(
            q_own.at[unit, rows], q_all.at[s], q_sem.at[0], q_sem.at[1],
            {"sp": z_at(dz) * 4 + c + 2 * unit, "tp": y * 2 + core},
        )

    def each_query(act):
        for unit in range(2):
            for dz in range(4):
                for dc in range(2):
                    if (dz, dc) == (0, 0):
                        pl.when(x != c + 2 * unit)(lambda: act(q_copy(unit, dz, dc)))
                    else:
                        act(q_copy(unit, dz, dc))

    each_query(lambda copy: copy.start())

    def ow(k, foreign, core):
        plane = 1 - y_odd if foreign else y_odd
        return outw.at[plane * 4 + core + 2 * k]

    mate = {"sp": s, "tp": y_mate * 2 + c}

    def ow_copy(k):
        return remote(ow(k, 0, c), ow(k, 0, c), ow_sem.at[2], ow_sem.at[k], mate)

    def ow_pair(k, foreign):
        ref = ow(k, foreign, c)
        return remote(ref, ref, ow_sem.at[3], ow_sem.at[4], neighbour["pair"])

    for copy in (ow_copy(0), ow_copy(1), ow_pair(0, 0), ow_pair(1, 0)):
        copy.start()

    def ow_pass(k):
        arrived(ow(k, 1, c), ow_sem.at[k])
        ow_pair(k, 1).start()

    arrived(outw.at[0], load_sem.at[3])
    for unit in range(2):
        pl.when(x != c + 2 * unit)(lambda: x_copy(unit).wait_send())
    run("sides")

    lane = lax.broadcasted_iota(jnp.int32, (512, 128), 1)
    zero = jnp.zeros((), BF16)
    ahead = (later // 32) * 256 + lax.rem(later, 32) - earlier + part * 32

    def attend(slot, zz, heads, chunks, scale):
        offs = kv_buf[slot, OFF:VAL, :].astype(F32) * LOG2E
        k = kv_buf[slot, pl.ds(0, 256), :]
        v = kv_buf[slot, pl.ds(VAL, 256), :]
        items = [(chunk, masked, h) for chunk, masked in chunks for h in range(heads)]
        scores, gone, weights = [], [], []
        for chunk, masked, h in items:
            product = lax.dot_general(
                head_buf[h, chunk * 256 : chunk * 256 + 256], k, (((1,), (1,)), ((), ())),
                preferred_element_type=F32,
            )
            off = jnp.concatenate([offs[2 * h : 2 * h + 1], offs[2 * h + 1 : 2 * h + 2]], axis=1)
            scores.append(product * scale + off)
        for (chunk, masked, h), score in zip(items, scores):
            drop = jnp.maximum(score, lax.log2(1.0 + lax.exp2(jnp.minimum(score, 126.0))))
            if masked:
                drop = jnp.where(ahead > slot * 256 - chunk * 2048, drop, 0.0)
            gone.append(jnp.dot(drop.astype(BF16), tri_buf[...], preferred_element_type=F32))
        for (chunk, masked, h), score, lost in zip(items, scores, gone):
            rows = slice(chunk * 256, chunk * 256 + 256)
            kept = kept_buf[zz, h, rows]
            weight = lax.exp2(score - lost - jnp.concatenate([kept, kept], axis=1))
            if masked:
                weight = jnp.where(ahead > slot * 256 - chunk * 2048, weight, 0.0)
            kept_buf[zz, h, rows] = kept + jnp.broadcast_to(lost[:, 0:1], (256, 128))
            weights.append(weight.astype(BF16))
        for chunk, _ in chunks:
            rows = slice(chunk * 256, chunk * 256 + 256)
            total = acc_buf[zz, rows]
            for (other, _, h), weight in zip(items, weights):
                if other == chunk:
                    values = v
                    if heads == 2:
                        values = jnp.where((lane[:256] < 64) if h == 0 else (lane[:256] >= 64), v, zero)
                    total = total + jnp.dot(weight, values, preferred_element_type=F32)
            acc_buf[zz, rows] = total

    def each_group(act):
        pl.when(x < 2)(lambda: act(2, LOG2E * 64**-0.5))
        pl.when(x >= 2)(lambda: act(1, LOG2E * 128**-0.5))

    def set_heads(heads, scale):
        queries = q_all[...].reshape(512, 128)
        if heads == 2:
            head_buf[0] = jnp.where(lane < 64, queries, zero)
            head_buf[1] = jnp.where(lane >= 64, queries, zero)
        else:
            head_buf[0] = queries

    def attend_row(dz):
        zz = z_at(-dz)

        def act(heads, scale):
            for near, chunks in ((True, ((1, True),)), (False, ((0, True), (1, False)))):

                @pl.when((zz >= 2) if near else (zz < 2))
                def _():
                    pl.loop(0, 4)(lambda k: attend(zz * 4 + 3 - k, zz, heads, chunks, scale))

        each_group(act)

    def join_rows(heads, scale):
        total, past = acc_buf[3], None
        for zz in (2, 1, 0):
            kept = kept_buf[zz + 1, 0]
            if heads == 2:
                kept = jnp.where(lane < 64, kept, kept_buf[zz + 1, 1])
            past = kept if past is None else past + kept
            total = total + acc_buf[zz] * lax.exp2(-past)
        mix_out[...] = total.reshape(16, 32, 128).astype(BF16)

    def secondary_waits(rows):
        @pl.when(jnp.logical_not(primary))
        def _():
            for dz in rows:
                arrived(kv_buf.at[pl.ds(pl.multiple_of(z_at(-dz) * 4, 4), 4)], kvp_sem.at[dz])

    @pl.when(primary)
    def _():
        for d in (1, 3):
            arrived(kv_buf.at[kv_slot(d, 0)], x_sem.at[d])
            to_column(d)
        from_row(0)
        arrived(kv_buf.at[kv_slot(2, 0)], x_sem.at[2])
        to_column(2)

    def all_but(mine, ref, sem):
        pl.when(mine)(lambda: arrived(ref.at[pl.ds(0, 15)], sem))
        pl.when(jnp.logical_not(mine))(lambda: arrived(ref, sem))

    all_but(primary, q_all, q_sem.at[1])
    each_group(set_heads)
    secondary_waits((0,))
    attend_row(0)

    @pl.when(primary)
    def _():
        from_row(1)
        from_row(3)
        from_row(2)

    run("keys1")
    secondary_waits((1, 3))
    attend_row(1)
    ow_pass(0)

    @pl.when(primary)
    def _():
        for d in (0, 1, 3, 2):
            from_far(d)

    run("keys2")
    attend_row(3)
    run("att1")
    secondary_waits((2,))
    attend_row(2)
    each_group(join_rows)

    def m_copy(dx, dz):
        return remote(
            mix_out.at[xz(dx, dz)], mix_all.at[mix_block, y_odd * 4 + x], m_sem.at[0],
            m_sem.at[1], {"sp": xz(dx, dz), "tp": mix_y * 2 + c},
        )

    def each_mixed(act):
        for dz in range(4):
            for dx in range(4):
                if (dx, dz) == (0, 0):
                    pl.when(jnp.logical_not(holds_own))(lambda: act(m_copy(dx, dz)))
                else:
                    act(m_copy(dx, dz))

    each_mixed(lambda copy: copy.start())

    @pl.when(holds_own)
    def _():
        mix_all[mix_block, y_odd * 4 + x] = mix_out[s]

    run("mix1")
    ow_pass(1)
    run("mix2")
    all_but(holds_own, mix_out, m_sem.at[1])
    arrived(outw.at[pl.ds(0, 4)], ow_sem.at[4])
    arrived(res_buf, load_sem.at[4])

    mixed = jnp.concatenate([mix_all[:, unit].reshape(64, 128) for unit in range(8)], axis=1)

    def ex_copy(n):
        columns = pl.ds(n * 512, 512)
        return remote(
            ex_out.at[:, columns], ex_in.at[:, columns], ex_sem.at[0], ex_sem.at[1],
            {"sp": s, "tp": (3 - y) * 2 + c},
        )

    for n in range(4):
        columns = slice(n * 512, n * 512 + 512)
        sums = jnp.dot(mixed, outw[:, :, columns].reshape(1024, 512), preferred_element_type=F32)
        att_buf[:, columns] = sums[:32]
        ex_out[:, columns] = sums[32:].astype(BF16)
        ex_copy(n).start()
    run("mix3")
    arrived(ex_in, ex_sem.at[1])
    updated = res_buf[...].astype(F32) + (att_buf[...] + ex_in[...].astype(F32))
    upd_buf[...] = updated
    scale = lax.rsqrt(jnp.mean(updated * updated, axis=-1, keepdims=True) + 1e-06)
    norm_buf[t] = (updated * scale * gain_ref[...]).astype(BF16)

    def row_copy(ref, target, k):
        return remote(ref, ref, row_sem.at[7], row_sem.at[k if k < 6 else 6], neighbour[target])

    def half_rows(dy, k, core=None):
        slot = y_at(dy) * 2 + (c if core is None else core)
        return norm_buf.at[slot, pl.ds(16 * k, 16)]

    def row_send_to(ref, target, k):
        row_copy(ref, target, k).start()

    row_send_to(half_rows(0, 0), ("y", 1), 0)
    row_send_to(half_rows(0, 1), ("y", -1), 1)
    row_send_to(half_rows(0, 1), ("y", 1), 2)
    row_send_to(half_rows(0, 0), ("y", -1), 3)
    row_send_to(norm_buf.at[t], "pair", 6)
    run("rows0")
    arrived(half_rows(-1, 0), row_sem.at[0])
    row_send_to(half_rows(-1, 0), ("y", 1), 4)
    arrived(half_rows(1, 1), row_sem.at[1])
    row_send_to(half_rows(1, 1), ("y", -1), 5)
    row_send_to(half_rows(-1, 0), "pair", 7)
    row_send_to(half_rows(1, 1), "pair", 8)
    run("rows1")
    arrived(half_rows(-1, 1), row_sem.at[2])
    row_send_to(half_rows(-1, 1), "pair", 9)
    arrived(half_rows(1, 0), row_sem.at[3])
    row_send_to(half_rows(1, 0), "pair", 10)
    run("rows2")
    arrived(half_rows(2, 0), row_sem.at[4])
    row_send_to(half_rows(2, 0), "pair", 11)
    arrived(half_rows(2, 1), row_sem.at[5])
    row_send_to(half_rows(2, 1), "pair", 12)
    arrived(norm_buf.at[pl.ds(0, 4)], row_sem.at[6])
    run("up")
    @pl.loop(0, 4)
    def _(n):
        columns = pl.ds(pl.multiple_of(n * 256, 256), 256)
        rows = norm_buf[...].reshape(256, 2048)
        pre = jnp.maximum(jnp.dot(rows, up_buf[:, columns], preferred_element_type=F32), 0.0)
        hidden_buf[:, columns] = (pre * pre).astype(BF16)

    def cols(r):
        return pl.ds(r * 512, 512)

    def pair_copy(r):
        return remote(
            part_buf.at[1 - c, :, :, cols(r)], pair_buf.at[:, :, cols(r)], y_send.at[0], pair_sem.at[r],
            neighbour["pair"],
        )

    def last_copy(r, k):
        return remote(
            last_out.at[k, :, cols(r)], last_in.at[k, :, cols(r)], y_send.at[1], last_sem.at[r],
            neighbour["y", (2, 1, -1)[k]],
        )

    def store_part(value, columns, width):
        blocks = value.reshape(4, 2, 32, width)
        for core in range(2):
            for yy in range(4):
                part_buf[core, yy, :, columns] = blocks[yy, core].astype(BF16)

    def pair_sum(r, dy):
        yy = y_at(dy)
        return part_buf[c, yy, :, cols(r)].astype(F32) + pair_buf[yy, :, cols(r)].astype(F32)

    def pair_step(r):
        pair_copy(r).wait_recv()
        for k, dy in enumerate((2, 1, -1)):
            last_out[k, :, cols(r)] = pair_sum(r, dy).astype(BF16)
            last_copy(r, k).start()

    def last_step(r):
        total = pair_sum(r, 0)
        arrived(last_in.at[:, :, cols(r)], last_sem.at[r])
        for k in range(3):
            total = total + last_in[k, :, cols(r)].astype(F32)
        return total

    def mixer_sums(r, dz):
        zz = lax.rem(z - dz + 4, 4)
        for pair in range(2):
            slot = zz * 4 + pair * 2
            w = jnp.concatenate([down_buf[slot], down_buf[slot + 1]], axis=1)
            value = jnp.dot(hidden_buf[...], w, preferred_element_type=F32)
            store_part(value, pl.ds(r * 512 + pair * 256, 256), 256)
        pair_copy(r).start()

    def finish(r, dz):
        columns = pl.ds(pl.multiple_of(lax.rem(z - dz + 4, 4) * 512, 512), 512)
        out_buf[:, columns] = (upd_buf[:, columns] + last_step(r)).astype(BF16)
        pltpu.make_async_copy(out_buf.at[:, columns], out_hbm.at[:, columns], out_sem.at[0]).start()

    rounds = tuple(enumerate(ROW_ORDER))
    for i, (r, dz) in enumerate(rounds):
        run(("row", dz))
        mixer_sums(r, dz)
        if i >= 1:
            pair_step(r - 1)
    pair_step(3)
    for r, dz in rounds:
        finish(r, dz)

    arrived(pair_buf, y_send.at[0])
    arrived(last_out, y_send.at[1])
    arrived(norm_buf.at[pl.ds(0, 7)], row_sem.at[7])
    arrived(outw.at[pl.ds(0, 2)], ow_sem.at[2])
    arrived(outw.at[pl.ds(0, 4)], ow_sem.at[3])
    arrived(ex_out, ex_sem.at[0])
    all_but(primary, q_all, q_sem.at[0])
    all_but(holds_own, mix_out, m_sem.at[0])
    for g, ref in enumerate((up_buf.at[pl.ds(0, 1920)], down_buf.at[pl.ds(0, 15)])):
        arrived(ref, send_sem.at[g])

    @pl.when(primary)
    def _():
        arrived(kv_buf.at[pl.ds(0, 12)], kv_send.at[0])
        arrived(kv_buf, kv_send.at[1])

    pltpu.make_async_copy(out_buf, out_hbm, out_sem.at[0]).wait()


def local(qn, kn, vn, qb, kb, vb, offn, offb, res, on, ob, gain, up, down):
    hbm = pl.BlockSpec(memory_space=pl.ANY)
    vmem = pl.BlockSpec(memory_space=pltpu.VMEM)
    dma = pltpu.SemaphoreType.DMA
    return pl.pallas_call(
        body,
        out_shape=jax.ShapeDtypeStruct((32, 2048), BF16),
        in_specs=[hbm, hbm, hbm, hbm, hbm, hbm, vmem, vmem, hbm, hbm, hbm, vmem, hbm, hbm],
        out_specs=hbm,
        scratch_shapes=[
            pltpu.VMEM((2, KV_ROWS, 128), BF16),
            pltpu.VMEM((16, KV_ROWS, 128), BF16),
            pltpu.VMEM((2048, 1024), BF16),
            pltpu.VMEM((16, 1024, 128), BF16),
            pltpu.VMEM((8, 128, 2048), BF16),
            pltpu.VMEM((2, 256, 128), BF16),
            pltpu.VMEM((16, 32, 128), BF16),
            pltpu.VMEM((2, 512, 128), BF16),
            pltpu.VMEM((4, 2, 512, 128), F32),
            pltpu.VMEM((4, 512, 128), F32),
            pltpu.VMEM((256, 256), BF16),
            pltpu.VMEM((16, 32, 128), BF16),
            pltpu.VMEM((2, 8, 32, 128), BF16),
            pltpu.VMEM((32, 2048), BF16),
            pltpu.VMEM((32, 2048), F32),
            pltpu.VMEM((32, 2048), BF16),
            pltpu.VMEM((32, 2048), BF16),
            pltpu.VMEM((2, 4, 32, 2048), BF16),
            pltpu.VMEM((4, 32, 2048), BF16),
            pltpu.VMEM((3, 32, 2048), BF16),
            pltpu.VMEM((3, 32, 2048), BF16),
            pltpu.VMEM((32, 2048), F32),
            pltpu.VMEM((8, 32, 2048), BF16),
            pltpu.VMEM((256, 1024), BF16),
            pltpu.VMEM((32, 2048), BF16),
            dma((7,)),
            dma((2, 4, 16)),
            dma((2,)),
            dma((4,)),
            dma((2,)),
            dma((4, 2)),
            dma((4, 2)),
            dma((2,)),
            dma((4,)),
            dma((2,)),
            dma((2,)),
            dma((5,)),
            dma((2,)),
            dma((4,)),
            dma((4,)),
            dma((8,)),
            dma((2,)),
            dma((1,)),
        ],
        compiler_params=pltpu.CompilerParams(
            collective_id=0, has_side_effects=True, vmem_limit_bytes=60 * 1024 * 1024
        ),
    )(qn, kn, vn, qb, kb, vb, offn, offb, res, on, ob, gain.reshape(1, 2048), up, down)


def solution(mesh):
    return jax.shard_map(
        local,
        mesh=mesh,
        in_specs=(
            P("sp", "tp"), P("sp", "tp"), P("sp", "tp"), P("sp", "tp"), P("sp", "tp"), P("sp", "tp"),
            P("tp", "sp"), P("tp", "sp"), P(("sp", "tp"), None), P("tp", None), P("tp", None), P(),
            P("sp", "tp"), P("tp", "sp"),
        ),
        out_specs=P(("sp", "tp"), None),
        check_vma=False,
    )
```

```python
import functools

import jax
import jax.numpy as jnp
from jax import lax
from jax.experimental import pallas as pl
from jax.experimental.pallas import tpu as pltpu
from jax.sharding import PartitionSpec as P

MESH = pl.DeviceIdType.MESH
LOG2E = 1.4426950408889634
F32 = jnp.float32
BF16 = jnp.bfloat16

OFF, VAL, KV_ROWS = 256, 272, 528


def children(q, dx, dz):
    first, second = (dx, dz) if q < 2 else (dz, dx)
    a, b = ("x", "z") if q < 2 else ("z", "x")
    odd = q % 2
    out = []

    def node(f, s):
        return (f, s) if q < 2 else (s, f)

    if second == 0:
        if first == 0:
            out += [(a, 1, *node(1, 0)), (a, -1, *node(3, 0))]
        elif first == 1 and odd == 0:
            out += [(a, 1, *node(2, 0))]
        elif first == 3 and odd == 1:
            out += [(a, -1, *node(2, 0))]
    if second == 0:
        out += [(b, 1, *node(first, 1)), (b, -1, *node(first, 3))]
    elif second == 1 and odd == 0:
        out += [(b, 1, *node(first, 2))]
    elif second == 3 and odd == 1:
        out += [(b, -1, *node(first, 2))]
    return out


WIRE, DELAY = 5.4, 2.2
POINTS = (
    ("first", 0.3, 4.0),
    ("sides", 2.8, 14.0),
    ("keys1", 15.5, 20.0),
    ("keys2", 19.0, 22.5),
    ("att1", 22.3, 24.5),
    ("mix1", 27.5, 32.5),
    ("mix2", 29.5, 35.5),
    ("mix3", 34.5, 40.5),
    ("rows0", 37.5, 42.5),
    ("rows1", 41.0, 45.5),
    ("rows2", 42.5, 49.5),
)
KEYS_END = 15.0
SIZES = ((16, 16, 48, 48), (336, 336, 176, 176))
STARTS = ((0, 16, 32, 80), (0, 336, 672, 848))


def plan():
    free = {(axis, step): 1.5 for axis in "xz" for step in (1, -1)}
    landing, backlog, steps = {}, [], {}
    left = {(g, dz): 12 if dz == 0 else 16 for g in range(2) for dz in range(4)}

    def offer(g, q, child):
        first = (child[0] == "x") == (q < 2)
        backlog.append((g, 0 if first else 1, len(backlog), q, child))

    def issue(now, out, until, axes=("x", "z")):
        for entry in sorted(backlog):
            g, _, _, q, child = entry
            axis, step, dx, dz = child
            if axis in axes and free[axis, step] <= until:
                start = max(now, free[axis, step])
                free[axis, step] = start + WIRE * SIZES[g][q] / sum(SIZES[g])
                landing[g, q, dx, dz] = free[axis, step] + DELAY
                out.append(("send", g, q, child))
                backlog.remove(entry)

    def take(out, event):
        g, q, dx, dz = event
        del landing[event]
        left[g, dz] -= 1
        out.append(("wait", g, q, (dx, dz)))
        for child in children(q, dx, dz):
            offer(g, q, child)

    for g in range(2):
        for q in range(4):
            for child in children(q, 0, 0):
                offer(g, q, child)
    for point, now, until in POINTS:
        out = []
        axes = {"first": ("z",), "sides": ("x",)}.get(point, ("x", "z"))
        for when, event in sorted((when, event) for event, when in landing.items()):
            if when <= now - 0.3:
                take(out, event)
        issue(now, out, until, axes)
        if point == "first":
            free["z", 1] = free["z", -1] = KEYS_END
        steps[point] = out
    order, out = [], []
    while landing or backlog:
        when, event = min((when, event) for event, when in landing.items())
        now = max(now, when)
        take(out, event)
        issue(now, out, now + 6.0)
        if not any(left[0, dz] for dz in range(4)) and "up" not in steps:
            steps["up"] = out
            out = []
        for dz in range(4):
            if "up" in steps and not left[1, dz] and dz not in order:
                order.append(dz)
                steps["row", dz] = out
                out = []
    return steps, order, now


PLAN, ROW_ORDER, PLAN_END = plan()


def body(
    qn_hbm, kn_hbm, vn_hbm, qb_hbm, kb_hbm, vb_hbm, offn_ref, offb_ref, res_hbm,
    on_hbm, ob_hbm, gain_ref, up_hbm, down_hbm, out_hbm,
    stage, kv_buf, up_buf, down_buf, outw, q_own, q_all, head_buf, kept_buf, acc_buf, tri_buf,
    mix_out, mix_all, res_buf, att_buf, ex_out, ex_in, part_buf, pair_buf, last_out, last_in,
    upd_buf, norm_buf, hidden_buf, out_buf,
    load_sem, recv_sem, send_sem, x_sem, x_send, z_sem, far_sem, kv_send, kvp_sem,
    q_sem, m_sem, ow_sem, ex_sem, pair_sem, last_sem, row_sem, y_send, out_sem,
):
    s = lax.axis_index("sp")
    t = lax.axis_index("tp")
    x, z = lax.rem(s, 4), lax.div(s, 4)
    c, y = lax.rem(t, 2), lax.div(t, 2)
    part = z * 2 + c
    primary = lax.rem(x, 2) == c
    y_odd = lax.rem(y, 2)
    y_mate = y + 1 - 2 * y_odd
    same_pair = lax.div(z, 2) == lax.div(y, 2)
    mix_y = jnp.where(same_pair, z, 3 - z)
    mix_block = jnp.where(same_pair, jnp.int32(0), jnp.int32(1))
    holds_own = mix_y == y

    def xz(dx, dz):
        return lax.rem(z + dz % 4, 4) * 4 + lax.rem(x + dx % 4, 4)

    def y_at(dy):
        return lax.rem(y + dy + 4, 4)

    def z_at(dz):
        return lax.rem(z + dz + 4, 4)

    neighbour = {
        ("x", 1): {"sp": xz(1, 0), "tp": t},
        ("x", -1): {"sp": xz(-1, 0), "tp": t},
        ("z", 1): {"sp": xz(0, 1), "tp": t},
        ("z", -1): {"sp": xz(0, -1), "tp": t},
        "pair": {"sp": s, "tp": y * 2 + (1 - c)},
        ("y", 1): {"sp": s, "tp": y_at(1) * 2 + c},
        ("y", -1): {"sp": s, "tp": y_at(-1) * 2 + c},
        ("y", 2): {"sp": s, "tp": y_at(2) * 2 + c},
    }

    def remote(src, dst, send, recv, target):
        return pltpu.make_async_remote_copy(
            src_ref=src, dst_ref=dst, send_sem=send, recv_sem=recv, device_id=target, device_id_type=MESH
        )

    def arrived(ref, sem):
        pltpu.make_async_copy(ref, ref, sem).wait()

    own = pl.multiple_of(s * 128, 128)
    loads = [
        (kn_hbm, stage.at[0, pl.ds(0, 256)]),
        (vn_hbm, stage.at[0, pl.ds(VAL, 256)]),
        (kb_hbm, stage.at[1, pl.ds(0, 256)]),
        (vb_hbm, stage.at[1, pl.ds(VAL, 256)]),
        (qn_hbm, q_own.at[0]),
        (qb_hbm, q_own.at[1]),
        (on_hbm, outw.at[y_odd * 4 + c]),
        (ob_hbm, outw.at[y_odd * 4 + 2 + c]),
        (up_hbm, up_buf.at[pl.ds(own, 128)]),
        (down_hbm, down_buf.at[s]),
        (res_hbm, res_buf),
    ]
    groups = (0, 0, 0, 0, 1, 1, 2, 2, 3, 3, 4)
    loads = [pltpu.make_async_copy(a, b, load_sem.at[k]) for k, (a, b) in zip(groups, loads)]
    for copy in loads:
        copy.start()

    mine = [
        [
            pltpu.make_async_copy(k_hbm, kv_buf.at[s, pl.ds(0, 256)], load_sem.at[5]),
            pltpu.make_async_copy(v_hbm, kv_buf.at[s, pl.ds(VAL, 256)], load_sem.at[5]),
            pltpu.make_async_copy(q_hbm.at[pl.ds(pl.multiple_of(part * 32, 32), 32)], q_all.at[s], load_sem.at[6]),
        ]
        for k_hbm, v_hbm, q_hbm in ((kn_hbm, vn_hbm, qn_hbm), (kb_hbm, vb_hbm, qb_hbm))
    ]
    for unit in range(2):

        @pl.when(x == c + 2 * unit)
        def _():
            for copy in mine[unit]:
                copy.start()

    def greet(target, unless=None):
        def signal():
            pl.semaphore_signal(barrier, inc=1, device_id=target, device_id_type=MESH)

        if unless is None:
            signal()
        else:
            pl.when(jnp.logical_not(unless))(signal)

    barrier = pltpu.get_barrier_semaphore()
    for target in neighbour.values():
        greet(target)
    for dz in range(4):
        for dx in range(4):
            here = (dx, dz) == (0, 0)
            greet({"sp": xz(dx, dz), "tp": y * 2 + lax.rem(x, 2)}, primary if here else None)
    for block, rows_z in enumerate((y, 3 - y)):
        for plane in (y, y_mate):
            for dx in range(4):
                here = dx == 0 and plane is y
                greet(
                    {"sp": rows_z * 4 + lax.rem(x + dx, 4), "tp": plane * 2 + c},
                    rows_z == z if here else None,
                )

    offn = offn_ref[...].astype(F32)
    offb = offb_ref[...].astype(F32)
    blank = jnp.zeros((14, 128), F32)
    narrow_rows = [offn[0:1, :128], offn[0:1, 128:], offn[1:2, :128], offn[1:2, 128:], blank[:12]]
    broad_rows = [offb[0:1, :128], offb[0:1, 128:], blank]
    for unit, rows in enumerate((narrow_rows, broad_rows)):
        value = jnp.concatenate(rows, axis=0).astype(BF16)
        stage[unit, OFF : OFF + 16, :] = value

        @pl.when(x == c + 2 * unit)
        def _():
            kv_buf[s, OFF : OFF + 16, :] = value

    later = lax.broadcasted_iota(jnp.int32, (256, 256), 0)
    earlier = lax.broadcasted_iota(jnp.int32, (256, 256), 1)
    tri_buf[...] = jnp.where(later >= earlier, 1.0, 0.0).astype(BF16)
    acc_buf[...] = jnp.zeros_like(acc_buf)
    kept_buf[...] = jnp.zeros_like(kept_buf)
    one, none = jnp.int32(1), jnp.int32(0)
    pl.semaphore_wait(barrier, 40 - jnp.where(primary, one, none) - jnp.where(holds_own, one, none))

    def piece(g, slot, q):
        if g == 0:
            return up_buf.at[pl.ds(pl.multiple_of(slot * 128 + STARTS[0][q], 16), SIZES[0][q])]
        return down_buf.at[slot, pl.ds(STARTS[1][q], SIZES[1][q])]

    def send(g, slot, q, axis, step, dx, dz):
        ref = piece(g, slot, q)
        remote(ref, ref, send_sem.at[g], recv_sem.at[g, q, dz * 4 + dx], neighbour[axis, step]).start()

    def run(point):
        for kind, g, q, what in PLAN[point]:
            if kind == "send":
                axis, step, dx, dz = what
                here = (dx - step, dz) if axis == "x" else (dx, dz - step)
                send(g, xz(-here[0], -here[1]), q, axis, step, dx, dz)
            else:
                dx, dz = what
                arrived(piece(g, xz(-dx, -dz), q), recv_sem.at[g, q, dz * 4 + dx])

    arrived(head_buf, load_sem.at[0])

    def x_copy(unit):
        col = c + 2 * unit
        return remote(
            stage.at[unit], kv_buf.at[s], x_send.at[unit], x_sem.at[lax.rem(x - col + 4, 4)],
            {"sp": z * 4 + col, "tp": t},
        )

    for unit in range(2):

        @pl.when(x != c + 2 * unit)
        def _():
            x_copy(unit).start()

    def kv_slot(d, dz):
        return xz(d, -dz)

    def to_column(d):
        ref = kv_buf.at[kv_slot(d, 0)]
        remote(ref, ref, kv_send.at[0], z_sem.at[d, 0], neighbour["z", 1]).start()
        remote(ref, ref, kv_send.at[0], z_sem.at[d, 1], neighbour["z", -1]).start()
        remote(ref, ref, kv_send.at[1], kvp_sem.at[0], neighbour["pair"]).start()

    def from_row(d):
        for k, dz in ((0, 1), (1, 3)):
            slot = kv_slot(d, dz)
            ref = kv_buf.at[slot]
            arrived(ref, z_sem.at[d, k])
            half = kv_buf.at[slot, pl.ds(0, VAL) if k == 0 else pl.ds(VAL, 256)]
            remote(half, half, kv_send.at[0], far_sem.at[d, k], neighbour["z", 1 if k == 0 else -1]).start()
            remote(ref, ref, kv_send.at[1], kvp_sem.at[dz], neighbour["pair"]).start()

    def far_half(d, k):
        return kv_buf.at[kv_slot(d, 2), pl.ds(0, VAL) if k == 0 else pl.ds(VAL, 256)]

    def from_far(d):
        for k in range(2):
            half = far_half(d, k)
            arrived(half, far_sem.at[d, k])
            remote(half, half, kv_send.at[1], kvp_sem.at[2], neighbour["pair"]).start()

    @pl.when(primary)
    def _():
        arrived(q_own, load_sem.at[5])
        arrived(q_all.at[s], load_sem.at[6])
        to_column(0)

    arrived(q_own, load_sem.at[1])
    arrived(outw.at[pl.ds(0, 2)], load_sem.at[2])

    def q_copy(unit, dz, dc):
        core = c if dc == 0 else 1 - c
        rows = pl.ds(pl.multiple_of((z_at(dz) * 2 + core) * 32, 32), 32)
        return remote(
            q_own.at[unit, rows], q_all.at[s], q_sem.at[0], q_sem.at[1],
            {"sp": z_at(dz) * 4 + c + 2 * unit, "tp": y * 2 + core},
        )

    def each_query(act):
        for unit in range(2):
            for dz in range(4):
                for dc in range(2):
                    if (dz, dc) == (0, 0):
                        pl.when(x != c + 2 * unit)(lambda: act(q_copy(unit, dz, dc)))
                    else:
                        act(q_copy(unit, dz, dc))

    each_query(lambda copy: copy.start())

    def ow(k, foreign, core):
        plane = 1 - y_odd if foreign else y_odd
        return outw.at[plane * 4 + core + 2 * k]

    mate = {"sp": s, "tp": y_mate * 2 + c}

    def ow_copy(k):
        return remote(ow(k, 0, c), ow(k, 0, c), ow_sem.at[2], ow_sem.at[k], mate)

    def ow_pair(k, foreign):
        ref = ow(k, foreign, c)
        return remote(ref, ref, ow_sem.at[3], ow_sem.at[4], neighbour["pair"])

    for copy in (ow_copy(0), ow_copy(1), ow_pair(0, 0), ow_pair(1, 0)):
        copy.start()

    def ow_pass(k):
        arrived(ow(k, 1, c), ow_sem.at[k])
        ow_pair(k, 1).start()

    arrived(outw.at[0], load_sem.at[3])
    run("first")
    for unit in range(2):
        pl.when(x != c + 2 * unit)(lambda: x_copy(unit).wait_send())
    run("sides")

    lane = lax.broadcasted_iota(jnp.int32, (512, 128), 1)
    zero = jnp.zeros((), BF16)
    ahead = (later // 32) * 256 + lax.rem(later, 32) - earlier + part * 32

    def attend(slot, zz, heads, chunks, scale):
        offs = kv_buf[slot, OFF:VAL, :].astype(F32) * LOG2E
        k = kv_buf[slot, pl.ds(0, 256), :]
        v = kv_buf[slot, pl.ds(VAL, 256), :]
        items = [(chunk, masked, h) for chunk, masked in chunks for h in range(heads)]
        scores, gone, weights = [], [], []
        for chunk, masked, h in items:
            product = lax.dot_general(
                head_buf[h, chunk * 256 : chunk * 256 + 256], k, (((1,), (1,)), ((), ())),
                preferred_element_type=F32,
            )
            off = jnp.concatenate([offs[2 * h : 2 * h + 1], offs[2 * h + 1 : 2 * h + 2]], axis=1)
            scores.append(product * scale + off)
        for (chunk, masked, h), score in zip(items, scores):
            drop = jnp.maximum(score, lax.log2(1.0 + lax.exp2(jnp.minimum(score, 126.0))))
            if masked:
                drop = jnp.where(ahead > slot * 256 - chunk * 2048, drop, 0.0)
            gone.append(jnp.dot(drop.astype(BF16), tri_buf[...], preferred_element_type=F32))
        for (chunk, masked, h), score, lost in zip(items, scores, gone):
            rows = slice(chunk * 256, chunk * 256 + 256)
            kept = kept_buf[zz, h, rows]
            weight = lax.exp2(score - lost - jnp.concatenate([kept, kept], axis=1))
            if masked:
                weight = jnp.where(ahead > slot * 256 - chunk * 2048, weight, 0.0)
            kept_buf[zz, h, rows] = kept + jnp.broadcast_to(lost[:, 0:1], (256, 128))
            weights.append(weight.astype(BF16))
        for chunk, _ in chunks:
            rows = slice(chunk * 256, chunk * 256 + 256)
            total = acc_buf[zz, rows]
            for (other, _, h), weight in zip(items, weights):
                if other == chunk:
                    values = v
                    if heads == 2:
                        values = jnp.where((lane[:256] < 64) if h == 0 else (lane[:256] >= 64), v, zero)
                    total = total + jnp.dot(weight, values, preferred_element_type=F32)
            acc_buf[zz, rows] = total

    def each_group(act):
        pl.when(x < 2)(lambda: act(2, LOG2E * 64**-0.5))
        pl.when(x >= 2)(lambda: act(1, LOG2E * 128**-0.5))

    def set_heads(heads, scale):
        queries = q_all[...].reshape(512, 128)
        if heads == 2:
            head_buf[0] = jnp.where(lane < 64, queries, zero)
            head_buf[1] = jnp.where(lane >= 64, queries, zero)
        else:
            head_buf[0] = queries

    def attend_row(dz):
        zz = z_at(-dz)

        def act(heads, scale):
            for near, chunks in ((True, ((1, True),)), (False, ((0, True), (1, False)))):

                @pl.when((zz >= 2) if near else (zz < 2))
                def _():
                    pl.loop(0, 4)(lambda k: attend(zz * 4 + 3 - k, zz, heads, chunks, scale))

        each_group(act)

    def join_rows(heads, scale):
        total, past = acc_buf[3], None
        for zz in (2, 1, 0):
            kept = kept_buf[zz + 1, 0]
            if heads == 2:
                kept = jnp.where(lane < 64, kept, kept_buf[zz + 1, 1])
            past = kept if past is None else past + kept
            total = total + acc_buf[zz] * lax.exp2(-past)
        mix_out[...] = total.reshape(16, 32, 128).astype(BF16)

    def secondary_waits(rows):
        @pl.when(jnp.logical_not(primary))
        def _():
            for dz in rows:
                arrived(kv_buf.at[pl.ds(pl.multiple_of(z_at(-dz) * 4, 4), 4)], kvp_sem.at[dz])

    @pl.when(primary)
    def _():
        for d in (1, 3):
            arrived(kv_buf.at[kv_slot(d, 0)], x_sem.at[d])
            to_column(d)
        from_row(0)
        arrived(kv_buf.at[kv_slot(2, 0)], x_sem.at[2])
        to_column(2)

    def all_but(mine, ref, sem):
        pl.when(mine)(lambda: arrived(ref.at[pl.ds(0, 15)], sem))
        pl.when(jnp.logical_not(mine))(lambda: arrived(ref, sem))

    all_but(primary, q_all, q_sem.at[1])
    each_group(set_heads)
    secondary_waits((0,))
    attend_row(0)

    @pl.when(primary)
    def _():
        from_row(1)
        from_row(3)
        from_row(2)

    run("keys1")
    secondary_waits((1, 3))
    attend_row(1)
    ow_pass(0)

    @pl.when(primary)
    def _():
        for d in (0, 1, 3, 2):
            from_far(d)

    run("keys2")
    attend_row(3)
    run("att1")
    secondary_waits((2,))
    attend_row(2)
    each_group(join_rows)

    def m_copy(dx, dz):
        return remote(
            mix_out.at[xz(dx, dz)], mix_all.at[mix_block, y_odd * 4 + x], m_sem.at[0],
            m_sem.at[1], {"sp": xz(dx, dz), "tp": mix_y * 2 + c},
        )

    def each_mixed(act):
        for dz in range(4):
            for dx in range(4):
                if (dx, dz) == (0, 0):
                    pl.when(jnp.logical_not(holds_own))(lambda: act(m_copy(dx, dz)))
                else:
                    act(m_copy(dx, dz))

    each_mixed(lambda copy: copy.start())

    @pl.when(holds_own)
    def _():
        mix_all[mix_block, y_odd * 4 + x] = mix_out[s]

    run("mix1")
    ow_pass(1)
    run("mix2")
    all_but(holds_own, mix_out, m_sem.at[1])
    arrived(outw.at[pl.ds(0, 4)], ow_sem.at[4])
    arrived(res_buf, load_sem.at[4])

    mixed = jnp.concatenate([mix_all[:, unit].reshape(64, 128) for unit in range(8)], axis=1)

    def ex_copy(n):
        columns = pl.ds(n * 512, 512)
        return remote(
            ex_out.at[:, columns], ex_in.at[:, columns], ex_sem.at[0], ex_sem.at[1],
            {"sp": s, "tp": (3 - y) * 2 + c},
        )

    for n in range(4):
        columns = slice(n * 512, n * 512 + 512)
        sums = jnp.dot(mixed, outw[:, :, columns].reshape(1024, 512), preferred_element_type=F32)
        att_buf[:, columns] = sums[:32]
        ex_out[:, columns] = sums[32:].astype(BF16)
        ex_copy(n).start()
    run("mix3")
    arrived(ex_in, ex_sem.at[1])
    updated = res_buf[...].astype(F32) + (att_buf[...] + ex_in[...].astype(F32))
    upd_buf[...] = updated
    scale = lax.rsqrt(jnp.mean(updated * updated, axis=-1, keepdims=True) + 1e-06)
    norm_buf[t] = (updated * scale * gain_ref[...]).astype(BF16)

    def row_copy(ref, target, k):
        return remote(ref, ref, row_sem.at[7], row_sem.at[k if k < 6 else 6], neighbour[target])

    def half_rows(dy, k, core=None):
        slot = y_at(dy) * 2 + (c if core is None else core)
        return norm_buf.at[slot, pl.ds(16 * k, 16)]

    def row_send_to(ref, target, k):
        row_copy(ref, target, k).start()

    row_send_to(half_rows(0, 0), ("y", 1), 0)
    row_send_to(half_rows(0, 1), ("y", -1), 1)
    row_send_to(half_rows(0, 1), ("y", 1), 2)
    row_send_to(half_rows(0, 0), ("y", -1), 3)
    row_send_to(norm_buf.at[t], "pair", 6)
    run("rows0")
    arrived(half_rows(-1, 0), row_sem.at[0])
    row_send_to(half_rows(-1, 0), ("y", 1), 4)
    arrived(half_rows(1, 1), row_sem.at[1])
    row_send_to(half_rows(1, 1), ("y", -1), 5)
    row_send_to(half_rows(-1, 0), "pair", 7)
    row_send_to(half_rows(1, 1), "pair", 8)
    run("rows1")
    arrived(half_rows(-1, 1), row_sem.at[2])
    row_send_to(half_rows(-1, 1), "pair", 9)
    arrived(half_rows(1, 0), row_sem.at[3])
    row_send_to(half_rows(1, 0), "pair", 10)
    run("rows2")
    arrived(half_rows(2, 0), row_sem.at[4])
    row_send_to(half_rows(2, 0), "pair", 11)
    arrived(half_rows(2, 1), row_sem.at[5])
    row_send_to(half_rows(2, 1), "pair", 12)
    arrived(norm_buf.at[pl.ds(0, 4)], row_sem.at[6])
    run("up")
    @pl.loop(0, 4)
    def _(n):
        columns = pl.ds(pl.multiple_of(n * 256, 256), 256)
        rows = norm_buf[...].reshape(256, 2048)
        pre = jnp.maximum(jnp.dot(rows, up_buf[:, columns], preferred_element_type=F32), 0.0)
        hidden_buf[:, columns] = (pre * pre).astype(BF16)

    def cols(r):
        return pl.ds(r * 512, 512)

    def pair_copy(r):
        return remote(
            part_buf.at[1 - c, :, :, cols(r)], pair_buf.at[:, :, cols(r)], y_send.at[0], pair_sem.at[r],
            neighbour["pair"],
        )

    def last_copy(r, k):
        return remote(
            last_out.at[k, :, cols(r)], last_in.at[k, :, cols(r)], y_send.at[1], last_sem.at[r],
            neighbour["y", (2, 1, -1)[k]],
        )

    def store_part(value, columns, width):
        blocks = value.reshape(4, 2, 32, width)
        for core in range(2):
            for yy in range(4):
                part_buf[core, yy, :, columns] = blocks[yy, core].astype(BF16)

    def pair_sum(r, dy):
        yy = y_at(dy)
        return part_buf[c, yy, :, cols(r)].astype(F32) + pair_buf[yy, :, cols(r)].astype(F32)

    def pair_step(r):
        pair_copy(r).wait_recv()
        for k, dy in enumerate((2, 1, -1)):
            last_out[k, :, cols(r)] = pair_sum(r, dy).astype(BF16)
            last_copy(r, k).start()

    def last_step(r):
        total = pair_sum(r, 0)
        arrived(last_in.at[:, :, cols(r)], last_sem.at[r])
        for k in range(3):
            total = total + last_in[k, :, cols(r)].astype(F32)
        return total

    def mixer_sums(r, dz):
        zz = lax.rem(z - dz + 4, 4)
        for pair in range(2):
            slot = zz * 4 + pair * 2
            w = jnp.concatenate([down_buf[slot], down_buf[slot + 1]], axis=1)
            value = jnp.dot(hidden_buf[...], w, preferred_element_type=F32)
            store_part(value, pl.ds(r * 512 + pair * 256, 256), 256)
        pair_copy(r).start()

    def finish(r, dz):
        columns = pl.ds(pl.multiple_of(lax.rem(z - dz + 4, 4) * 512, 512), 512)
        out_buf[:, columns] = (upd_buf[:, columns] + last_step(r)).astype(BF16)
        pltpu.make_async_copy(out_buf.at[:, columns], out_hbm.at[:, columns], out_sem.at[0]).start()

    rounds = tuple(enumerate(ROW_ORDER))
    for i, (r, dz) in enumerate(rounds):
        run(("row", dz))
        mixer_sums(r, dz)
        if i >= 1:
            pair_step(r - 1)
    pair_step(3)
    for r, dz in rounds:
        finish(r, dz)

    arrived(pair_buf, y_send.at[0])
    arrived(last_out, y_send.at[1])
    arrived(norm_buf.at[pl.ds(0, 7)], row_sem.at[7])
    arrived(outw.at[pl.ds(0, 2)], ow_sem.at[2])
    arrived(outw.at[pl.ds(0, 4)], ow_sem.at[3])
    arrived(ex_out, ex_sem.at[0])
    all_but(primary, q_all, q_sem.at[0])
    all_but(holds_own, mix_out, m_sem.at[0])
    for g, ref in enumerate((up_buf.at[pl.ds(0, 1920)], down_buf.at[pl.ds(0, 15)])):
        arrived(ref, send_sem.at[g])

    @pl.when(primary)
    def _():
        arrived(kv_buf.at[pl.ds(0, 12)], kv_send.at[0])
        arrived(kv_buf, kv_send.at[1])

    pltpu.make_async_copy(out_buf, out_hbm, out_sem.at[0]).wait()


def local(qn, kn, vn, qb, kb, vb, offn, offb, res, on, ob, gain, up, down):
    hbm = pl.BlockSpec(memory_space=pl.ANY)
    vmem = pl.BlockSpec(memory_space=pltpu.VMEM)
    dma = pltpu.SemaphoreType.DMA
    return pl.pallas_call(
        body,
        out_shape=jax.ShapeDtypeStruct((32, 2048), BF16),
        in_specs=[hbm, hbm, hbm, hbm, hbm, hbm, vmem, vmem, hbm, hbm, hbm, vmem, hbm, hbm],
        out_specs=hbm,
        scratch_shapes=[
            pltpu.VMEM((2, KV_ROWS, 128), BF16),
            pltpu.VMEM((16, KV_ROWS, 128), BF16),
            pltpu.VMEM((2048, 1024), BF16),
            pltpu.VMEM((16, 1024, 128), BF16),
            pltpu.VMEM((8, 128, 2048), BF16),
            pltpu.VMEM((2, 256, 128), BF16),
            pltpu.VMEM((16, 32, 128), BF16),
            pltpu.VMEM((2, 512, 128), BF16),
            pltpu.VMEM((4, 2, 512, 128), F32),
            pltpu.VMEM((4, 512, 128), F32),
            pltpu.VMEM((256, 256), BF16),
            pltpu.VMEM((16, 32, 128), BF16),
            pltpu.VMEM((2, 8, 32, 128), BF16),
            pltpu.VMEM((32, 2048), BF16),
            pltpu.VMEM((32, 2048), F32),
            pltpu.VMEM((32, 2048), BF16),
            pltpu.VMEM((32, 2048), BF16),
            pltpu.VMEM((2, 4, 32, 2048), BF16),
            pltpu.VMEM((4, 32, 2048), BF16),
            pltpu.VMEM((3, 32, 2048), BF16),
            pltpu.VMEM((3, 32, 2048), BF16),
            pltpu.VMEM((32, 2048), F32),
            pltpu.VMEM((8, 32, 2048), BF16),
            pltpu.VMEM((256, 1024), BF16),
            pltpu.VMEM((32, 2048), BF16),
            dma((7,)),
            dma((2, 4, 16)),
            dma((2,)),
            dma((4,)),
            dma((2,)),
            dma((4, 2)),
            dma((4, 2)),
            dma((2,)),
            dma((4,)),
            dma((2,)),
            dma((2,)),
            dma((5,)),
            dma((2,)),
            dma((4,)),
            dma((4,)),
            dma((8,)),
            dma((2,)),
            dma((1,)),
        ],
        compiler_params=pltpu.CompilerParams(
            collective_id=0, has_side_effects=True, vmem_limit_bytes=60 * 1024 * 1024
        ),
    )(qn, kn, vn, qb, kb, vb, offn, offb, res, on, ob, gain.reshape(1, 2048), up, down)


def solution(mesh):
    return jax.shard_map(
        local,
        mesh=mesh,
        in_specs=(
            P("sp", "tp"), P("sp", "tp"), P("sp", "tp"), P("sp", "tp"), P("sp", "tp"), P("sp", "tp"),
            P("tp", "sp"), P("tp", "sp"), P(("sp", "tp"), None), P("tp", None), P("tp", None), P(),
            P("sp", "tp"), P("tp", "sp"),
        ),
        out_specs=P(("sp", "tp"), None),
        check_vma=False,
    )
```

```python
import functools

import jax
import jax.numpy as jnp
from jax import lax
from jax.experimental import pallas as pl
from jax.experimental.pallas import tpu as pltpu
from jax.sharding import PartitionSpec as P

MESH = pl.DeviceIdType.MESH
LOG2E = 1.4426950408889634
F32 = jnp.float32
BF16 = jnp.bfloat16

OFF, VAL, KV_ROWS = 256, 272, 528


def children(q, dx, dz):
    first, second = (dx, dz) if q < 2 else (dz, dx)
    a, b = ("x", "z") if q < 2 else ("z", "x")
    odd = q % 2
    out = []

    def node(f, s):
        return (f, s) if q < 2 else (s, f)

    if second == 0:
        if first == 0:
            out += [(a, 1, *node(1, 0)), (a, -1, *node(3, 0))]
        elif first == 1 and odd == 0:
            out += [(a, 1, *node(2, 0))]
        elif first == 3 and odd == 1:
            out += [(a, -1, *node(2, 0))]
    if second == 0:
        out += [(b, 1, *node(first, 1)), (b, -1, *node(first, 3))]
    elif second == 1 and odd == 0:
        out += [(b, 1, *node(first, 2))]
    elif second == 3 and odd == 1:
        out += [(b, -1, *node(first, 2))]
    return out


WIRE, DELAY = 5.4, 2.2
POINTS = (
    ("first", 0.3, 4.0),
    ("sides", 2.8, 14.0),
    ("keys1", 15.5, 20.0),
    ("keys2", 19.0, 22.5),
    ("att1", 22.3, 24.5),
    ("mix1", 27.5, 32.5),
    ("mix2", 29.5, 35.5),
    ("mix3", 34.5, 40.5),
    ("rows0", 37.5, 42.5),
    ("rows1", 41.0, 45.5),
    ("rows2", 42.5, 49.5),
)
KEYS_END = 15.0
SIZES = ((16, 16, 48, 48), (336, 336, 176, 176))
STARTS = ((0, 16, 32, 80), (0, 336, 672, 848))


def plan():
    free = {(axis, step): 1.5 for axis in "xz" for step in (1, -1)}
    landing, backlog, steps = {}, [], {}
    left = {(g, dz): 12 if dz == 0 else 16 for g in range(2) for dz in range(4)}

    def offer(g, q, child):
        first = (child[0] == "x") == (q < 2)
        backlog.append((g, 0 if first else 1, len(backlog), q, child))

    def issue(now, out, until, axes=("x", "z")):
        for entry in sorted(backlog):
            g, _, _, q, child = entry
            axis, step, dx, dz = child
            if axis in axes and free[axis, step] <= until:
                start = max(now, free[axis, step])
                free[axis, step] = start + WIRE * SIZES[g][q] / sum(SIZES[g])
                landing[g, q, dx, dz] = free[axis, step] + DELAY
                out.append(("send", g, q, child))
                backlog.remove(entry)

    def take(out, event):
        g, q, dx, dz = event
        del landing[event]
        left[g, dz] -= 1
        out.append(("wait", g, q, (dx, dz)))
        for child in children(q, dx, dz):
            offer(g, q, child)

    for g in range(2):
        for q in range(4):
            for child in children(q, 0, 0):
                offer(g, q, child)
    for point, now, until in POINTS:
        out = []
        axes = {"first": ("z",), "sides": ("x",)}.get(point, ("x", "z"))
        for when, event in sorted((when, event) for event, when in landing.items()):
            if when <= now - 0.3:
                take(out, event)
        issue(now, out, until, axes)
        if point == "first":
            free["z", 1] = free["z", -1] = KEYS_END
        steps[point] = out
    order, out = [], []
    while landing or backlog:
        when, event = min((when, event) for event, when in landing.items())
        now = max(now, when)
        take(out, event)
        issue(now, out, now + 6.0)
        if not any(left[0, dz] for dz in range(4)) and "up" not in steps:
            steps["up"] = out
            out = []
        for dz in range(4):
            if "up" in steps and not left[1, dz] and dz not in order:
                order.append(dz)
                steps["row", dz] = out
                out = []
    return steps, order, now


PLAN, ROW_ORDER, PLAN_END = plan()


def body(
    qn_hbm, kn_hbm, vn_hbm, qb_hbm, kb_hbm, vb_hbm, offn_ref, offb_ref, res_hbm,
    on_hbm, ob_hbm, gain_ref, up_hbm, down_hbm, out_hbm,
    stage, kv_buf, up_buf, down_buf, outw, q_own, q_all, head_buf, kept_buf, acc_buf, tri_buf,
    mix_out, mix_all, res_buf, att_buf, ex_out, ex_in, part_buf, pair_buf, last_out, last_in,
    upd_buf, norm_buf, hidden_buf, out_buf,
    load_sem, recv_sem, send_sem, x_sem, x_send, z_sem, far_sem, kv_send, kvp_sem,
    q_sem, m_sem, ow_sem, ex_sem, pair_sem, last_sem, row_sem, y_send, out_sem,
):
    s = lax.axis_index("sp")
    t = lax.axis_index("tp")
    x, z = lax.rem(s, 4), lax.div(s, 4)
    c, y = lax.rem(t, 2), lax.div(t, 2)
    part = z * 2 + c
    primary = lax.rem(x, 2) == c
    y_odd = lax.rem(y, 2)
    y_mate = y + 1 - 2 * y_odd
    same_pair = lax.div(z, 2) == lax.div(y, 2)
    mix_y = jnp.where(same_pair, z, 3 - z)
    mix_block = jnp.where(same_pair, jnp.int32(0), jnp.int32(1))
    holds_own = mix_y == y

    def xz(dx, dz):
        return lax.rem(z + dz % 4, 4) * 4 + lax.rem(x + dx % 4, 4)

    def y_at(dy):
        return lax.rem(y + dy + 4, 4)

    def z_at(dz):
        return lax.rem(z + dz + 4, 4)

    neighbour = {
        ("x", 1): {"sp": xz(1, 0), "tp": t},
        ("x", -1): {"sp": xz(-1, 0), "tp": t},
        ("z", 1): {"sp": xz(0, 1), "tp": t},
        ("z", -1): {"sp": xz(0, -1), "tp": t},
        "pair": {"sp": s, "tp": y * 2 + (1 - c)},
        ("y", 1): {"sp": s, "tp": y_at(1) * 2 + c},
        ("y", -1): {"sp": s, "tp": y_at(-1) * 2 + c},
        ("y", 2): {"sp": s, "tp": y_at(2) * 2 + c},
    }

    def remote(src, dst, send, recv, target):
        return pltpu.make_async_remote_copy(
            src_ref=src, dst_ref=dst, send_sem=send, recv_sem=recv, device_id=target, device_id_type=MESH
        )

    def arrived(ref, sem):
        pltpu.make_async_copy(ref, ref, sem).wait()

    own = pl.multiple_of(s * 128, 128)
    loads = [
        (kn_hbm, stage.at[0, pl.ds(0, 256)]),
        (vn_hbm, stage.at[0, pl.ds(VAL, 256)]),
        (kb_hbm, stage.at[1, pl.ds(0, 256)]),
        (vb_hbm, stage.at[1, pl.ds(VAL, 256)]),
        (qn_hbm, q_own.at[0]),
        (qb_hbm, q_own.at[1]),
        (on_hbm, outw.at[y_odd * 4 + c]),
        (ob_hbm, outw.at[y_odd * 4 + 2 + c]),
        (up_hbm, up_buf.at[pl.ds(own, 128)]),
        (down_hbm, down_buf.at[s]),
        (res_hbm, res_buf),
    ]
    groups = (0, 0, 0, 0, 1, 1, 2, 2, 3, 3, 4)
    loads = [pltpu.make_async_copy(a, b, load_sem.at[k]) for k, (a, b) in zip(groups, loads)]
    for copy in loads:
        copy.start()

    mine = [
        [
            pltpu.make_async_copy(k_hbm, kv_buf.at[s, pl.ds(0, 256)], load_sem.at[5]),
            pltpu.make_async_copy(v_hbm, kv_buf.at[s, pl.ds(VAL, 256)], load_sem.at[5]),
            pltpu.make_async_copy(q_hbm.at[pl.ds(pl.multiple_of(part * 32, 32), 32)], q_all.at[s], load_sem.at[6]),
        ]
        for k_hbm, v_hbm, q_hbm in ((kn_hbm, vn_hbm, qn_hbm), (kb_hbm, vb_hbm, qb_hbm))
    ]
    for unit in range(2):

        @pl.when(x == c + 2 * unit)
        def _():
            for copy in mine[unit]:
                copy.start()

    def greet(target, unless=None):
        def signal():
            pl.semaphore_signal(barrier, inc=1, device_id=target, device_id_type=MESH)

        if unless is None:
            signal()
        else:
            pl.when(jnp.logical_not(unless))(signal)

    barrier = pltpu.get_barrier_semaphore()
    for target in neighbour.values():
        greet(target)
    for dz in range(4):
        for dx in range(4):
            here = (dx, dz) == (0, 0)
            greet({"sp": xz(dx, dz), "tp": y * 2 + lax.rem(x, 2)}, primary if here else None)
    for block, rows_z in enumerate((y, 3 - y)):
        for plane in (y, y_mate):
            for dx in range(4):
                here = dx == 0 and plane is y
                greet(
                    {"sp": rows_z * 4 + lax.rem(x + dx, 4), "tp": plane * 2 + c},
                    rows_z == z if here else None,
                )

    offn = offn_ref[...].astype(F32)
    offb = offb_ref[...].astype(F32)
    blank = jnp.zeros((14, 128), F32)
    narrow_rows = [offn[0:1, :128], offn[0:1, 128:], offn[1:2, :128], offn[1:2, 128:], blank[:12]]
    broad_rows = [offb[0:1, :128], offb[0:1, 128:], blank]
    for unit, rows in enumerate((narrow_rows, broad_rows)):
        value = jnp.concatenate(rows, axis=0).astype(BF16)
        stage[unit, OFF : OFF + 16, :] = value

        @pl.when(x == c + 2 * unit)
        def _():
            kv_buf[s, OFF : OFF + 16, :] = value

    later = lax.broadcasted_iota(jnp.int32, (256, 256), 0)
    earlier = lax.broadcasted_iota(jnp.int32, (256, 256), 1)
    tri_buf[...] = jnp.where(later >= earlier, 1.0, 0.0).astype(BF16)
    acc_buf[...] = jnp.zeros_like(acc_buf)
    kept_buf[...] = jnp.zeros_like(kept_buf)
    one, none = jnp.int32(1), jnp.int32(0)
    pl.semaphore_wait(barrier, 40 - jnp.where(primary, one, none) - jnp.where(holds_own, one, none))

    def piece(g, slot, q):
        if g == 0:
            return up_buf.at[pl.ds(pl.multiple_of(slot * 128 + STARTS[0][q], 16), SIZES[0][q])]
        return down_buf.at[slot, pl.ds(STARTS[1][q], SIZES[1][q])]

    def send(g, slot, q, axis, step, dx, dz):
        ref = piece(g, slot, q)
        remote(ref, ref, send_sem.at[g], recv_sem.at[g, q, dz * 4 + dx - 1], neighbour[axis, step]).start()

    def run(point):
        for kind, g, q, what in PLAN[point]:
            if kind == "send":
                axis, step, dx, dz = what
                here = (dx - step, dz) if axis == "x" else (dx, dz - step)
                send(g, xz(-here[0], -here[1]), q, axis, step, dx, dz)
            else:
                dx, dz = what
                arrived(piece(g, xz(-dx, -dz), q), recv_sem.at[g, q, dz * 4 + dx - 1])

    arrived(head_buf, load_sem.at[0])

    def x_copy(unit):
        col = c + 2 * unit
        return remote(
            stage.at[unit], kv_buf.at[s], x_send.at[unit], x_sem.at[lax.rem(x - col + 4, 4)],
            {"sp": z * 4 + col, "tp": t},
        )

    for unit in range(2):

        @pl.when(x != c + 2 * unit)
        def _():
            x_copy(unit).start()

    def kv_slot(d, dz):
        return xz(d, -dz)

    def to_column(d):
        ref = kv_buf.at[kv_slot(d, 0)]
        remote(ref, ref, kv_send.at[0], z_sem.at[d, 0], neighbour["z", 1]).start()
        remote(ref, ref, kv_send.at[0], z_sem.at[d, 1], neighbour["z", -1]).start()
        remote(ref, ref, kv_send.at[1], kvp_sem.at[0], neighbour["pair"]).start()

    def from_row(d):
        for k, dz in ((0, 1), (1, 3)):
            slot = kv_slot(d, dz)
            ref = kv_buf.at[slot]
            arrived(ref, z_sem.at[d, k])
            half = kv_buf.at[slot, pl.ds(0, VAL) if k == 0 else pl.ds(VAL, 256)]
            remote(half, half, kv_send.at[0], far_sem.at[d, k], neighbour["z", 1 if k == 0 else -1]).start()
            remote(ref, ref, kv_send.at[1], kvp_sem.at[dz], neighbour["pair"]).start()

    def far_half(d, k):
        return kv_buf.at[kv_slot(d, 2), pl.ds(0, VAL) if k == 0 else pl.ds(VAL, 256)]

    def from_far(d):
        for k in range(2):
            half = far_half(d, k)
            arrived(half, far_sem.at[d, k])
            remote(half, half, kv_send.at[1], kvp_sem.at[2], neighbour["pair"]).start()

    @pl.when(primary)
    def _():
        arrived(q_own, load_sem.at[5])
        arrived(q_all.at[s], load_sem.at[6])
        to_column(0)

    arrived(q_own, load_sem.at[1])
    arrived(outw.at[pl.ds(0, 2)], load_sem.at[2])

    def q_copy(unit, dz, dc):
        core = c if dc == 0 else 1 - c
        rows = pl.ds(pl.multiple_of((z_at(dz) * 2 + core) * 32, 32), 32)
        return remote(
            q_own.at[unit, rows], q_all.at[s], q_sem.at[0], q_sem.at[1],
            {"sp": z_at(dz) * 4 + c + 2 * unit, "tp": y * 2 + core},
        )

    def each_query(act):
        for unit in range(2):
            for dz in range(4):
                for dc in range(2):
                    if (dz, dc) == (0, 0):
                        pl.when(x != c + 2 * unit)(lambda: act(q_copy(unit, dz, dc)))
                    else:
                        act(q_copy(unit, dz, dc))

    each_query(lambda copy: copy.start())

    def ow(k, foreign, core):
        plane = 1 - y_odd if foreign else y_odd
        return outw.at[plane * 4 + core + 2 * k]

    mate = {"sp": s, "tp": y_mate * 2 + c}

    def ow_copy(k):
        return remote(ow(k, 0, c), ow(k, 0, c), ow_sem.at[2], ow_sem.at[k], mate)

    def ow_pair(k, foreign):
        ref = ow(k, foreign, c)
        return remote(ref, ref, ow_sem.at[3], ow_sem.at[4], neighbour["pair"])

    for copy in (ow_copy(0), ow_copy(1), ow_pair(0, 0), ow_pair(1, 0)):
        copy.start()

    def ow_pass(k):
        arrived(ow(k, 1, c), ow_sem.at[k])
        ow_pair(k, 1).start()

    arrived(outw.at[0], load_sem.at[3])
    run("first")
    for unit in range(2):
        pl.when(x != c + 2 * unit)(lambda: x_copy(unit).wait_send())
    run("sides")

    lane = lax.broadcasted_iota(jnp.int32, (512, 128), 1)
    zero = jnp.zeros((), BF16)
    ahead = (later // 32) * 256 + lax.rem(later, 32) - earlier + part * 32

    def attend(slot, zz, heads, chunks, scale):
        offs = kv_buf[slot, OFF:VAL, :].astype(F32) * LOG2E
        k = kv_buf[slot, pl.ds(0, 256), :]
        v = kv_buf[slot, pl.ds(VAL, 256), :]
        items = [(chunk, masked, h) for chunk, masked in chunks for h in range(heads)]
        scores, gone, weights = [], [], []
        for chunk, masked, h in items:
            product = lax.dot_general(
                head_buf[h, chunk * 256 : chunk * 256 + 256], k, (((1,), (1,)), ((), ())),
                preferred_element_type=F32,
            )
            off = jnp.concatenate([offs[2 * h : 2 * h + 1], offs[2 * h + 1 : 2 * h + 2]], axis=1)
            scores.append(product * scale + off)
        for (chunk, masked, h), score in zip(items, scores):
            drop = jnp.maximum(score, lax.log2(1.0 + lax.exp2(jnp.minimum(score, 126.0))))
            if masked:
                drop = jnp.where(ahead > slot * 256 - chunk * 2048, drop, 0.0)
            gone.append(jnp.dot(drop.astype(BF16), tri_buf[...], preferred_element_type=F32))
        for (chunk, masked, h), score, lost in zip(items, scores, gone):
            rows = slice(chunk * 256, chunk * 256 + 256)
            kept = kept_buf[zz, h, rows]
            weight = lax.exp2(score - lost - jnp.concatenate([kept, kept], axis=1))
            if masked:
                weight = jnp.where(ahead > slot * 256 - chunk * 2048, weight, 0.0)
            kept_buf[zz, h, rows] = kept + jnp.broadcast_to(lost[:, 0:1], (256, 128))
            weights.append(weight.astype(BF16))
        for chunk, _ in chunks:
            rows = slice(chunk * 256, chunk * 256 + 256)
            total = acc_buf[zz, rows]
            for (other, _, h), weight in zip(items, weights):
                if other == chunk:
                    values = v
                    if heads == 2:
                        values = jnp.where((lane[:256] < 64) if h == 0 else (lane[:256] >= 64), v, zero)
                    total = total + jnp.dot(weight, values, preferred_element_type=F32)
            acc_buf[zz, rows] = total

    def each_group(act):
        pl.when(x < 2)(lambda: act(2, LOG2E * 64**-0.5))
        pl.when(x >= 2)(lambda: act(1, LOG2E * 128**-0.5))

    def set_heads(heads, scale):
        queries = q_all[...].reshape(512, 128)
        if heads == 2:
            head_buf[0] = jnp.where(lane < 64, queries, zero)
            head_buf[1] = jnp.where(lane >= 64, queries, zero)
        else:
            head_buf[0] = queries

    def attend_row(dz):
        zz = z_at(-dz)

        def act(heads, scale):
            for near, chunks in ((True, ((1, True),)), (False, ((0, True), (1, False)))):

                @pl.when((zz >= 2) if near else (zz < 2))
                def _():
                    pl.loop(0, 4)(lambda k: attend(zz * 4 + 3 - k, zz, heads, chunks, scale))

        each_group(act)

    def join_rows(heads, scale):
        total, past = acc_buf[3], None
        for zz in (2, 1, 0):
            kept = kept_buf[zz + 1, 0]
            if heads == 2:
                kept = jnp.where(lane < 64, kept, kept_buf[zz + 1, 1])
            past = kept if past is None else past + kept
            total = total + acc_buf[zz] * lax.exp2(-past)
        mix_out[...] = total.reshape(16, 32, 128).astype(BF16)

    def secondary_waits(rows):
        @pl.when(jnp.logical_not(primary))
        def _():
            for dz in rows:
                arrived(kv_buf.at[pl.ds(pl.multiple_of(z_at(-dz) * 4, 4), 4)], kvp_sem.at[dz])

    @pl.when(primary)
    def _():
        for d in (1, 3):
            arrived(kv_buf.at[kv_slot(d, 0)], x_sem.at[d])
            to_column(d)
        from_row(0)
        arrived(kv_buf.at[kv_slot(2, 0)], x_sem.at[2])
        to_column(2)

    def all_but(mine, ref, sem):
        pl.when(mine)(lambda: arrived(ref.at[pl.ds(0, 15)], sem))
        pl.when(jnp.logical_not(mine))(lambda: arrived(ref, sem))

    all_but(primary, q_all, q_sem.at[1])
    each_group(set_heads)
    secondary_waits((0,))
    attend_row(0)

    @pl.when(primary)
    def _():
        from_row(1)
        from_row(3)
        from_row(2)

    run("keys1")
    secondary_waits((1, 3))
    attend_row(1)
    ow_pass(0)

    @pl.when(primary)
    def _():
        for d in (0, 1, 3, 2):
            from_far(d)

    run("keys2")
    attend_row(3)
    run("att1")
    secondary_waits((2,))
    attend_row(2)
    each_group(join_rows)

    def m_copy(dx, dz):
        return remote(
            mix_out.at[xz(dx, dz)], mix_all.at[mix_block, y_odd * 4 + x], m_sem.at[0],
            m_sem.at[1], {"sp": xz(dx, dz), "tp": mix_y * 2 + c},
        )

    def each_mixed(act):
        for dz in range(4):
            for dx in range(4):
                if (dx, dz) == (0, 0):
                    pl.when(jnp.logical_not(holds_own))(lambda: act(m_copy(dx, dz)))
                else:
                    act(m_copy(dx, dz))

    each_mixed(lambda copy: copy.start())

    @pl.when(holds_own)
    def _():
        mix_all[mix_block, y_odd * 4 + x] = mix_out[s]

    run("mix1")
    ow_pass(1)
    run("mix2")
    all_but(holds_own, mix_out, m_sem.at[1])
    arrived(outw.at[pl.ds(0, 4)], ow_sem.at[4])
    arrived(res_buf, load_sem.at[4])

    mixed = jnp.concatenate([mix_all[:, unit].reshape(64, 128) for unit in range(8)], axis=1)

    def ex_copy(n):
        columns = pl.ds(n * 512, 512)
        return remote(
            ex_out.at[:, columns], ex_in.at[:, columns], ex_sem.at[0], ex_sem.at[1],
            {"sp": s, "tp": (3 - y) * 2 + c},
        )

    for n in range(4):
        columns = slice(n * 512, n * 512 + 512)
        sums = jnp.dot(mixed, outw[:, :, columns].reshape(1024, 512), preferred_element_type=F32)
        att_buf[:, columns] = sums[:32]
        ex_out[:, columns] = sums[32:].astype(BF16)
        ex_copy(n).start()
    run("mix3")
    arrived(ex_in, ex_sem.at[1])
    updated = res_buf[...].astype(F32) + (att_buf[...] + ex_in[...].astype(F32))
    upd_buf[...] = updated
    scale = lax.rsqrt(jnp.mean(updated * updated, axis=-1, keepdims=True) + 1e-06)
    norm_buf[t] = (updated * scale * gain_ref[...]).astype(BF16)

    def row_copy(ref, target, k):
        return remote(ref, ref, row_sem.at[7], row_sem.at[k if k < 6 else 6], neighbour[target])

    def half_rows(dy, k, core=None):
        slot = y_at(dy) * 2 + (c if core is None else core)
        return norm_buf.at[slot, pl.ds(16 * k, 16)]

    def row_send_to(ref, target, k):
        row_copy(ref, target, k).start()

    row_send_to(half_rows(0, 0), ("y", 1), 0)
    row_send_to(half_rows(0, 1), ("y", -1), 1)
    row_send_to(half_rows(0, 1), ("y", 1), 2)
    row_send_to(half_rows(0, 0), ("y", -1), 3)
    row_send_to(norm_buf.at[t], "pair", 6)
    run("rows0")
    arrived(half_rows(-1, 0), row_sem.at[0])
    row_send_to(half_rows(-1, 0), ("y", 1), 4)
    arrived(half_rows(1, 1), row_sem.at[1])
    row_send_to(half_rows(1, 1), ("y", -1), 5)
    row_send_to(half_rows(-1, 0), "pair", 7)
    row_send_to(half_rows(1, 1), "pair", 8)
    run("rows1")
    arrived(half_rows(-1, 1), row_sem.at[2])
    row_send_to(half_rows(-1, 1), "pair", 9)
    arrived(half_rows(1, 0), row_sem.at[3])
    row_send_to(half_rows(1, 0), "pair", 10)
    run("rows2")
    arrived(half_rows(2, 0), row_sem.at[4])
    row_send_to(half_rows(2, 0), "pair", 11)
    arrived(half_rows(2, 1), row_sem.at[5])
    row_send_to(half_rows(2, 1), "pair", 12)
    arrived(norm_buf.at[pl.ds(0, 4)], row_sem.at[6])
    run("up")
    @pl.loop(0, 4)
    def _(n):
        columns = pl.ds(pl.multiple_of(n * 256, 256), 256)
        rows = norm_buf[...].reshape(256, 2048)
        pre = jnp.maximum(jnp.dot(rows, up_buf[:, columns], preferred_element_type=F32), 0.0)
        hidden_buf[:, columns] = (pre * pre).astype(BF16)

    def cols(r):
        return pl.ds(r * 512, 512)

    def pair_copy(r, half):
        columns = pl.ds(r * 512 + half * 256, 256)
        return remote(
            part_buf.at[1 - c, :, :, columns], pair_buf.at[:, :, columns], y_send.at[0], pair_sem.at[r],
            neighbour["pair"],
        )

    def last_copy(r, k):
        return remote(
            last_out.at[k, :, cols(r)], last_in.at[k, :, cols(r)], y_send.at[1], last_sem.at[r],
            neighbour["y", (2, 1, -1)[k]],
        )

    def store_part(value, columns, width):
        blocks = value.reshape(4, 2, 32, width)
        for core in range(2):
            for yy in range(4):
                part_buf[core, yy, :, columns] = blocks[yy, core].astype(BF16)

    def pair_sum(r, dy):
        yy = y_at(dy)
        return part_buf[c, yy, :, cols(r)].astype(F32) + pair_buf[yy, :, cols(r)].astype(F32)

    def pair_step(r):
        arrived(pair_buf.at[:, :, cols(r)], pair_sem.at[r])
        for k, dy in enumerate((2, 1, -1)):
            last_out[k, :, cols(r)] = pair_sum(r, dy).astype(BF16)
            last_copy(r, k).start()

    def last_step(r):
        total = pair_sum(r, 0)
        arrived(last_in.at[:, :, cols(r)], last_sem.at[r])
        for k in range(3):
            total = total + last_in[k, :, cols(r)].astype(F32)
        return total

    def mixer_sums(r, dz):
        zz = lax.rem(z - dz + 4, 4)
        for pair in range(2):
            slot = zz * 4 + pair * 2
            w = jnp.concatenate([down_buf[slot], down_buf[slot + 1]], axis=1)
            value = jnp.dot(hidden_buf[...], w, preferred_element_type=F32)
            store_part(value, pl.ds(r * 512 + pair * 256, 256), 256)
            pair_copy(r, pair).start()

    def finish(r, dz):
        columns = pl.ds(pl.multiple_of(lax.rem(z - dz + 4, 4) * 512, 512), 512)
        out_buf[:, columns] = (upd_buf[:, columns] + last_step(r)).astype(BF16)
        pltpu.make_async_copy(out_buf.at[:, columns], out_hbm.at[:, columns], out_sem.at[0]).start()

    rounds = tuple(enumerate(ROW_ORDER))
    for i, (r, dz) in enumerate(rounds):
        run(("row", dz))
        mixer_sums(r, dz)
        if i >= 1:
            pair_step(r - 1)
    pair_step(3)
    for r, dz in rounds:
        finish(r, dz)

    arrived(pair_buf, y_send.at[0])
    arrived(last_out, y_send.at[1])
    arrived(norm_buf.at[pl.ds(0, 7)], row_sem.at[7])
    arrived(outw.at[pl.ds(0, 2)], ow_sem.at[2])
    arrived(outw.at[pl.ds(0, 4)], ow_sem.at[3])
    arrived(ex_out, ex_sem.at[0])
    all_but(primary, q_all, q_sem.at[0])
    all_but(holds_own, mix_out, m_sem.at[0])
    for g, ref in enumerate((up_buf.at[pl.ds(0, 1920)], down_buf.at[pl.ds(0, 15)])):
        arrived(ref, send_sem.at[g])

    @pl.when(primary)
    def _():
        arrived(kv_buf.at[pl.ds(0, 12)], kv_send.at[0])
        arrived(kv_buf, kv_send.at[1])

    pltpu.make_async_copy(out_buf, out_hbm, out_sem.at[0]).wait()


def local(qn, kn, vn, qb, kb, vb, offn, offb, res, on, ob, gain, up, down):
    hbm = pl.BlockSpec(memory_space=pl.ANY)
    vmem = pl.BlockSpec(memory_space=pltpu.VMEM)
    dma = pltpu.SemaphoreType.DMA
    return pl.pallas_call(
        body,
        out_shape=jax.ShapeDtypeStruct((32, 2048), BF16),
        in_specs=[hbm, hbm, hbm, hbm, hbm, hbm, vmem, vmem, hbm, hbm, hbm, vmem, hbm, hbm],
        out_specs=hbm,
        scratch_shapes=[
            pltpu.VMEM((2, KV_ROWS, 128), BF16),
            pltpu.VMEM((16, KV_ROWS, 128), BF16),
            pltpu.VMEM((2048, 1024), BF16),
            pltpu.VMEM((16, 1024, 128), BF16),
            pltpu.VMEM((8, 128, 2048), BF16),
            pltpu.VMEM((2, 256, 128), BF16),
            pltpu.VMEM((16, 32, 128), BF16),
            pltpu.VMEM((2, 512, 128), BF16),
            pltpu.VMEM((4, 2, 512, 128), F32),
            pltpu.VMEM((4, 512, 128), F32),
            pltpu.VMEM((256, 256), BF16),
            pltpu.VMEM((16, 32, 128), BF16),
            pltpu.VMEM((2, 8, 32, 128), BF16),
            pltpu.VMEM((32, 2048), BF16),
            pltpu.VMEM((32, 2048), F32),
            pltpu.VMEM((32, 2048), BF16),
            pltpu.VMEM((32, 2048), BF16),
            pltpu.VMEM((2, 4, 32, 2048), BF16),
            pltpu.VMEM((4, 32, 2048), BF16),
            pltpu.VMEM((3, 32, 2048), BF16),
            pltpu.VMEM((3, 32, 2048), BF16),
            pltpu.VMEM((32, 2048), F32),
            pltpu.VMEM((8, 32, 2048), BF16),
            pltpu.VMEM((256, 1024), BF16),
            pltpu.VMEM((32, 2048), BF16),
            dma((7,)),
            dma((2, 4, 15)),
            dma((2,)),
            dma((4,)),
            dma((2,)),
            dma((4, 2)),
            dma((4, 2)),
            dma((2,)),
            dma((4,)),
            dma((2,)),
            dma((2,)),
            dma((5,)),
            dma((2,)),
            dma((4,)),
            dma((4,)),
            dma((8,)),
            dma((2,)),
            dma((1,)),
        ],
        compiler_params=pltpu.CompilerParams(
            collective_id=0, has_side_effects=True, vmem_limit_bytes=60 * 1024 * 1024
        ),
    )(qn, kn, vn, qb, kb, vb, offn, offb, res, on, ob, gain.reshape(1, 2048), up, down)


def solution(mesh):
    return jax.shard_map(
        local,
        mesh=mesh,
        in_specs=(
            P("sp", "tp"), P("sp", "tp"), P("sp", "tp"), P("sp", "tp"), P("sp", "tp"), P("sp", "tp"),
            P("tp", "sp"), P("tp", "sp"), P(("sp", "tp"), None), P("tp", None), P("tp", None), P(),
            P("sp", "tp"), P("tp", "sp"),
        ),
        out_specs=P(("sp", "tp"), None),
        check_vma=False,
    )
```

```python
import functools

import jax
import jax.numpy as jnp
from jax import lax
from jax.experimental import pallas as pl
from jax.experimental.pallas import tpu as pltpu
from jax.sharding import PartitionSpec as P

MESH = pl.DeviceIdType.MESH
LOG2E = 1.4426950408889634
F32 = jnp.float32
BF16 = jnp.bfloat16

OFF, VAL, KV_ROWS = 256, 272, 528


def children(q, dx, dz):
    first, second = (dx, dz) if q < 2 else (dz, dx)
    a, b = ("x", "z") if q < 2 else ("z", "x")
    odd = q % 2
    out = []

    def node(f, s):
        return (f, s) if q < 2 else (s, f)

    if second == 0:
        if first == 0:
            out += [(a, 1, *node(1, 0)), (a, -1, *node(3, 0))]
        elif first == 1 and odd == 0:
            out += [(a, 1, *node(2, 0))]
        elif first == 3 and odd == 1:
            out += [(a, -1, *node(2, 0))]
    if second == 0:
        out += [(b, 1, *node(first, 1)), (b, -1, *node(first, 3))]
    elif second == 1 and odd == 0:
        out += [(b, 1, *node(first, 2))]
    elif second == 3 and odd == 1:
        out += [(b, -1, *node(first, 2))]
    return out


WIRE, DELAY = 5.4, 2.2
POINTS = (
    ("first", 0.3, 4.0),
    ("sides", 2.8, 14.0),
    ("keys1", 15.5, 20.0),
    ("keys2", 19.0, 22.5),
    ("att1", 22.3, 24.5),
    ("mix1", 27.5, 32.5),
    ("mix2", 29.5, 35.5),
    ("mix3", 34.5, 40.5),
    ("rows0", 37.5, 42.5),
    ("rows1", 41.0, 45.5),
    ("rows2", 42.5, 49.5),
)
KEYS_END = 15.0
SIZES = ((16, 16, 48, 48), (336, 336, 176, 176))
STARTS = ((0, 16, 32, 80), (0, 336, 672, 848))


def plan():
    free = {(axis, step): 1.5 for axis in "xz" for step in (1, -1)}
    landing, backlog, steps = {}, [], {}
    left = {(g, dz): 12 if dz == 0 else 16 for g in range(2) for dz in range(4)}

    def offer(g, q, child):
        first = (child[0] == "x") == (q < 2)
        backlog.append((g, 0 if first else 1, len(backlog), q, child))

    def issue(now, out, until, axes=("x", "z")):
        for entry in sorted(backlog):
            g, _, _, q, child = entry
            axis, step, dx, dz = child
            if axis in axes and free[axis, step] <= until:
                start = max(now, free[axis, step])
                free[axis, step] = start + WIRE * SIZES[g][q] / sum(SIZES[g])
                landing[g, q, dx, dz] = free[axis, step] + DELAY
                out.append(("send", g, q, child))
                backlog.remove(entry)

    def take(out, event):
        g, q, dx, dz = event
        del landing[event]
        left[g, dz] -= 1
        out.append(("wait", g, q, (dx, dz)))
        for child in children(q, dx, dz):
            offer(g, q, child)

    for g in range(2):
        for q in range(4):
            for child in children(q, 0, 0):
                offer(g, q, child)
    for point, now, until in POINTS:
        out = []
        axes = {"first": ("z",), "sides": ("x",)}.get(point, ("x", "z"))
        for when, event in sorted((when, event) for event, when in landing.items()):
            if when <= now - 0.3:
                take(out, event)
        issue(now, out, until, axes)
        if point == "first":
            free["z", 1] = free["z", -1] = KEYS_END
        steps[point] = out
    order, out = [], []
    while landing or backlog:
        when, event = min((when, event) for event, when in landing.items())
        now = max(now, when)
        take(out, event)
        issue(now, out, now + 6.0)
        if not any(left[0, dz] for dz in range(4)) and "up" not in steps:
            steps["up"] = out
            out = []
        for dz in range(4):
            if "up" in steps and not left[1, dz] and dz not in order:
                order.append(dz)
                steps["row", dz] = out
                out = []
    return steps, order, now


PLAN, ROW_ORDER, PLAN_END = plan()


def body(
    qn_hbm, kn_hbm, vn_hbm, qb_hbm, kb_hbm, vb_hbm, offn_ref, offb_ref, res_hbm,
    on_hbm, ob_hbm, gain_ref, up_hbm, down_hbm, out_hbm,
    stage, kv_buf, up_buf, down_buf, outw, q_own, q_all, head_buf, kept_buf, acc_buf, tri_buf,
    mix_out, mix_all, res_buf, att_buf, ex_out, ex_in, part_buf, pair_buf, last_out, last_in,
    upd_buf, norm_buf, hidden_buf, out_buf,
    load_sem, recv_sem, send_sem, x_sem, x_send, z_sem, far_sem, kv_send, kvp_sem,
    q_sem, m_sem, ow_sem, ex_sem, pair_sem, last_sem, row_sem, y_send, out_sem,
):
    s = lax.axis_index("sp")
    t = lax.axis_index("tp")
    x, z = lax.rem(s, 4), lax.div(s, 4)
    c, y = lax.rem(t, 2), lax.div(t, 2)
    part = z * 2 + c
    primary = lax.rem(x, 2) == c
    y_odd = lax.rem(y, 2)
    y_mate = y + 1 - 2 * y_odd
    same_pair = lax.div(z, 2) == lax.div(y, 2)
    mix_y = jnp.where(same_pair, z, 3 - z)
    mix_block = jnp.where(same_pair, jnp.int32(0), jnp.int32(1))
    holds_own = mix_y == y

    def xz(dx, dz):
        return lax.rem(z + dz % 4, 4) * 4 + lax.rem(x + dx % 4, 4)

    def y_at(dy):
        return lax.rem(y + dy + 4, 4)

    def z_at(dz):
        return lax.rem(z + dz + 4, 4)

    neighbour = {
        ("x", 1): {"sp": xz(1, 0), "tp": t},
        ("x", -1): {"sp": xz(-1, 0), "tp": t},
        ("z", 1): {"sp": xz(0, 1), "tp": t},
        ("z", -1): {"sp": xz(0, -1), "tp": t},
        "pair": {"sp": s, "tp": y * 2 + (1 - c)},
        ("y", 1): {"sp": s, "tp": y_at(1) * 2 + c},
        ("y", -1): {"sp": s, "tp": y_at(-1) * 2 + c},
        ("y", 2): {"sp": s, "tp": y_at(2) * 2 + c},
    }

    def remote(src, dst, send, recv, target):
        return pltpu.make_async_remote_copy(
            src_ref=src, dst_ref=dst, send_sem=send, recv_sem=recv, device_id=target, device_id_type=MESH
        )

    def arrived(ref, sem):
        pltpu.make_async_copy(ref, ref, sem).wait()

    own = pl.multiple_of(s * 128, 128)
    loads = [
        (kn_hbm, stage.at[0, pl.ds(0, 256)]),
        (vn_hbm, stage.at[0, pl.ds(VAL, 256)]),
        (kb_hbm, stage.at[1, pl.ds(0, 256)]),
        (vb_hbm, stage.at[1, pl.ds(VAL, 256)]),
        (qn_hbm, q_own.at[0]),
        (qb_hbm, q_own.at[1]),
        (on_hbm, outw.at[y_odd * 4 + c]),
        (ob_hbm, outw.at[y_odd * 4 + 2 + c]),
        (up_hbm, up_buf.at[pl.ds(own, 128)]),
        (down_hbm, down_buf.at[s]),
        (res_hbm, res_buf),
    ]
    groups = (0, 0, 0, 0, 1, 1, 2, 2, 3, 3, 4)
    loads = [pltpu.make_async_copy(a, b, load_sem.at[k]) for k, (a, b) in zip(groups, loads)]
    for copy in loads:
        copy.start()

    mine = [
        [
            pltpu.make_async_copy(k_hbm, kv_buf.at[s, pl.ds(0, 256)], load_sem.at[5]),
            pltpu.make_async_copy(v_hbm, kv_buf.at[s, pl.ds(VAL, 256)], load_sem.at[5]),
            pltpu.make_async_copy(q_hbm.at[pl.ds(pl.multiple_of(part * 32, 32), 32)], q_all.at[s], load_sem.at[6]),
        ]
        for k_hbm, v_hbm, q_hbm in ((kn_hbm, vn_hbm, qn_hbm), (kb_hbm, vb_hbm, qb_hbm))
    ]
    for unit in range(2):

        @pl.when(x == c + 2 * unit)
        def _():
            for copy in mine[unit]:
                copy.start()

    def greet(target, unless=None):
        def signal():
            pl.semaphore_signal(barrier, inc=1, device_id=target, device_id_type=MESH)

        if unless is None:
            signal()
        else:
            pl.when(jnp.logical_not(unless))(signal)

    barrier = pltpu.get_barrier_semaphore()
    for target in neighbour.values():
        greet(target)
    for dz in range(4):
        for dx in range(4):
            here = (dx, dz) == (0, 0)
            greet({"sp": xz(dx, dz), "tp": y * 2 + lax.rem(x, 2)}, primary if here else None)
    for block, rows_z in enumerate((y, 3 - y)):
        for plane in (y, y_mate):
            for dx in range(4):
                here = dx == 0 and plane is y
                greet(
                    {"sp": rows_z * 4 + lax.rem(x + dx, 4), "tp": plane * 2 + c},
                    rows_z == z if here else None,
                )

    offn = offn_ref[...].astype(F32)
    offb = offb_ref[...].astype(F32)
    blank = jnp.zeros((14, 128), F32)
    narrow_rows = [offn[0:1, :128], offn[0:1, 128:], offn[1:2, :128], offn[1:2, 128:], blank[:12]]
    broad_rows = [offb[0:1, :128], offb[0:1, 128:], blank]
    for unit, rows in enumerate((narrow_rows, broad_rows)):
        value = jnp.concatenate(rows, axis=0).astype(BF16)
        stage[unit, OFF : OFF + 16, :] = value

        @pl.when(x == c + 2 * unit)
        def _():
            kv_buf[s, OFF : OFF + 16, :] = value

    later = lax.broadcasted_iota(jnp.int32, (256, 256), 0)
    earlier = lax.broadcasted_iota(jnp.int32, (256, 256), 1)
    tri_buf[...] = jnp.where(later >= earlier, 1.0, 0.0).astype(BF16)
    acc_buf[...] = jnp.zeros_like(acc_buf)
    kept_buf[...] = jnp.zeros_like(kept_buf)
    one, none = jnp.int32(1), jnp.int32(0)
    pl.semaphore_wait(barrier, 40 - jnp.where(primary, one, none) - jnp.where(holds_own, one, none))

    def piece(g, slot, q):
        if g == 0:
            return up_buf.at[pl.ds(pl.multiple_of(slot * 128 + STARTS[0][q], 16), SIZES[0][q])]
        return down_buf.at[slot, pl.ds(STARTS[1][q], SIZES[1][q])]

    def send(g, slot, q, axis, step, dx, dz):
        ref = piece(g, slot, q)
        remote(ref, ref, send_sem.at[g], recv_sem.at[g, q, dz * 4 + dx - 1], neighbour[axis, step]).start()

    def run(point):
        for kind, g, q, what in PLAN[point]:
            if kind == "send":
                axis, step, dx, dz = what
                here = (dx - step, dz) if axis == "x" else (dx, dz - step)
                send(g, xz(-here[0], -here[1]), q, axis, step, dx, dz)
            else:
                dx, dz = what
                arrived(piece(g, xz(-dx, -dz), q), recv_sem.at[g, q, dz * 4 + dx - 1])

    arrived(head_buf, load_sem.at[0])

    def x_copy(unit):
        col = c + 2 * unit
        return remote(
            stage.at[unit], kv_buf.at[s], x_send.at[unit], x_sem.at[lax.rem(x - col + 4, 4)],
            {"sp": z * 4 + col, "tp": t},
        )

    for unit in range(2):

        @pl.when(x != c + 2 * unit)
        def _():
            x_copy(unit).start()

    def kv_slot(d, dz):
        return xz(d, -dz)

    def to_column(d):
        ref = kv_buf.at[kv_slot(d, 0)]
        remote(ref, ref, kv_send.at[0], z_sem.at[d, 0], neighbour["z", 1]).start()
        remote(ref, ref, kv_send.at[0], z_sem.at[d, 1], neighbour["z", -1]).start()
        remote(ref, ref, kv_send.at[1], kvp_sem.at[0], neighbour["pair"]).start()

    def from_row(d):
        for k, dz in ((0, 1), (1, 3)):
            slot = kv_slot(d, dz)
            ref = kv_buf.at[slot]
            arrived(ref, z_sem.at[d, k])
            half = kv_buf.at[slot, pl.ds(0, VAL) if k == 0 else pl.ds(VAL, 256)]
            remote(half, half, kv_send.at[0], far_sem.at[d, k], neighbour["z", 1 if k == 0 else -1]).start()
            remote(ref, ref, kv_send.at[1], kvp_sem.at[dz], neighbour["pair"]).start()

    def far_half(d, k):
        return kv_buf.at[kv_slot(d, 2), pl.ds(0, VAL) if k == 0 else pl.ds(VAL, 256)]

    def from_far(d):
        for k in range(2):
            half = far_half(d, k)
            arrived(half, far_sem.at[d, k])
            remote(half, half, kv_send.at[1], kvp_sem.at[2], neighbour["pair"]).start()

    @pl.when(primary)
    def _():
        arrived(q_own, load_sem.at[5])
        arrived(q_all.at[s], load_sem.at[6])
        to_column(0)

    arrived(q_own, load_sem.at[1])
    arrived(outw.at[pl.ds(0, 2)], load_sem.at[2])

    def q_copy(unit, dz, dc):
        core = c if dc == 0 else 1 - c
        rows = pl.ds(pl.multiple_of((z_at(dz) * 2 + core) * 32, 32), 32)
        return remote(
            q_own.at[unit, rows], q_all.at[s], q_sem.at[0], q_sem.at[1],
            {"sp": z_at(dz) * 4 + c + 2 * unit, "tp": y * 2 + core},
        )

    def each_query(act):
        for unit in range(2):
            for dz in range(4):
                for dc in range(2):
                    if (dz, dc) == (0, 0):
                        pl.when(x != c + 2 * unit)(lambda: act(q_copy(unit, dz, dc)))
                    else:
                        act(q_copy(unit, dz, dc))

    each_query(lambda copy: copy.start())

    def ow(k, foreign, core):
        plane = 1 - y_odd if foreign else y_odd
        return outw.at[plane * 4 + core + 2 * k]

    mate = {"sp": s, "tp": y_mate * 2 + c}

    def ow_copy(k):
        return remote(ow(k, 0, c), ow(k, 0, c), ow_sem.at[2], ow_sem.at[k], mate)

    def ow_pair(k, foreign):
        ref = ow(k, foreign, c)
        return remote(ref, ref, ow_sem.at[3], ow_sem.at[4], neighbour["pair"])

    for copy in (ow_copy(0), ow_copy(1), ow_pair(0, 0), ow_pair(1, 0)):
        copy.start()

    def ow_pass(k):
        arrived(ow(k, 1, c), ow_sem.at[k])
        ow_pair(k, 1).start()

    arrived(outw.at[0], load_sem.at[3])
    run("first")
    for unit in range(2):
        pl.when(x != c + 2 * unit)(lambda: x_copy(unit).wait_send())
    run("sides")

    lane = lax.broadcasted_iota(jnp.int32, (512, 128), 1)
    zero = jnp.zeros((), BF16)
    ahead = (later // 32) * 256 + lax.rem(later, 32) - earlier + part * 32

    def attend(slot, zz, heads, chunks, scale):
        offs = kv_buf[slot, OFF:VAL, :].astype(F32) * LOG2E
        k = kv_buf[slot, pl.ds(0, 256), :]
        v = kv_buf[slot, pl.ds(VAL, 256), :]
        items = [(chunk, masked, h) for chunk, masked in chunks for h in range(heads)]
        scores, gone, weights = [], [], []
        for chunk, masked, h in items:
            product = lax.dot_general(
                head_buf[h, chunk * 256 : chunk * 256 + 256], k, (((1,), (1,)), ((), ())),
                preferred_element_type=F32,
            )
            off = jnp.concatenate([offs[2 * h : 2 * h + 1], offs[2 * h + 1 : 2 * h + 2]], axis=1)
            scores.append(product * scale + off)
        for (chunk, masked, h), score in zip(items, scores):
            drop = jnp.maximum(score, lax.log2(1.0 + lax.exp2(jnp.minimum(score, 126.0))))
            if masked:
                drop = jnp.where(ahead > slot * 256 - chunk * 2048, drop, 0.0)
            gone.append(jnp.dot(drop.astype(BF16), tri_buf[...], preferred_element_type=F32))
        for (chunk, masked, h), score, lost in zip(items, scores, gone):
            rows = slice(chunk * 256, chunk * 256 + 256)
            kept = kept_buf[zz, h, rows]
            weight = lax.exp2(score - lost - jnp.concatenate([kept, kept], axis=1))
            if masked:
                weight = jnp.where(ahead > slot * 256 - chunk * 2048, weight, 0.0)
            kept_buf[zz, h, rows] = kept + jnp.broadcast_to(lost[:, 0:1], (256, 128))
            weights.append(weight.astype(BF16))
        for chunk, _ in chunks:
            rows = slice(chunk * 256, chunk * 256 + 256)
            total = acc_buf[zz, rows]
            for (other, _, h), weight in zip(items, weights):
                if other == chunk:
                    values = v
                    if heads == 2:
                        values = jnp.where((lane[:256] < 64) if h == 0 else (lane[:256] >= 64), v, zero)
                    total = total + jnp.dot(weight, values, preferred_element_type=F32)
            acc_buf[zz, rows] = total

    def each_group(act):
        pl.when(x < 2)(lambda: act(2, LOG2E * 64**-0.5))
        pl.when(x >= 2)(lambda: act(1, LOG2E * 128**-0.5))

    def set_heads(heads, scale):
        queries = q_all[...].reshape(512, 128)
        if heads == 2:
            head_buf[0] = jnp.where(lane < 64, queries, zero)
            head_buf[1] = jnp.where(lane >= 64, queries, zero)
        else:
            head_buf[0] = queries

    def attend_row(dz):
        zz = z_at(-dz)

        def act(heads, scale):
            for near, chunks in ((True, ((1, True),)), (False, ((0, True), (1, False)))):

                @pl.when((zz >= 2) if near else (zz < 2))
                def _():
                    pl.loop(0, 4)(lambda k: attend(zz * 4 + 3 - k, zz, heads, chunks, scale))

        each_group(act)

    def join_rows(heads, scale):
        total, past = acc_buf[3], None
        for zz in (2, 1, 0):
            kept = kept_buf[zz + 1, 0]
            if heads == 2:
                kept = jnp.where(lane < 64, kept, kept_buf[zz + 1, 1])
            past = kept if past is None else past + kept
            total = total + acc_buf[zz] * lax.exp2(-past)
        mix_out[...] = total.reshape(16, 32, 128).astype(BF16)

    def secondary_waits(rows):
        @pl.when(jnp.logical_not(primary))
        def _():
            for dz in rows:
                arrived(kv_buf.at[pl.ds(pl.multiple_of(z_at(-dz) * 4, 4), 4)], kvp_sem.at[dz])

    @pl.when(primary)
    def _():
        for d in (1, 3):
            arrived(kv_buf.at[kv_slot(d, 0)], x_sem.at[d])
            to_column(d)
        from_row(0)
        arrived(kv_buf.at[kv_slot(2, 0)], x_sem.at[2])
        to_column(2)

    def all_but(mine, ref, sem):
        pl.when(mine)(lambda: arrived(ref.at[pl.ds(0, 15)], sem))
        pl.when(jnp.logical_not(mine))(lambda: arrived(ref, sem))

    all_but(primary, q_all, q_sem.at[1])
    each_group(set_heads)
    secondary_waits((0,))
    attend_row(0)

    @pl.when(primary)
    def _():
        from_row(1)
        from_row(3)
        from_row(2)

    run("keys1")
    secondary_waits((1, 3))
    attend_row(1)
    ow_pass(0)

    @pl.when(primary)
    def _():
        for d in (0, 1, 3, 2):
            from_far(d)

    run("keys2")
    attend_row(3)
    run("att1")
    secondary_waits((2,))
    attend_row(2)
    each_group(join_rows)

    def m_copy(dx, dz):
        return remote(
            mix_out.at[xz(dx, dz)], mix_all.at[mix_block, y_odd * 4 + x], m_sem.at[0],
            m_sem.at[1], {"sp": xz(dx, dz), "tp": mix_y * 2 + c},
        )

    def each_mixed(act):
        for dz in range(4):
            for dx in range(4):
                if (dx, dz) == (0, 0):
                    pl.when(jnp.logical_not(holds_own))(lambda: act(m_copy(dx, dz)))
                else:
                    act(m_copy(dx, dz))

    each_mixed(lambda copy: copy.start())

    @pl.when(holds_own)
    def _():
        mix_all[mix_block, y_odd * 4 + x] = mix_out[s]

    run("mix1")
    ow_pass(1)
    run("mix2")
    all_but(holds_own, mix_out, m_sem.at[1])
    arrived(outw.at[pl.ds(0, 4)], ow_sem.at[4])
    arrived(res_buf, load_sem.at[4])

    mixed = jnp.concatenate([mix_all[:, unit].reshape(64, 128) for unit in range(8)], axis=1)

    def ex_copy(n):
        columns = pl.ds(n * 512, 512)
        return remote(
            ex_out.at[:, columns], ex_in.at[:, columns], ex_sem.at[0], ex_sem.at[1],
            {"sp": s, "tp": (3 - y) * 2 + c},
        )

    for n in range(4):
        columns = slice(n * 512, n * 512 + 512)
        sums = jnp.dot(mixed, outw[:, :, columns].reshape(1024, 512), preferred_element_type=F32)
        att_buf[:, columns] = sums[:32]
        ex_out[:, columns] = sums[32:].astype(BF16)
        ex_copy(n).start()
    run("mix3")
    arrived(ex_in, ex_sem.at[1])
    updated = res_buf[...].astype(F32) + (att_buf[...] + ex_in[...].astype(F32))
    upd_buf[...] = updated
    scale = lax.rsqrt(jnp.mean(updated * updated, axis=-1, keepdims=True) + 1e-06)
    norm_buf[t] = (updated * scale * gain_ref[...]).astype(BF16)

    def row_copy(ref, target, k):
        return remote(ref, ref, row_sem.at[7], row_sem.at[k if k < 6 else 6], neighbour[target])

    def half_rows(dy, k, core=None):
        slot = y_at(dy) * 2 + (c if core is None else core)
        return norm_buf.at[slot, pl.ds(16 * k, 16)]

    def row_send_to(ref, target, k):
        row_copy(ref, target, k).start()

    row_send_to(half_rows(0, 0), ("y", 1), 0)
    row_send_to(half_rows(0, 1), ("y", -1), 1)
    row_send_to(half_rows(0, 1), ("y", 1), 2)
    row_send_to(half_rows(0, 0), ("y", -1), 3)
    row_send_to(norm_buf.at[t], "pair", 6)
    run("rows0")
    arrived(half_rows(-1, 0), row_sem.at[0])
    row_send_to(half_rows(-1, 0), ("y", 1), 4)
    arrived(half_rows(1, 1), row_sem.at[1])
    row_send_to(half_rows(1, 1), ("y", -1), 5)
    row_send_to(half_rows(-1, 0), "pair", 7)
    row_send_to(half_rows(1, 1), "pair", 8)
    run("rows1")
    arrived(half_rows(-1, 1), row_sem.at[2])
    row_send_to(half_rows(-1, 1), "pair", 9)
    arrived(half_rows(1, 0), row_sem.at[3])
    row_send_to(half_rows(1, 0), "pair", 10)
    run("rows2")
    arrived(half_rows(2, 0), row_sem.at[4])
    row_send_to(half_rows(2, 0), "pair", 11)
    arrived(half_rows(2, 1), row_sem.at[5])
    row_send_to(half_rows(2, 1), "pair", 12)
    arrived(norm_buf.at[pl.ds(0, 4)], row_sem.at[6])
    run("up")
    @pl.loop(0, 4)
    def _(n):
        columns = pl.ds(pl.multiple_of(n * 256, 256), 256)
        rows = norm_buf[...].reshape(256, 2048)
        pre = jnp.maximum(jnp.dot(rows, up_buf[:, columns], preferred_element_type=F32), 0.0)
        hidden_buf[:, columns] = (pre * pre).astype(BF16)

    def cols(r):
        return pl.ds(r * 512, 512)

    def pair_copy(r):
        return remote(
            part_buf.at[1 - c, :, :, cols(r)], pair_buf.at[:, :, cols(r)], y_send.at[0], pair_sem.at[r],
            neighbour["pair"],
        )

    def last_copy(r, k):
        return remote(
            last_out.at[k, :, cols(r)], last_in.at[k, :, cols(r)], y_send.at[1], last_sem.at[r],
            neighbour["y", (2, 1, -1)[k]],
        )

    def store_part(value, columns, width):
        blocks = value.reshape(4, 2, 32, width)
        for core in range(2):
            for yy in range(4):
                part_buf[core, yy, :, columns] = blocks[yy, core].astype(BF16)

    def pair_sum(r, dy):
        yy = y_at(dy)
        return part_buf[c, yy, :, cols(r)].astype(F32) + pair_buf[yy, :, cols(r)].astype(F32)

    def pair_step(r):
        pair_copy(r).wait_recv()
        for k, dy in enumerate((2, 1, -1)):
            last_out[k, :, cols(r)] = pair_sum(r, dy).astype(BF16)
            last_copy(r, k).start()

    def last_step(r):
        total = pair_sum(r, 0)
        arrived(last_in.at[:, :, cols(r)], last_sem.at[r])
        for k in range(3):
            total = total + last_in[k, :, cols(r)].astype(F32)
        return total

    def mixer_sums(r, dz):
        zz = lax.rem(z - dz + 4, 4)
        for pair in range(2):
            slot = zz * 4 + pair * 2
            w = jnp.concatenate([down_buf[slot], down_buf[slot + 1]], axis=1)
            value = jnp.dot(hidden_buf[...], w, preferred_element_type=F32)
            store_part(value, pl.ds(r * 512 + pair * 256, 256), 256)
        pair_copy(r).start()

    def finish(r, dz):
        columns = pl.ds(pl.multiple_of(lax.rem(z - dz + 4, 4) * 512, 512), 512)
        out_buf[:, columns] = (upd_buf[:, columns] + last_step(r)).astype(BF16)
        pltpu.make_async_copy(out_buf.at[:, columns], out_hbm.at[:, columns], out_sem.at[0]).start()

    rounds = tuple(enumerate(ROW_ORDER))
    for i, (r, dz) in enumerate(rounds):
        run(("row", dz))
        mixer_sums(r, dz)
        if i >= 1:
            pair_step(r - 1)
    pair_step(3)
    for r, dz in rounds:
        finish(r, dz)

    arrived(pair_buf, y_send.at[0])
    arrived(last_out, y_send.at[1])
    arrived(norm_buf.at[pl.ds(0, 7)], row_sem.at[7])
    arrived(outw.at[pl.ds(0, 2)], ow_sem.at[2])
    arrived(outw.at[pl.ds(0, 4)], ow_sem.at[3])
    arrived(ex_out, ex_sem.at[0])
    all_but(primary, q_all, q_sem.at[0])
    all_but(holds_own, mix_out, m_sem.at[0])
    for g, ref in enumerate((up_buf.at[pl.ds(0, 1920)], down_buf.at[pl.ds(0, 15)])):
        arrived(ref, send_sem.at[g])

    @pl.when(primary)
    def _():
        arrived(kv_buf.at[pl.ds(0, 12)], kv_send.at[0])
        arrived(kv_buf, kv_send.at[1])

    pltpu.make_async_copy(out_buf, out_hbm, out_sem.at[0]).wait()


def local(qn, kn, vn, qb, kb, vb, offn, offb, res, on, ob, gain, up, down):
    hbm = pl.BlockSpec(memory_space=pl.ANY)
    vmem = pl.BlockSpec(memory_space=pltpu.VMEM)
    dma = pltpu.SemaphoreType.DMA
    return pl.pallas_call(
        body,
        out_shape=jax.ShapeDtypeStruct((32, 2048), BF16),
        in_specs=[hbm, hbm, hbm, hbm, hbm, hbm, vmem, vmem, hbm, hbm, hbm, vmem, hbm, hbm],
        out_specs=hbm,
        scratch_shapes=[
            pltpu.VMEM((2, KV_ROWS, 128), BF16),
            pltpu.VMEM((16, KV_ROWS, 128), BF16),
            pltpu.VMEM((2048, 1024), BF16),
            pltpu.VMEM((16, 1024, 128), BF16),
            pltpu.VMEM((8, 128, 2048), BF16),
            pltpu.VMEM((2, 256, 128), BF16),
            pltpu.VMEM((16, 32, 128), BF16),
            pltpu.VMEM((2, 512, 128), BF16),
            pltpu.VMEM((4, 2, 512, 128), F32),
            pltpu.VMEM((4, 512, 128), F32),
            pltpu.VMEM((256, 256), BF16),
            pltpu.VMEM((16, 32, 128), BF16),
            pltpu.VMEM((2, 8, 32, 128), BF16),
            pltpu.VMEM((32, 2048), BF16),
            pltpu.VMEM((32, 2048), F32),
            pltpu.VMEM((32, 2048), BF16),
            pltpu.VMEM((32, 2048), BF16),
            pltpu.VMEM((2, 4, 32, 2048), BF16),
            pltpu.VMEM((4, 32, 2048), BF16),
            pltpu.VMEM((3, 32, 2048), BF16),
            pltpu.VMEM((3, 32, 2048), BF16),
            pltpu.VMEM((32, 2048), F32),
            pltpu.VMEM((8, 32, 2048), BF16),
            pltpu.VMEM((256, 1024), BF16),
            pltpu.VMEM((32, 2048), BF16),
            dma((7,)),
            dma((2, 4, 15)),
            dma((2,)),
            dma((4,)),
            dma((2,)),
            dma((4, 2)),
            dma((4, 2)),
            dma((2,)),
            dma((4,)),
            dma((2,)),
            dma((2,)),
            dma((5,)),
            dma((2,)),
            dma((4,)),
            dma((4,)),
            dma((8,)),
            dma((2,)),
            dma((1,)),
        ],
        compiler_params=pltpu.CompilerParams(
            collective_id=0, has_side_effects=True, vmem_limit_bytes=60 * 1024 * 1024
        ),
    )(qn, kn, vn, qb, kb, vb, offn, offb, res, on, ob, gain.reshape(1, 2048), up, down)


def solution(mesh):
    return jax.shard_map(
        local,
        mesh=mesh,
        in_specs=(
            P("sp", "tp"), P("sp", "tp"), P("sp", "tp"), P("sp", "tp"), P("sp", "tp"), P("sp", "tp"),
            P("tp", "sp"), P("tp", "sp"), P(("sp", "tp"), None), P("tp", None), P("tp", None), P(),
            P("sp", "tp"), P("tp", "sp"),
        ),
        out_specs=P(("sp", "tp"), None),
        check_vma=False,
    )
```
